32 devices in a mesh: grp: 2 (over x), tp: 16 (over z, y, core).
Axes of the slice: x: 2, y: 2, z: 4, core: 2. Of those that a mesh axis runs over, the one named last changes fastest.
Arguments:
- residual_channel: bfloat16 [256, 8, 4096], P('grp', None, 'tp'), parts along dimension 0, may hold values from -18 to 18, as said below
- prior_block_multiplier: float32 [2, 4096], replicated, may hold values from 0.1 to 1.9
- probe_map_matrix: bfloat16 [2, 4096, 2048], P(None, None, 'tp'), may hold values from -0.09375 to 0.09375
- lookup_map_matrix: bfloat16 [2, 4096, 2048], P(None, None, 'tp'), may hold values from -0.09375 to 0.09375
- content_map_matrix: bfloat16 [2, 4096, 2048], P(None, None, 'tp'), may hold values from -0.09375 to 0.09375
- emission_valve_matrix: bfloat16 [2, 4096, 2048], P(None, None, 'tp'), may hold values from -0.09375 to 0.09375
- forgetting_map_matrix: bfloat16 [2, 4096, 32], replicated, may hold values from -0.09375 to 0.09375
- insertion_rate_matrix: bfloat16 [2, 4096, 32], replicated, may hold values from -0.09375 to 0.09375
- forgetting_magnitude_exponent: float32 [2, 32], P(None, 'tp'), may hold values from -4.6 to -1.2
- channel_forgetting_offset: float32 [2, 32], P(None, 'tp'), may hold values from -2 to 1
- surplus_forgetting_amounts: float32 [2, 256, 8, 32], P(None, 'grp', None, 'tp'), parts along dimension 1, may hold values from -0.7 to 0
- readout_rescale_multiplier: float32 [2, 2048], P(None, 'tp'), may hold values from 0.1 to 1.9
- emission_map_matrix: bfloat16 [2, 2048, 4096], P(None, None, 'tp'), may hold values from -2 to 2
- post_mixing_multiplier: float32 [2, 4096], replicated, may hold values from 0.1 to 1.9
- recurrent_matrices: float32 [2, 256, 32, 4096], P(None, 'grp', 'tp'), parts along dimension 1, may hold values from -6 to 6
Outputs:
- new_stream: bfloat16 [256, 8, 4096], P('grp', None, 'tp'), parts along dimension 0
- new_memory: float32 [2, 256, 32, 4096], P(None, 'grp', 'tp'), parts along dimension 1
The draws below stay inside these ranges and needn't reach their ends.
There are 2 independent parts, one for each index of `grp`. The reference program is written for one: setup_inputs(seed, part) draws one part's arguments, and reference() takes and returns one part's arrays. A program takes and returns all parts, laid end to end along the dimension named above; an argument that names none is the same for every part. Nothing has to cross between parts.
Inputs may be any that keep to these rules, and one draw needn't show every extreme that they name: `residual_channel`: column scales of the features differ widely.
All inputs are finite; a program needn't handle non-finite values.
Results may differ from the reference program's by a relative error of at most 0.0081.
Values may be sent and summed in bfloat16 or wider, within the bound.
A program may use at most 192 MiB of HBM per device.

```python
import math
import jax
import jax.numpy as jnp
from jax import lax

D = 4096
HEADS = 32
HEAD_DIM = 64
LAYERS = 2
STEPS = 8
SEQS = 128
MIXW = 2048


def column_scales(key, count):
    ramp = jnp.exp(math.log(0.4) + math.log(8.0) * jnp.arange(count, dtype=jnp.float32) / count)
    return ramp * jax.random.uniform(key, (count,), jnp.float32, 0.6, 1.4)


def draw_residual_channel(key, part):
    key_cols = jax.random.fold_in(key, 11)
    key_vals = jax.random.fold_in(key, 12)
    columns = column_scales(key_cols, D)
    entries = jnp.clip(jax.random.normal(key_vals, (SEQS, STEPS, D), jnp.float32), -4.0, 4.0)
    return (entries * columns).astype(jnp.bfloat16)


def draw_emission_map_matrix(key, part):
    key_cols = jax.random.fold_in(key, 21)
    key_vals = jax.random.fold_in(key, 22)
    columns = column_scales(key_cols, D)
    entries = jnp.clip(jax.random.normal(key_vals, (LAYERS, MIXW, D), jnp.float32), -3.0, 3.0)
    return (entries * columns * MIXW ** (-0.5)).astype(jnp.bfloat16)


def draw_surplus_forgetting_amounts(key, part):
    key_mask = jax.random.fold_in(key, 31)
    key_depth = jax.random.fold_in(key, 32)
    chosen = jax.random.bernoulli(key_mask, 0.12, (LAYERS, SEQS, STEPS, HEADS))
    depth = jax.random.uniform(key_depth, (LAYERS, SEQS, STEPS, HEADS), jnp.float32, math.log(0.5), math.log(0.8))
    return jnp.where(chosen, depth, 0.0).astype(jnp.float32)


def level_of(key, extent, pieces, least, largest):
    level = 1.0
    for dim, shards_of in pieces:
        heights = jax.random.uniform(jax.random.fold_in(jax.random.fold_in(key, 6), dim), (shards_of,), jnp.float32, least / len(pieces), largest / len(pieces))
        level = level * jnp.repeat(jnp.exp(heights), extent[dim] // shards_of).reshape((-1,) + (1,) * (len(extent) - 1 - dim))
    return level


def normal_values(stream_key, shape, width, bound, split=(), held_as=jnp.bfloat16):
    gain = level_of(stream_key, shape, split, -0.22, 0.18) if split else 1.0
    result = jax.random.normal(stream_key, shape, jnp.float32) * width * gain
    return jnp.minimum(jnp.maximum(result, -bound), bound).astype(held_as)


def setup_inputs(seed: int = 0, part: int = 0) -> dict:
    key_of = jax.random.split(jax.random.key(seed), 16)
    own_keys = jax.random.split(jax.random.fold_in(key_of[15], part), 16)
    return {
        "residual_channel": draw_residual_channel(jax.random.fold_in(jax.random.fold_in(key_of[15], part), 71), part),
        "prior_block_multiplier": jnp.clip(1.0 + 0.18 * jax.random.normal(key_of[1], (LAYERS, D), jnp.float32), 0.1, 1.9),
        "probe_map_matrix": normal_values(key_of[2], (LAYERS, D, MIXW), D ** -0.5, 0.09375, ((2, 16),)),
        "lookup_map_matrix": normal_values(key_of[3], (LAYERS, D, MIXW), D ** -0.5, 0.09375, ((2, 16),)),
        "content_map_matrix": normal_values(key_of[4], (LAYERS, D, MIXW), D ** -0.5, 0.09375, ((2, 16),)),
        "emission_valve_matrix": normal_values(key_of[5], (LAYERS, D, MIXW), D ** -0.5, 0.09375, ((2, 16),)),
        "forgetting_map_matrix": normal_values(key_of[6], (LAYERS, D, HEADS), D ** -0.5, 0.09375),
        "insertion_rate_matrix": normal_values(key_of[7], (LAYERS, D, HEADS), D ** -0.5, 0.09375),
        "forgetting_magnitude_exponent": jnp.clip(-4.6 + 3.3999999 * jax.random.uniform(key_of[8], (LAYERS, HEADS), jnp.float32) ** level_of(key_of[8], (LAYERS, HEADS), ((1, 16),), -0.2, 0.2), -4.6, -1.2),
        "channel_forgetting_offset": jnp.clip(-2.0 + 3.0 * jax.random.uniform(key_of[9], (LAYERS, HEADS), jnp.float32) ** level_of(key_of[9], (LAYERS, HEADS), ((1, 16),), -0.2, 0.2), -2.0, 1.0),
        "surplus_forgetting_amounts": draw_surplus_forgetting_amounts(jax.random.fold_in(jax.random.fold_in(key_of[15], part), 71), part),
        "readout_rescale_multiplier": jnp.clip(1.0 + 0.18 * jax.random.normal(key_of[11], (LAYERS, MIXW), jnp.float32), 0.1, 1.9),
        "emission_map_matrix": draw_emission_map_matrix(jax.random.fold_in(key_of[15], 71), part),
        "post_mixing_multiplier": jnp.clip(1.0 + 0.18 * jax.random.normal(key_of[13], (LAYERS, D), jnp.float32), 0.1, 1.9),
        "recurrent_matrices": normal_values(own_keys[14], (LAYERS, SEQS, HEADS, HEAD_DIM * HEAD_DIM), 1.0, 6.0, ((2, 16),), jnp.float32),
    }


EPS = 1e-06
HIGH = lax.Precision.HIGHEST

def solve_lower(a_mat, right_side):
    length = right_side.shape[-2]
    solved_rows = []
    for row_at in range(length):
        current_row = right_side[..., row_at, :]
        for col_at in range(row_at):
            current_row = current_row - a_mat[..., row_at, col_at][..., None] * solved_rows[col_at]
        solved_rows.append(current_row)
    return jnp.stack(solved_rows, axis=-2)

def delta_block(queries, key_rows, values, forgetting_exponent_amount, strength, matrix_state):
    length = queries.shape[2]
    causal = jnp.tril(jnp.ones((length, length), bool))
    strict = jnp.tril(jnp.ones((length, length), bool), -1)
    cumulative = jnp.cumsum(forgetting_exponent_amount, axis=-1)
    decay_mat = jnp.where(causal, jnp.exp(jnp.where(causal, cumulative[..., :, None] - cumulative[..., None, :], 0.0)), 0.0)
    key_gram = jnp.einsum('bhtd,bhsd->bhts', key_rows, key_rows, precision=HIGH)
    a_mat = jnp.where(strict, strength[..., :, None] * decay_mat * key_gram, 0.0)
    right_side = jnp.concatenate([strength[..., None] * values, (strength * jnp.exp(cumulative))[..., None] * key_rows], axis=-1)
    solved = solve_lower(a_mat, right_side)
    width_v = values.shape[-1]
    update = solved[..., :width_v] - jnp.einsum('bhtk,bhkv->bhtv', solved[..., width_v:], matrix_state, precision=HIGH)
    scores = jnp.einsum('bhtd,bhsd->bhts', queries, key_rows, precision=HIGH) * decay_mat
    output = jnp.exp(cumulative)[..., None] * jnp.einsum('bhtk,bhkv->bhtv', queries, matrix_state, precision=HIGH)
    output = output + jnp.einsum('bhts,bhsv->bhtv', scores, update, precision=HIGH)
    final_log = cumulative[..., -1:]
    revised_memory_matrix = jnp.exp(final_log)[..., None] * matrix_state + jnp.einsum('bhsk,bhsv->bhkv', key_rows * jnp.exp(final_log - cumulative)[..., None], update, precision=HIGH)
    return (output, revised_memory_matrix)

def unit_rows(matrix):
    return matrix * lax.rsqrt(lax.optimization_barrier(jnp.sum(matrix * matrix, axis=-1, keepdims=True)) + EPS)

def token_blender(mapped_token_vectors, magnitude_exponent, offset_terms_array, surplus_forgetting_exponent, multiplier_terms_array, incoming_memory_matrix, batch_total, generation_round_total):
    rounded = [lax.optimization_barrier(part_sum.astype(jnp.bfloat16)).astype(jnp.float32) for part_sum in mapped_token_vectors]
    queries, keys_raw, values_raw, gate_raw, decay_pre, strength_pre = rounded
    head_count = incoming_memory_matrix.shape[1]

    def to_heads(matrix):
        return matrix.reshape(batch_total, generation_round_total, head_count, HEAD_DIM).transpose(0, 2, 1, 3)

    def per_head(matrix):
        return matrix.reshape(batch_total, generation_round_total, head_count).transpose(0, 2, 1)
    queries = unit_rows(jax.nn.silu(to_heads(queries))) * HEAD_DIM ** (-0.5)
    key_rows = unit_rows(jax.nn.silu(to_heads(keys_raw)))
    values = jax.nn.silu(to_heads(values_raw))
    forgetting_exponent_amount = -jnp.exp(magnitude_exponent)[None, :, None] * jax.nn.softplus(per_head(decay_pre) + offset_terms_array[None, :, None])
    forgetting_exponent_amount = forgetting_exponent_amount + surplus_forgetting_exponent.transpose(0, 2, 1)
    strength = jax.nn.sigmoid(per_head(strength_pre))
    matrix_state = incoming_memory_matrix.reshape(batch_total, head_count, HEAD_DIM, HEAD_DIM)
    output, revised_memory_matrix = delta_block(queries, key_rows, values, forgetting_exponent_amount, strength, matrix_state)
    normed = output * lax.rsqrt(lax.optimization_barrier(jnp.mean(output * output, axis=-1, keepdims=True)) + EPS)
    normed = normed * multiplier_terms_array.reshape(head_count, HEAD_DIM)[None, :, None, :] * jax.nn.silu(to_heads(gate_raw))
    blended_token_vectors = normed.transpose(0, 2, 1, 3).reshape(batch_total * generation_round_total, head_count * HEAD_DIM).astype(jnp.bfloat16)
    return (blended_token_vectors, revised_memory_matrix.reshape(batch_total, head_count, HEAD_DIM * HEAD_DIM))

def reference(residual_channel, prior_block_multiplier, probe_map_matrix, lookup_map_matrix, content_map_matrix, emission_valve_matrix, forgetting_map_matrix, insertion_rate_matrix, forgetting_magnitude_exponent, channel_forgetting_offset, surplus_forgetting_amounts, readout_rescale_multiplier, emission_map_matrix, post_mixing_multiplier, recurrent_matrices):
    batch_total, generation_round_total = (residual_channel.shape[0], residual_channel.shape[1])
    current = residual_channel.reshape(batch_total * generation_round_total, D)
    states = []
    for block_index_number in range(LAYERS):
        widened = current.astype(jnp.float32)
        inv_rms = lax.rsqrt(lax.optimization_barrier(jnp.mean(widened * widened, axis=-1, keepdims=True)) + EPS)
        hidden = (widened * inv_rms * prior_block_multiplier[block_index_number]).astype(jnp.bfloat16)
        mapped_token_vectors = tuple((jnp.dot(hidden, weight[block_index_number], preferred_element_type=jnp.float32) for weight in (probe_map_matrix, lookup_map_matrix, content_map_matrix, emission_valve_matrix, forgetting_map_matrix, insertion_rate_matrix)))
        blended_token_vectors, revised_memory_matrix = token_blender(mapped_token_vectors, forgetting_magnitude_exponent[block_index_number], channel_forgetting_offset[block_index_number], surplus_forgetting_amounts[block_index_number], readout_rescale_multiplier[block_index_number], recurrent_matrices[block_index_number], batch_total, generation_round_total)
        mixed_out = jnp.dot(blended_token_vectors, emission_map_matrix[block_index_number], preferred_element_type=jnp.float32).astype(jnp.bfloat16)
        mixed_wide = lax.optimization_barrier(mixed_out).astype(jnp.float32)
        post_rms = lax.rsqrt(lax.optimization_barrier(jnp.mean(mixed_wide * mixed_wide, axis=-1, keepdims=True)) + EPS)
        current = lax.optimization_barrier((widened + mixed_wide * post_rms * post_mixing_multiplier[block_index_number]).astype(jnp.bfloat16))
        states.append(revised_memory_matrix)
    return (current.reshape(batch_total, generation_round_total, D), jnp.stack(states, axis=0))
```

```python
import jax
import jax.numpy as jnp
from jax import lax
from jax.experimental import pallas as pl
from jax.experimental.pallas import tpu as pltpu
from jax.sharding import PartitionSpec as P

D = 4096
HEAD_DIM = 64
LAYERS = 2


EPS = 1e-06
HIGH = lax.Precision.HIGHEST


def solve_lower(a_mat, right_side):
    length = right_side.shape[-2]
    solved_rows = []
    for row_at in range(length):
        current_row = right_side[..., row_at, :]
        for col_at in range(row_at):
            current_row = current_row - a_mat[..., row_at, col_at][..., None] * solved_rows[col_at]
        solved_rows.append(current_row)
    return jnp.stack(solved_rows, axis=-2)


def delta_block(queries, key_rows, values, forgetting_exponent_amount, strength, matrix_state):
    length = queries.shape[2]
    causal = jnp.tril(jnp.ones((length, length), bool))
    strict = jnp.tril(jnp.ones((length, length), bool), -1)
    cumulative = jnp.cumsum(forgetting_exponent_amount, axis=-1)
    decay_mat = jnp.where(
        causal,
        jnp.exp(jnp.where(causal, cumulative[..., :, None] - cumulative[..., None, :], 0.0)),
        0.0,
    )
    key_gram = jnp.einsum("bhtd,bhsd->bhts", key_rows, key_rows, precision=HIGH)
    a_mat = jnp.where(strict, strength[..., :, None] * decay_mat * key_gram, 0.0)
    right_side = jnp.concatenate(
        [strength[..., None] * values, (strength * jnp.exp(cumulative))[..., None] * key_rows],
        axis=-1,
    )
    solved = solve_lower(a_mat, right_side)
    width_v = values.shape[-1]
    update = solved[..., :width_v] - jnp.einsum(
        "bhtk,bhkv->bhtv", solved[..., width_v:], matrix_state, precision=HIGH
    )
    scores = jnp.einsum("bhtd,bhsd->bhts", queries, key_rows, precision=HIGH) * decay_mat
    output = jnp.exp(cumulative)[..., None] * jnp.einsum(
        "bhtk,bhkv->bhtv", queries, matrix_state, precision=HIGH
    )
    output = output + jnp.einsum("bhts,bhsv->bhtv", scores, update, precision=HIGH)
    final_log = cumulative[..., -1:]
    revised_memory_matrix = jnp.exp(final_log)[..., None] * matrix_state + jnp.einsum(
        "bhsk,bhsv->bhkv",
        key_rows * jnp.exp(final_log - cumulative)[..., None],
        update,
        precision=HIGH,
    )
    return (output, revised_memory_matrix)


def unit_rows(matrix):
    return matrix * lax.rsqrt(jnp.sum(matrix * matrix, axis=-1, keepdims=True) + EPS)


def token_blender(
    mapped_token_vectors,
    magnitude_exponent,
    offset_terms_array,
    surplus_forgetting_exponent,
    multiplier_terms_array,
    incoming_memory_matrix,
    batch_total,
    generation_round_total,
):
    rounded = [
        lax.optimization_barrier(part_sum.astype(jnp.bfloat16)).astype(jnp.float32)
        for part_sum in mapped_token_vectors
    ]
    queries, keys_raw, values_raw, gate_raw, decay_pre, strength_pre = rounded
    head_count = incoming_memory_matrix.shape[1]

    def to_heads(matrix):
        return matrix.reshape(batch_total, generation_round_total, head_count, HEAD_DIM).transpose(
            0, 2, 1, 3
        )

    def per_head(matrix):
        return matrix.reshape(batch_total, generation_round_total, head_count).transpose(0, 2, 1)

    queries = unit_rows(jax.nn.silu(to_heads(queries))) * HEAD_DIM ** (-0.5)
    key_rows = unit_rows(jax.nn.silu(to_heads(keys_raw)))
    values = jax.nn.silu(to_heads(values_raw))
    forgetting_exponent_amount = -jnp.exp(magnitude_exponent)[None, :, None] * jax.nn.softplus(
        per_head(decay_pre) + offset_terms_array[None, :, None]
    )
    forgetting_exponent_amount = forgetting_exponent_amount + surplus_forgetting_exponent.transpose(
        0, 2, 1
    )
    strength = jax.nn.sigmoid(per_head(strength_pre))
    matrix_state = incoming_memory_matrix.reshape(batch_total, head_count, HEAD_DIM, HEAD_DIM)
    output, revised_memory_matrix = delta_block(
        queries, key_rows, values, forgetting_exponent_amount, strength, matrix_state
    )
    normed = output * lax.rsqrt(jnp.mean(output * output, axis=-1, keepdims=True) + EPS)
    normed = (
        normed
        * multiplier_terms_array.reshape(head_count, HEAD_DIM)[None, :, None, :]
        * jax.nn.silu(to_heads(gate_raw))
    )
    blended_token_vectors = (
        normed.transpose(0, 2, 1, 3)
        .reshape(batch_total * generation_round_total, head_count * HEAD_DIM)
        .astype(jnp.bfloat16)
    )
    return (
        blended_token_vectors,
        revised_memory_matrix.reshape(batch_total, head_count, HEAD_DIM * HEAD_DIM),
    )


LANES = 128


def bf16_dot(left, right):
    return jnp.dot(left, right, preferred_element_type=jnp.float32)


def head_sums(squares, ones):
    high = squares.astype(jnp.bfloat16)
    low = (squares - high.astype(jnp.float32)).astype(jnp.bfloat16)
    return bf16_dot(high, ones) + bf16_dot(low, ones)


def project(portion, weights):
    return tuple(
        (jnp.dot(portion, weight, preferred_element_type=jnp.float32) for weight in weights)
    )


def out_project(blended_token_vectors, weight_rows):
    return jnp.dot(
        lax.all_gather(blended_token_vectors, "tp", axis=1, tiled=True),
        weight_rows,
        preferred_element_type=jnp.float32,
    ).astype(jnp.bfloat16)


def post_residual(widened, mixed_out, multiplier_terms_array, complete):
    mixed_wide = lax.optimization_barrier(mixed_out).astype(jnp.float32)
    squares = jnp.sum(mixed_wide * mixed_wide, axis=-1)
    if not complete:
        squares = lax.psum(squares, "tp")
    post_rms = lax.rsqrt(squares / D + EPS)[:, None]
    return lax.optimization_barrier(
        (widened + mixed_wide * post_rms * multiplier_terms_array).astype(jnp.bfloat16)
    )


def local(
    residual_channel,
    prior_block_multiplier,
    probe_map_matrix,
    lookup_map_matrix,
    content_map_matrix,
    emission_valve_matrix,
    forgetting_map_matrix,
    insertion_rate_matrix,
    forgetting_magnitude_exponent,
    channel_forgetting_offset,
    surplus_forgetting_amounts,
    readout_rescale_multiplier,
    emission_map_matrix,
    post_mixing_multiplier,
    recurrent_matrices,
):
    batch_total, generation_round_total, own_width = residual_channel.shape
    head_count = recurrent_matrices.shape[2]
    row_count = batch_total * generation_round_total
    col_offset = lax.axis_index("tp") * own_width
    head_offset = lax.axis_index("tp") * head_count
    new_states = []

    def mix_layer(mapped_token_vectors, block_index_number):
        blended_token_vectors, revised_memory_matrix = token_blender(
            mapped_token_vectors,
            forgetting_magnitude_exponent[block_index_number],
            channel_forgetting_offset[block_index_number],
            surplus_forgetting_amounts[block_index_number],
            readout_rescale_multiplier[block_index_number],
            recurrent_matrices[block_index_number],
            batch_total,
            generation_round_total,
        )
        new_states.append(revised_memory_matrix)
        return out_project(blended_token_vectors, emission_map_matrix[block_index_number])

    def own_cols(matrix):
        return lax.dynamic_slice_in_dim(matrix, col_offset, own_width, matrix.ndim - 1)

    whole_rows = lax.all_gather(
        residual_channel.reshape(row_count, own_width), "tp", axis=1, tiled=True
    )
    current = whole_rows
    for block_index_number in range(LAYERS):
        widened = whole_rows.astype(jnp.float32)
        inv_rms = lax.rsqrt(jnp.mean(widened * widened, axis=-1, keepdims=True) + EPS)
        hidden = (widened * inv_rms * prior_block_multiplier[block_index_number]).astype(
            jnp.bfloat16
        )
        weights = (
            probe_map_matrix[block_index_number],
            lookup_map_matrix[block_index_number],
            content_map_matrix[block_index_number],
            emission_valve_matrix[block_index_number],
            lax.dynamic_slice_in_dim(
                forgetting_map_matrix[block_index_number], head_offset, head_count, 1
            ),
            lax.dynamic_slice_in_dim(
                insertion_rate_matrix[block_index_number], head_offset, head_count, 1
            ),
        )
        mapped_token_vectors = project(hidden, weights)
        mixed_out = mix_layer(mapped_token_vectors, block_index_number)
        if block_index_number < LAYERS - 1:
            gathered = lax.all_gather(mixed_out, "tp", axis=1, tiled=True)
            whole_rows = post_residual(
                widened, gathered, post_mixing_multiplier[block_index_number], True
            )
        else:
            current = post_residual(
                own_cols(widened),
                mixed_out,
                own_cols(post_mixing_multiplier[block_index_number]),
                False,
            )
    return (
        current.reshape(batch_total, generation_round_total, own_width),
        jnp.stack(new_states, axis=0),
    )


CHUNKS = 4
GROUP_ROWS = 64


def step_kernel(
    count,
    chunks,
    x_hbm,
    probe_hbm,
    lookup_hbm,
    content_hbm,
    valve_hbm,
    forget_hbm,
    insert_hbm,
    emission_hbm,
    states_hbm,
    surplus_ref,
    pre_gain_ref,
    post_gain_ref,
    read_gain_ref,
    magnitude_ref,
    offset_ref,
    out_ref,
    new_hbm,
    in_ref,
    y_ref,
    w_ref,
    wo_ref,
    rates_ref,
    h_ref,
    x1_ref,
    xown_ref,
    mown_ref,
    sq_ref,
    sur_ref,
    state_ref,
    new_ref,
    proj_ref,
    rate_ref,
    grown_ref,
    qk_ref,
    xq_ref,
    kd_ref,
    u_ref,
    qs_ref,
    dec_ref,
    spread_ref,
    ones_ref,
    perm_ref,
    load_sem,
    state_sem,
    own_sem,
    in_sem,
    y_sem,
    sq_sem,
):
    f32, bf16 = jnp.float32, jnp.bfloat16
    me = lax.axis_index("tp")
    depth = count // 4
    core, row, line = lax.rem(me, 2), lax.rem(me // 2, 2), me // 4
    over, twin = me + 2 - 4 * row, me + 1 - 2 * core
    items = 2 * chunks
    rows = h_ref.shape[0]
    seqs, steps = qk_ref.shape[1], qk_ref.shape[2]
    width = in_ref.shape[3]
    heads = forget_hbm.shape[1]
    own_heads = heads // count

    loads = []
    for layer in range(2):
        for at, matrix in enumerate((probe_hbm, lookup_hbm, content_hbm, valve_hbm)):
            loads.append(
                (matrix.at[layer], w_ref.at[layer, :, pl.ds(at * LANES, LANES)])
            )
        loads.append((forget_hbm.at[layer], rates_ref.at[layer, pl.ds(0, heads), :]))
        loads.append((insert_hbm.at[layer], rates_ref.at[layer, pl.ds(heads, heads), :]))
        loads.append((emission_hbm.at[layer], wo_ref.at[layer]))
    loads = [
        pltpu.make_async_copy(source, target, load_sem.at[at])
        for at, (source, target) in enumerate(loads)
    ]
    for copy in loads:
        copy.start()

    def state_load(item):
        return pltpu.make_async_copy(
            states_hbm.at[item // chunks, pl.ds(lax.rem(item, chunks) * seqs, seqs)],
            state_ref.at[lax.rem(item, 2)],
            state_sem.at[0, lax.rem(item, 2)],
        )

    def state_store(item):
        return pltpu.make_async_copy(
            new_ref.at[lax.rem(item, 2)],
            new_hbm.at[item // chunks, pl.ds(lax.rem(item, chunks) * seqs, seqs)],
            state_sem.at[1, lax.rem(item, 2)],
        )

    state_load(0).start()

    barrier = pltpu.get_barrier_semaphore()
    for step in range(1, count):
        pl.semaphore_signal(
            barrier,
            inc=1,
            device_id={"tp": lax.rem(me + step, count)},
            device_id_type=pl.DeviceIdType.MESH,
        )
    pl.semaphore_wait(barrier, count - 1)

    def remote(source, target, send_sem, land_sem, device):
        return pltpu.make_async_remote_copy(
            src_ref=source,
            dst_ref=target,
            send_sem=send_sem,
            recv_sem=land_sem,
            device_id={"tp": device},
            device_id_type=pl.DeviceIdType.MESH,
        )

    def along(step):
        return 4 * (lax.rem(line + step, depth) - line)

    def begin(buf, sems, item, source):
        for step in range(1, depth):
            remote(
                source, buf.at[item, me], sems.at[0, item], sems.at[1, item], me + along(step)
            ).start()
        remote(source, buf.at[item, me], sems.at[0, item], sems.at[1, item], over).start()
        remote(source, buf.at[item, me], sems.at[0, item], sems.at[3, item], twin).start()

    def pass_on(buf, sems, item, origin, kind, device):
        block = buf.at[item, origin]
        remote(block, block, sems.at[0, item], sems.at[kind, item], device).start()

    def landed(buf, sems, item, kind, blocks):
        part = buf.at[item, pl.ds(0, blocks)]
        remote(part, part, sems.at[0, item], sems.at[kind, item], twin).wait_recv()

    def relay_over(buf, sems, item):
        landed(buf, sems, item, 1, depth)
        for step in range(1, depth):
            pass_on(buf, sems, item, me + along(depth - step), 2, over)
        for step in range(1, depth):
            pass_on(buf, sems, item, me + along(depth - step), 3, twin)
        pass_on(buf, sems, item, over, 3, twin)

    def relay_twin(buf, sems, item):
        landed(buf, sems, item, 2, depth - 1)
        for step in range(1, depth):
            pass_on(buf, sems, item, over + along(depth - step), 3, twin)

    def complete(buf, sems, item):
        landed(buf, sems, item, 3, 2 * depth)

    def drained(buf, sems, item):
        blocks = (depth + 1) + (2 * depth - 1) + (depth - 1)
        part = buf.at[item, pl.ds(0, blocks)]
        remote(part, part, sems.at[0, item], sems.at[1, item], twin).wait_send()

    def own_copy(item):
        return pltpu.make_async_copy(
            x_hbm.at[pl.ds(item * rows, rows), :], in_ref.at[item, me], own_sem.at[item]
        )

    def begin_x(item):
        begin(in_ref, in_sem, item, x_hbm.at[pl.ds(item * rows, rows), :])
        own_copy(item).start()

    begin_x(0)
    begin_x(1)

    def iota(shape, axis):
        return lax.broadcasted_iota(jnp.int32, shape, axis)

    shape = (2 * heads, 2 * LANES)
    wanted = iota(shape, 1) // HEAD_DIM
    wanted = jnp.where(wanted >= 2, wanted - 2 + heads, wanted) + me * own_heads
    spread_ref[...] = jnp.where(iota(shape, 0) == wanted, 1.0, 0.0).astype(bf16)
    shape = (2 * LANES, 2 * LANES)
    ones_ref[...] = jnp.where(
        iota(shape, 0) // HEAD_DIM == iota(shape, 1) // HEAD_DIM, 1.0, 0.0
    ).astype(bf16)
    shape = (LANES, LANES)
    head, channel = iota(shape, 0) // HEAD_DIM, iota(shape, 0) % HEAD_DIM
    target = (channel % 2) * HEAD_DIM + (channel // 2) * 2 + head
    perm_ref[...] = jnp.where(target == iota(shape, 1), 1.0, 0.0).astype(bf16)
    all_seqs = sur_ref.shape[1]
    first_head = iota((LANES, all_seqs), 0) < HEAD_DIM
    for layer in range(2):
        for step in range(steps):
            pair = surplus_ref[layer, step]
            wide = jnp.where(first_head, pair[0:1, :], pair[1:2, :])
            sur_ref[layer, :, step, :] = wide.T

    relay_over(in_ref, in_sem, 0)
    relay_twin(in_ref, in_sem, 0)
    for copy in loads:
        copy.wait()

    def squares(matrix):
        return matrix[:, :LANES] * matrix[:, :LANES] + matrix[:, LANES:] * matrix[:, LANES:]

    def inverse(total):
        return lax.rsqrt(jnp.sum(total, axis=1, keepdims=True) * (1.0 / D) + EPS)

    def cols_of(origin):
        return pl.ds(origin * width, width)

    def first_hidden(item):
        def part(group, carry):
            at = pl.ds(group * GROUP_ROWS, GROUP_ROWS)
            total = jnp.zeros((GROUP_ROWS, LANES), f32)
            for origin in range(count):
                total = total + squares(in_ref[item, origin, at, :].astype(f32))
            scale = inverse(total)
            for origin in range(count):
                block = in_ref[item, origin, at, :].astype(f32)
                gain = pre_gain_ref[0:1, cols_of(origin)]
                h_ref[at, cols_of(origin)] = (block * scale * gain).astype(bf16)
            return carry

        lax.fori_loop(0, rows // GROUP_ROWS, part, 0)

    def second_hidden(item):
        earlier = item - chunks

        def part(group, carry):
            at = pl.ds(group * GROUP_ROWS, GROUP_ROWS)
            total = jnp.zeros((GROUP_ROWS, LANES), f32)
            for origin in range(count):
                total = total + squares(in_ref[item, origin, at, :].astype(f32))
            scale = inverse(total)
            total = jnp.zeros((GROUP_ROWS, LANES), f32)
            for origin in range(count):
                mixed = in_ref[item, origin, at, :].astype(f32)
                before = in_ref[earlier, origin, at, :].astype(f32)
                gain = post_gain_ref[0:1, cols_of(origin)]
                after = (before + mixed * scale * gain).astype(bf16)
                x1_ref[origin, at, :] = after
                total = total + squares(after.astype(f32))
            scale = inverse(total)
            for origin in range(count):
                block = x1_ref[origin, at, :].astype(f32)
                gain = pre_gain_ref[1:2, cols_of(origin)]
                h_ref[at, cols_of(origin)] = (block * scale * gain).astype(bf16)
            xown_ref[earlier, at, :] = x1_ref[me, at, :]
            return carry

        lax.fori_loop(0, rows // GROUP_ROWS, part, 0)

    def cols(at):
        return proj_ref[:, at * LANES : (at + 1) * LANES].astype(f32)

    def tokens(matrix):
        return matrix.reshape(seqs, steps, LANES)

    def lane_pair(ref, layer):
        left = iota((1, LANES), 1) < HEAD_DIM
        return jnp.where(left, ref[layer, 0], ref[layer, 1])

    def prepare(layer, chunk):
        ones = ones_ref[...]
        perm = perm_ref[...]
        queries = jax.nn.silu(cols(0))
        keys = jax.nn.silu(cols(1))
        sums = head_sums(jnp.concatenate([queries * queries, keys * keys], axis=1), ones)
        queries = tokens(queries * lax.rsqrt(sums[:, :LANES] + EPS) * HEAD_DIM ** (-0.5))
        keys = tokens(keys * lax.rsqrt(sums[:, LANES:] + EPS))
        spread = bf16_dot(rate_ref[...], spread_ref[...])
        biased = spread[:, :LANES] + lane_pair(offset_ref, layer)
        softplus = jnp.maximum(biased, 0.0) + jnp.log1p(jnp.exp(-jnp.abs(biased)))
        pace = -jnp.exp(lane_pair(magnitude_ref, layer))
        cumulative = tokens(pace * softplus) + sur_ref[layer, pl.ds(chunk * seqs, seqs)]
        beta = tokens(jax.nn.sigmoid(spread[:, LANES:]))
        token = lax.broadcasted_iota(jnp.int32, (seqs, steps, LANES), 1)
        shift = 1
        while shift < steps:
            moved = pltpu.roll(cumulative, shift, axis=1)
            cumulative = cumulative + jnp.where(token >= shift, moved, 0.0)
            shift *= 2
        grown = jnp.exp(cumulative)
        grown_ref[...] = grown
        solved_u = beta * tokens(jax.nn.silu(cols(2)))
        solved_p = beta * grown * keys
        for at in range(steps):
            causal = token >= at
            gap = jnp.where(causal, cumulative - cumulative[:, at : at + 1, :], 0.0)
            decay = jnp.where(causal, jnp.exp(gap), 0.0)
            key_row = keys[:, at : at + 1, :]
            pair = jnp.concatenate([queries * key_row, keys * key_row], axis=2)
            dots = bf16_dot(pair.reshape(rows, 2 * LANES).astype(bf16), ones)
            qk_ref[at] = tokens(dots[:, :LANES]) * decay
            if at < steps - 1:
                a_col = jnp.where(token > at, beta * decay * tokens(dots[:, LANES:]), 0.0)
                solved_u = solved_u - a_col * solved_u[:, at : at + 1, :]
                solved_p = solved_p - a_col * solved_p[:, at : at + 1, :]
        last = cumulative[:, steps - 1 : steps, :]
        faded = keys * jnp.exp(last - cumulative)

        def permuted(first, second):
            both = jnp.concatenate([first, second], axis=1).reshape(2 * rows, LANES)
            return bf16_dot(both.astype(bf16), perm).astype(bf16).reshape(seqs, 2 * steps, LANES)

        xq_ref[...] = permuted(queries, solved_p)
        kd_ref[...] = permuted(faded, faded)
        u_ref[...] = solved_u
        dec_ref[...] = jnp.broadcast_to(jnp.exp(last), (seqs, steps, LANES))

    state_rows = state_ref.shape[2]

    def advance(slot):
        even = iota((state_rows, LANES), 0) % 2 == 0
        left = iota((state_rows, LANES), 1) < HEAD_DIM
        kept = even == left

        def one_sequence(at, carry):
            state = state_ref[slot, at]
            turned = pltpu.roll(state, HEAD_DIM, axis=1)
            upper = jnp.where(kept, jnp.where(even, state, turned), 0.0)
            lower = jnp.where(kept, jnp.where(even, turned, state), 0.0)
            wide = jnp.concatenate([upper, lower], axis=0).astype(bf16)
            read = bf16_dot(xq_ref[at], wide)
            qs_ref[at] = read[:steps]
            update = u_ref[at] - read[steps:]
            u_ref[at] = update
            high = update.astype(bf16).astype(f32)
            split = jnp.concatenate([high, update - high], axis=0).astype(bf16)
            grow = lax.dot_general(
                kd_ref[at], split, (((0,), (0,)), ((), ())), preferred_element_type=f32
            )
            grow_0, grow_1 = grow[:state_rows], grow[state_rows:]
            crossed = pltpu.roll(jnp.where(even, grow_1, grow_0), HEAD_DIM, axis=1)
            added = jnp.where(kept, jnp.where(even, grow_0, grow_1), crossed)
            fade = dec_ref[at]
            fade_turned = pltpu.roll(fade, HEAD_DIM, axis=1)
            copies = state_rows // steps
            factor = jnp.where(
                kept,
                jnp.concatenate([fade] * copies, axis=0),
                jnp.concatenate([fade_turned] * copies, axis=0),
            )
            new_ref[slot, at] = factor * state + added
            return carry

        lax.fori_loop(0, seqs, one_sequence, 0, unroll=8)

    def read_out(item, layer):
        update = u_ref[...]
        output = grown_ref[...] * qs_ref[...]
        for at in range(steps):
            output = output + qk_ref[at] * update[:, at : at + 1, :]
        output = output.reshape(rows, LANES)
        sums = head_sums(output * output, ones_ref[:LANES, :LANES])
        output = output * lax.rsqrt(sums * (1.0 / HEAD_DIM) + EPS)
        gain = read_gain_ref[pl.ds(layer, 1), :]
        y_ref[item, me] = (output * gain * jax.nn.silu(cols(3))).astype(bf16)

    def emit(item):
        whole = jnp.concatenate([y_ref[item, origin] for origin in range(count)], axis=1)
        return bf16_dot(whole, wo_ref[item // chunks]).astype(bf16)

    def emit_middle(item):
        in_ref[item + chunks, me] = emit(item)

    def emit_last(item):
        mixed = emit(item)
        chunk = item - chunks
        mown_ref[chunk] = mixed
        wide = mixed.astype(f32)
        total = jnp.sum(squares(wide), axis=1, keepdims=True)
        sq_ref[chunk, me] = jnp.broadcast_to(total, (rows, LANES)).T[:8]

    def sums_begin(chunk):
        block = sq_ref.at[chunk, me]
        for step in range(1, count):
            remote(
                block, block, sq_sem.at[0, chunk], sq_sem.at[1, chunk], lax.rem(me + step, count)
            ).start()

    def sums_all(chunk):
        part = sq_ref.at[chunk, pl.ds(0, count - 1)]
        return remote(part, part, sq_sem.at[0, chunk], sq_sem.at[1, chunk], twin)

    def finish(chunk):
        sums_all(chunk).wait_recv()
        total = sq_ref[chunk, 0]
        for origin in range(1, count):
            total = total + sq_ref[chunk, origin]
        total = jnp.broadcast_to(total[0:1, :], (LANES, rows)).T
        scale = lax.rsqrt(total * (1.0 / D) + EPS)
        for half in range(width // LANES):
            at = pl.ds(half * LANES, LANES)
            gain = post_gain_ref[1:2, pl.ds(pl.multiple_of(me * width + half * LANES, LANES), LANES)]
            before = xown_ref[chunk, :, at].astype(f32)
            mixed = mown_ref[chunk, :, at].astype(f32)
            out_ref[pl.ds(chunk * rows, rows), at] = (before + mixed * scale * gain).astype(bf16)

    lag = 3

    def slot_of(item, carry):
        layer, chunk, slot = item // chunks, lax.rem(item, chunks), lax.rem(item, 2)

        @pl.when(item + 1 < items)
        def _():
            state_load(item + 1).start()

        @pl.when(item + 2 < chunks)
        def _():
            begin_x(item + 2)

        complete(in_ref, in_sem, item)

        @pl.when(layer == 0)
        def _():
            own_copy(item).wait()
            first_hidden(item)

        @pl.when(layer == 1)
        def _():
            second_hidden(item)

        hidden = h_ref[...]
        proj_ref[...] = bf16_dot(hidden, w_ref[layer]).astype(bf16)
        rate_ref[...] = lax.dot_general(
            hidden, rates_ref[layer], (((1,), (1,)), ((), ())), preferred_element_type=f32
        ).astype(bf16)

        @pl.when(item >= 1)
        def _():
            relay_over(y_ref, y_sem, item - 1)

        prepare(layer, chunk)

        @pl.when(item + 1 < chunks)
        def _():
            relay_over(in_ref, in_sem, item + 1)

        @pl.when((item >= lag) & (item < lag + chunks))
        def _():
            relay_over(in_ref, in_sem, item + chunks - lag)

        state_load(item).wait()

        @pl.when(item >= 2)
        def _():
            state_store(item - 2).wait()

        advance(slot)

        @pl.when(item >= 1)
        def _():
            relay_twin(y_ref, y_sem, item - 1)

        read_out(item, layer)
        state_store(item).start()

        @pl.when(item >= 1)
        def _():
            complete(y_ref, y_sem, item - 1)

        begin(y_ref, y_sem, item, y_ref.at[item, me])

        @pl.when((item >= 1) & (item <= chunks))
        def _():
            emit_middle(item - 1)

        @pl.when(item > chunks)
        def _():
            emit_last(item - 1)

        @pl.when(item + 1 < chunks)
        def _():
            relay_twin(in_ref, in_sem, item + 1)

        @pl.when((item >= lag) & (item < lag + chunks))
        def _():
            relay_twin(in_ref, in_sem, item + chunks - lag)

        @pl.when((item >= 1) & (item <= chunks))
        def _():
            begin(in_ref, in_sem, item + chunks - 1, in_ref.at[item + chunks - 1, me])

        @pl.when(item > chunks)
        def _():
            sums_begin(item - 1 - chunks)

        return carry

    lax.fori_loop(0, items, slot_of, 0)
    final = items - 1
    relay_over(y_ref, y_sem, final)
    for chunk in range(chunks - 1):
        finish(chunk)
    relay_twin(y_ref, y_sem, final)
    state_store(final - 1).wait()
    state_store(final).wait()
    complete(y_ref, y_sem, final)
    emit_last(final)
    for item in range(items):
        drained(in_ref, in_sem, item)
        drained(y_ref, y_sem, item)
    sums_begin(chunks - 1)
    finish(chunks - 1)
    for chunk in range(chunks):
        sums_all(chunk).wait_send()


def local_two_heads(
    residual_channel,
    prior_block_multiplier,
    probe_map_matrix,
    lookup_map_matrix,
    content_map_matrix,
    emission_valve_matrix,
    forgetting_map_matrix,
    insertion_rate_matrix,
    forgetting_magnitude_exponent,
    channel_forgetting_offset,
    surplus_forgetting_amounts,
    readout_rescale_multiplier,
    emission_map_matrix,
    post_mixing_multiplier,
    recurrent_matrices,
):
    batch_total, steps, own_width = residual_channel.shape
    layers, _, head_count, state_size = recurrent_matrices.shape
    row_count = batch_total * steps
    count = lax.axis_size("tp")
    groups = state_size // LANES
    chunks = CHUNKS
    seqs, rows = batch_total // chunks, row_count // chunks
    heads = forgetting_map_matrix.shape[2]
    features = forgetting_map_matrix.shape[1]
    mix_width = emission_map_matrix.shape[1]
    states = (
        recurrent_matrices.reshape(layers, batch_total, head_count, groups, LANES)
        .transpose(0, 1, 3, 2, 4)
        .reshape(layers, batch_total, groups * head_count, LANES)
    )
    f32, bf16 = jnp.float32, jnp.bfloat16
    dma = pltpu.SemaphoreType.DMA
    hbm = pl.BlockSpec(memory_space=pl.ANY)
    vmem = pl.BlockSpec(memory_space=pltpu.VMEM)
    smem = pl.BlockSpec(memory_space=pltpu.SMEM)
    tile = (seqs, steps, LANES)
    state_tile = (2, seqs, groups * head_count, LANES)
    current, new_memory = pl.pallas_call(
        lambda *refs: step_kernel(count, chunks, *refs),
        out_shape=[
            jax.ShapeDtypeStruct((row_count, own_width), bf16),
            jax.ShapeDtypeStruct(states.shape, f32),
        ],
        in_specs=[hbm] * 9 + [vmem] * 4 + [smem] * 2,
        out_specs=[vmem, hbm],
        scratch_shapes=[
            pltpu.VMEM((2 * chunks, count, rows, own_width), bf16),
            pltpu.VMEM((2 * chunks, count, rows, LANES), bf16),
            pltpu.VMEM((layers, features, 4 * LANES), bf16),
            pltpu.VMEM((layers, mix_width, own_width), bf16),
            pltpu.VMEM((layers, 2 * heads, features), bf16),
            pltpu.VMEM((rows, features), bf16),
            pltpu.VMEM((count, rows, own_width), bf16),
            pltpu.VMEM((chunks, rows, own_width), bf16),
            pltpu.VMEM((chunks, rows, own_width), bf16),
            pltpu.VMEM((chunks, count, 8, rows), f32),
            pltpu.VMEM((layers, batch_total, steps, LANES), f32),
            pltpu.VMEM(state_tile, f32),
            pltpu.VMEM(state_tile, f32),
            pltpu.VMEM((rows, 4 * LANES), bf16),
            pltpu.VMEM((rows, 2 * heads), bf16),
            pltpu.VMEM(tile, f32),
            pltpu.VMEM((steps,) + tile, f32),
            pltpu.VMEM((seqs, 2 * steps, LANES), bf16),
            pltpu.VMEM((seqs, 2 * steps, LANES), bf16),
            pltpu.VMEM(tile, f32),
            pltpu.VMEM(tile, f32),
            pltpu.VMEM(tile, f32),
            pltpu.VMEM((2 * heads, 2 * LANES), bf16),
            pltpu.VMEM((2 * LANES, 2 * LANES), bf16),
            pltpu.VMEM((LANES, LANES), bf16),
            dma((14,)),
            dma((2, 2)),
            dma((chunks,)),
            dma((4, 2 * chunks)),
            dma((4, 2 * chunks)),
            dma((2, chunks)),
        ],
        compiler_params=pltpu.CompilerParams(
            collective_id=1, has_side_effects=True, vmem_limit_bytes=62 * 1024 * 1024
        ),
        name="step",
    )(
        residual_channel.reshape(row_count, own_width),
        probe_map_matrix,
        lookup_map_matrix,
        content_map_matrix,
        emission_valve_matrix,
        forgetting_map_matrix.transpose(0, 2, 1),
        insertion_rate_matrix.transpose(0, 2, 1),
        emission_map_matrix,
        states,
        surplus_forgetting_amounts.transpose(0, 2, 3, 1),
        prior_block_multiplier,
        post_mixing_multiplier,
        readout_rescale_multiplier,
        forgetting_magnitude_exponent,
        channel_forgetting_offset,
    )
    new_memory = (
        new_memory.reshape(layers, batch_total, groups, head_count, LANES)
        .transpose(0, 1, 3, 2, 4)
        .reshape(recurrent_matrices.shape)
    )
    return current.reshape(batch_total, steps, own_width), new_memory


def local_any(*arrays):
    residual_channel, recurrent_matrices = arrays[0], arrays[-1]
    two_heads = (
        recurrent_matrices.shape[2] * HEAD_DIM == LANES
        and residual_channel.shape[1] == 8
        and residual_channel.shape[0] % (8 * CHUNKS) == 0
        and residual_channel.shape[2] % LANES == 0
        and lax.axis_size("tp") % 4 == 0
        and lax.axis_size("tp") > 4
    )
    return (local_two_heads if two_heads else local)(*arrays)


def solution(mesh):
    return jax.shard_map(
        local_any,
        mesh=mesh,
        in_specs=(
            P("grp", None, "tp"),
            P(),
            P(None, None, "tp"),
            P(None, None, "tp"),
            P(None, None, "tp"),
            P(None, None, "tp"),
            P(),
            P(),
            P(None, "tp"),
            P(None, "tp"),
            P(None, "grp", None, "tp"),
            P(None, "tp"),
            P(None, None, "tp"),
            P(),
            P(None, "grp", "tp", None),
        ),
        out_specs=(P("grp", None, "tp"), P(None, "grp", "tp", None)),
        check_vma=False,
    )
```

```python
import jax
import jax.numpy as jnp
from jax import lax
from jax.experimental import pallas as pl
from jax.experimental.pallas import tpu as pltpu
from jax.sharding import PartitionSpec as P

D = 4096
HEAD_DIM = 64
LAYERS = 2


EPS = 1e-06
HIGH = lax.Precision.HIGHEST


def solve_lower(a_mat, right_side):
    length = right_side.shape[-2]
    solved_rows = []
    for row_at in range(length):
        current_row = right_side[..., row_at, :]
        for col_at in range(row_at):
            current_row = current_row - a_mat[..., row_at, col_at][..., None] * solved_rows[col_at]
        solved_rows.append(current_row)
    return jnp.stack(solved_rows, axis=-2)


def delta_block(queries, key_rows, values, forgetting_exponent_amount, strength, matrix_state):
    length = queries.shape[2]
    causal = jnp.tril(jnp.ones((length, length), bool))
    strict = jnp.tril(jnp.ones((length, length), bool), -1)
    cumulative = jnp.cumsum(forgetting_exponent_amount, axis=-1)
    decay_mat = jnp.where(
        causal,
        jnp.exp(jnp.where(causal, cumulative[..., :, None] - cumulative[..., None, :], 0.0)),
        0.0,
    )
    key_gram = jnp.einsum("bhtd,bhsd->bhts", key_rows, key_rows, precision=HIGH)
    a_mat = jnp.where(strict, strength[..., :, None] * decay_mat * key_gram, 0.0)
    right_side = jnp.concatenate(
        [strength[..., None] * values, (strength * jnp.exp(cumulative))[..., None] * key_rows],
        axis=-1,
    )
    solved = solve_lower(a_mat, right_side)
    width_v = values.shape[-1]
    update = solved[..., :width_v] - jnp.einsum(
        "bhtk,bhkv->bhtv", solved[..., width_v:], matrix_state, precision=HIGH
    )
    scores = jnp.einsum("bhtd,bhsd->bhts", queries, key_rows, precision=HIGH) * decay_mat
    output = jnp.exp(cumulative)[..., None] * jnp.einsum(
        "bhtk,bhkv->bhtv", queries, matrix_state, precision=HIGH
    )
    output = output + jnp.einsum("bhts,bhsv->bhtv", scores, update, precision=HIGH)
    final_log = cumulative[..., -1:]
    revised_memory_matrix = jnp.exp(final_log)[..., None] * matrix_state + jnp.einsum(
        "bhsk,bhsv->bhkv",
        key_rows * jnp.exp(final_log - cumulative)[..., None],
        update,
        precision=HIGH,
    )
    return (output, revised_memory_matrix)


def unit_rows(matrix):
    return matrix * lax.rsqrt(jnp.sum(matrix * matrix, axis=-1, keepdims=True) + EPS)


def token_blender(
    mapped_token_vectors,
    magnitude_exponent,
    offset_terms_array,
    surplus_forgetting_exponent,
    multiplier_terms_array,
    incoming_memory_matrix,
    batch_total,
    generation_round_total,
):
    rounded = [
        lax.optimization_barrier(part_sum.astype(jnp.bfloat16)).astype(jnp.float32)
        for part_sum in mapped_token_vectors
    ]
    queries, keys_raw, values_raw, gate_raw, decay_pre, strength_pre = rounded
    head_count = incoming_memory_matrix.shape[1]

    def to_heads(matrix):
        return matrix.reshape(batch_total, generation_round_total, head_count, HEAD_DIM).transpose(
            0, 2, 1, 3
        )

    def per_head(matrix):
        return matrix.reshape(batch_total, generation_round_total, head_count).transpose(0, 2, 1)

    queries = unit_rows(jax.nn.silu(to_heads(queries))) * HEAD_DIM ** (-0.5)
    key_rows = unit_rows(jax.nn.silu(to_heads(keys_raw)))
    values = jax.nn.silu(to_heads(values_raw))
    forgetting_exponent_amount = -jnp.exp(magnitude_exponent)[None, :, None] * jax.nn.softplus(
        per_head(decay_pre) + offset_terms_array[None, :, None]
    )
    forgetting_exponent_amount = forgetting_exponent_amount + surplus_forgetting_exponent.transpose(
        0, 2, 1
    )
    strength = jax.nn.sigmoid(per_head(strength_pre))
    matrix_state = incoming_memory_matrix.reshape(batch_total, head_count, HEAD_DIM, HEAD_DIM)
    output, revised_memory_matrix = delta_block(
        queries, key_rows, values, forgetting_exponent_amount, strength, matrix_state
    )
    normed = output * lax.rsqrt(jnp.mean(output * output, axis=-1, keepdims=True) + EPS)
    normed = (
        normed
        * multiplier_terms_array.reshape(head_count, HEAD_DIM)[None, :, None, :]
        * jax.nn.silu(to_heads(gate_raw))
    )
    blended_token_vectors = (
        normed.transpose(0, 2, 1, 3)
        .reshape(batch_total * generation_round_total, head_count * HEAD_DIM)
        .astype(jnp.bfloat16)
    )
    return (
        blended_token_vectors,
        revised_memory_matrix.reshape(batch_total, head_count, HEAD_DIM * HEAD_DIM),
    )


LANES = 128


def bf16_dot(left, right):
    return jnp.dot(left, right, preferred_element_type=jnp.float32)


def head_sums(squares, ones):
    high = squares.astype(jnp.bfloat16)
    low = (squares - high.astype(jnp.float32)).astype(jnp.bfloat16)
    return bf16_dot(high, ones) + bf16_dot(low, ones)


def project(portion, weights):
    return tuple(
        (jnp.dot(portion, weight, preferred_element_type=jnp.float32) for weight in weights)
    )


def out_project(blended_token_vectors, weight_rows):
    return jnp.dot(
        lax.all_gather(blended_token_vectors, "tp", axis=1, tiled=True),
        weight_rows,
        preferred_element_type=jnp.float32,
    ).astype(jnp.bfloat16)


def post_residual(widened, mixed_out, multiplier_terms_array, complete):
    mixed_wide = lax.optimization_barrier(mixed_out).astype(jnp.float32)
    squares = jnp.sum(mixed_wide * mixed_wide, axis=-1)
    if not complete:
        squares = lax.psum(squares, "tp")
    post_rms = lax.rsqrt(squares / D + EPS)[:, None]
    return lax.optimization_barrier(
        (widened + mixed_wide * post_rms * multiplier_terms_array).astype(jnp.bfloat16)
    )


def local(
    residual_channel,
    prior_block_multiplier,
    probe_map_matrix,
    lookup_map_matrix,
    content_map_matrix,
    emission_valve_matrix,
    forgetting_map_matrix,
    insertion_rate_matrix,
    forgetting_magnitude_exponent,
    channel_forgetting_offset,
    surplus_forgetting_amounts,
    readout_rescale_multiplier,
    emission_map_matrix,
    post_mixing_multiplier,
    recurrent_matrices,
):
    batch_total, generation_round_total, own_width = residual_channel.shape
    head_count = recurrent_matrices.shape[2]
    row_count = batch_total * generation_round_total
    col_offset = lax.axis_index("tp") * own_width
    head_offset = lax.axis_index("tp") * head_count
    new_states = []

    def mix_layer(mapped_token_vectors, block_index_number):
        blended_token_vectors, revised_memory_matrix = token_blender(
            mapped_token_vectors,
            forgetting_magnitude_exponent[block_index_number],
            channel_forgetting_offset[block_index_number],
            surplus_forgetting_amounts[block_index_number],
            readout_rescale_multiplier[block_index_number],
            recurrent_matrices[block_index_number],
            batch_total,
            generation_round_total,
        )
        new_states.append(revised_memory_matrix)
        return out_project(blended_token_vectors, emission_map_matrix[block_index_number])

    def own_cols(matrix):
        return lax.dynamic_slice_in_dim(matrix, col_offset, own_width, matrix.ndim - 1)

    whole_rows = lax.all_gather(
        residual_channel.reshape(row_count, own_width), "tp", axis=1, tiled=True
    )
    current = whole_rows
    for block_index_number in range(LAYERS):
        widened = whole_rows.astype(jnp.float32)
        inv_rms = lax.rsqrt(jnp.mean(widened * widened, axis=-1, keepdims=True) + EPS)
        hidden = (widened * inv_rms * prior_block_multiplier[block_index_number]).astype(
            jnp.bfloat16
        )
        weights = (
            probe_map_matrix[block_index_number],
            lookup_map_matrix[block_index_number],
            content_map_matrix[block_index_number],
            emission_valve_matrix[block_index_number],
            lax.dynamic_slice_in_dim(
                forgetting_map_matrix[block_index_number], head_offset, head_count, 1
            ),
            lax.dynamic_slice_in_dim(
                insertion_rate_matrix[block_index_number], head_offset, head_count, 1
            ),
        )
        mapped_token_vectors = project(hidden, weights)
        mixed_out = mix_layer(mapped_token_vectors, block_index_number)
        if block_index_number < LAYERS - 1:
            gathered = lax.all_gather(mixed_out, "tp", axis=1, tiled=True)
            whole_rows = post_residual(
                widened, gathered, post_mixing_multiplier[block_index_number], True
            )
        else:
            current = post_residual(
                own_cols(widened),
                mixed_out,
                own_cols(post_mixing_multiplier[block_index_number]),
                False,
            )
    return (
        current.reshape(batch_total, generation_round_total, own_width),
        jnp.stack(new_states, axis=0),
    )


CHUNKS = 8
GROUP_ROWS = 64


def step_kernel(
    count,
    chunks,
    x_hbm,
    probe_hbm,
    lookup_hbm,
    content_hbm,
    valve_hbm,
    forget_hbm,
    insert_hbm,
    emission_hbm,
    states_hbm,
    surplus_hbm,
    pre_gain_hbm,
    post_gain_hbm,
    read_gain_hbm,
    magnitude_hbm,
    offset_hbm,
    out_ref,
    new_hbm,
    in_ref,
    y_ref,
    w_ref,
    wo_ref,
    rates_ref,
    h_ref,
    x1_ref,
    xown_ref,
    mown_ref,
    sq_ref,
    sur_ref,
    state_ref,
    new_ref,
    proj_ref,
    grown_ref,
    qk_ref,
    xq_ref,
    kd_ref,
    u_ref,
    qs_ref,
    dec_ref,
    spread_ref,
    ones_ref,
    perm_ref,
    surplus_ref,
    pre_gain_ref,
    post_gain_ref,
    read_gain_ref,
    magnitude_ref,
    offset_ref,
    load_sem,
    state_sem,
    own_sem,
    in_sem,
    y_sem,
    sq_sem,
):
    f32, bf16 = jnp.float32, jnp.bfloat16
    me = lax.axis_index("tp")
    depth = count // 4
    core, row, line = lax.rem(me, 2), lax.rem(me // 2, 2), me // 4
    over, twin = me + 2 - 4 * row, me + 1 - 2 * core
    items = 2 * chunks
    rows = h_ref.shape[0]
    seqs, steps = qk_ref.shape[1], qk_ref.shape[2]
    width = in_ref.shape[3]
    heads = forget_hbm.shape[1]
    own_heads = heads // count

    barrier = pltpu.get_barrier_semaphore()
    for step in range(1, count):
        pl.semaphore_signal(
            barrier,
            inc=1,
            device_id={"tp": lax.rem(me + step, count)},
            device_id_type=pl.DeviceIdType.MESH,
        )

    loads = []
    for layer in range(2):
        for at, matrix in enumerate((probe_hbm, lookup_hbm, content_hbm, valve_hbm)):
            loads.append(
                (matrix.at[layer], w_ref.at[layer, :, pl.ds(at * LANES, LANES)])
            )
        loads.append((forget_hbm.at[layer], rates_ref.at[layer, pl.ds(0, heads), :]))
        loads.append((insert_hbm.at[layer], rates_ref.at[layer, pl.ds(heads, heads), :]))
        loads.append((emission_hbm.at[layer], wo_ref.at[layer]))
    loads += [
        (surplus_hbm, surplus_ref),
        (pre_gain_hbm, pre_gain_ref),
        (post_gain_hbm, post_gain_ref),
        (read_gain_hbm, read_gain_ref),
        (magnitude_hbm, magnitude_ref),
        (offset_hbm, offset_ref),
    ]
    loads = [
        pltpu.make_async_copy(source, target, load_sem.at[at])
        for at, (source, target) in enumerate(loads)
    ]
    for copy in loads:
        copy.start()

    def state_load(item):
        return pltpu.make_async_copy(
            states_hbm.at[item // chunks, pl.ds(lax.rem(item, chunks) * seqs, seqs)],
            state_ref.at[lax.rem(item, 2)],
            state_sem.at[0, lax.rem(item, 2)],
        )

    def state_store(item):
        return pltpu.make_async_copy(
            new_ref.at[lax.rem(item, 2)],
            new_hbm.at[item // chunks, pl.ds(lax.rem(item, chunks) * seqs, seqs)],
            state_sem.at[1, lax.rem(item, 2)],
        )

    state_load(0).start()

    pl.semaphore_wait(barrier, count - 1)

    def remote(source, target, send_sem, land_sem, device):
        return pltpu.make_async_remote_copy(
            src_ref=source,
            dst_ref=target,
            send_sem=send_sem,
            recv_sem=land_sem,
            device_id={"tp": device},
            device_id_type=pl.DeviceIdType.MESH,
        )

    def along(step):
        return 4 * (lax.rem(line + step, depth) - line)

    def begin(buf, sems, item, source):
        for step in range(1, depth):
            remote(
                source, buf.at[item, me], sems.at[0, item], sems.at[1, item], me + along(step)
            ).start()
        remote(source, buf.at[item, me], sems.at[0, item], sems.at[1, item], over).start()
        remote(source, buf.at[item, me], sems.at[0, item], sems.at[3, item], twin).start()

    def pass_on(buf, sems, item, origin, kind, device):
        block = buf.at[item, origin]
        remote(block, block, sems.at[0, item], sems.at[kind, item], device).start()

    def landed(buf, sems, item, kind, blocks):
        part = buf.at[item, pl.ds(0, blocks)]
        remote(part, part, sems.at[0, item], sems.at[kind, item], twin).wait_recv()

    def relay_over(buf, sems, item):
        landed(buf, sems, item, 1, depth)
        for step in range(1, depth):
            pass_on(buf, sems, item, me + along(depth - step), 2, over)
        for step in range(1, depth):
            pass_on(buf, sems, item, me + along(depth - step), 3, twin)
        pass_on(buf, sems, item, over, 3, twin)

    def relay_twin(buf, sems, item):
        landed(buf, sems, item, 2, depth - 1)
        for step in range(1, depth):
            pass_on(buf, sems, item, over + along(depth - step), 3, twin)

    def complete(buf, sems, item):
        landed(buf, sems, item, 3, 2 * depth)

    def drained(buf, sems, item):
        blocks = (depth + 1) + (2 * depth - 1) + (depth - 1)
        part = buf.at[item, pl.ds(0, blocks)]
        remote(part, part, sems.at[0, item], sems.at[1, item], twin).wait_send()

    def own_copy(item):
        return pltpu.make_async_copy(
            x_hbm.at[pl.ds(item * rows, rows), :], in_ref.at[item, me], own_sem.at[item]
        )

    def begin_x(item):
        begin(in_ref, in_sem, item, x_hbm.at[pl.ds(item * rows, rows), :])
        own_copy(item).start()

    for item in range(3):
        begin_x(item)

    def iota(shape, axis):
        return lax.broadcasted_iota(jnp.int32, shape, axis)

    shape = (2 * heads, 2 * LANES)
    wanted = iota(shape, 1) // HEAD_DIM
    wanted = jnp.where(wanted >= 2, wanted - 2 + heads, wanted) + me * own_heads
    spread_ref[...] = jnp.where(iota(shape, 0) == wanted, 1.0, 0.0).astype(bf16)
    shape = (2 * LANES, 2 * LANES)
    ones_ref[...] = jnp.where(
        iota(shape, 0) // HEAD_DIM == iota(shape, 1) // HEAD_DIM, 1.0, 0.0
    ).astype(bf16)
    shape = (LANES, LANES)
    head, channel = iota(shape, 0) // HEAD_DIM, iota(shape, 0) % HEAD_DIM
    target = (channel % 2) * HEAD_DIM + (channel // 2) * 2 + head
    perm_ref[...] = jnp.where(target == iota(shape, 1), 1.0, 0.0).astype(bf16)
    for copy in loads:
        copy.wait()
    all_seqs = sur_ref.shape[1]
    first_head = iota((LANES, all_seqs), 0) < HEAD_DIM
    for layer in range(2):
        for step in range(steps):
            pair = surplus_ref[layer, step]
            wide = jnp.where(first_head, pair[0:1, :], pair[1:2, :])
            sur_ref[layer, :, step, :] = wide.T
        for origin in range(count):
            at = pl.ds(origin * width, width)
            pair = rates_ref[layer, :, at].astype(f32)
            filled = jnp.concatenate([pair, jnp.zeros((LANES - 2 * heads, width), f32)], axis=0)
            w_ref[layer, at, pl.ds(4 * LANES, LANES)] = filled.T.astype(bf16)

    relay_over(in_ref, in_sem, 0)
    relay_twin(in_ref, in_sem, 0)
    relay_over(in_ref, in_sem, 1)

    def squares(matrix):
        return matrix[:, :LANES] * matrix[:, :LANES] + matrix[:, LANES:] * matrix[:, LANES:]

    def inverse(total):
        return lax.rsqrt(jnp.sum(total, axis=1, keepdims=True) * (1.0 / D) + EPS)

    def cols_of(origin):
        return pl.ds(origin * width, width)

    def first_hidden(item):
        def part(group, carry):
            at = pl.ds(group * GROUP_ROWS, GROUP_ROWS)
            total = jnp.zeros((GROUP_ROWS, LANES), f32)
            for origin in range(count):
                total = total + squares(in_ref[item, origin, at, :].astype(f32))
            scale = inverse(total)
            for origin in range(count):
                block = in_ref[item, origin, at, :].astype(f32)
                gain = pre_gain_ref[0:1, cols_of(origin)]
                h_ref[at, cols_of(origin)] = (block * scale * gain).astype(bf16)
            return carry

        lax.fori_loop(0, rows // GROUP_ROWS, part, 0)

    def second_hidden(item):
        earlier = item - chunks

        def part(group, carry):
            at = pl.ds(group * GROUP_ROWS, GROUP_ROWS)
            total = jnp.zeros((GROUP_ROWS, LANES), f32)
            for origin in range(count):
                total = total + squares(in_ref[item, origin, at, :].astype(f32))
            scale = inverse(total)
            total = jnp.zeros((GROUP_ROWS, LANES), f32)
            for origin in range(count):
                mixed = in_ref[item, origin, at, :].astype(f32)
                before = in_ref[earlier, origin, at, :].astype(f32)
                gain = post_gain_ref[0:1, cols_of(origin)]
                after = (before + mixed * scale * gain).astype(bf16)
                x1_ref[origin, at, :] = after
                total = total + squares(after.astype(f32))
            scale = inverse(total)
            for origin in range(count):
                block = x1_ref[origin, at, :].astype(f32)
                gain = pre_gain_ref[1:2, cols_of(origin)]
                h_ref[at, cols_of(origin)] = (block * scale * gain).astype(bf16)
            xown_ref[earlier, at, :] = x1_ref[me, at, :]
            return carry

        lax.fori_loop(0, rows // GROUP_ROWS, part, 0)

    def cols(at):
        return proj_ref[:, at * LANES : (at + 1) * LANES].astype(f32)

    def tokens(matrix):
        return matrix.reshape(seqs, steps, LANES)

    def lane_pair(ref, layer):
        left = iota((1, LANES), 1) < HEAD_DIM
        return jnp.where(left, ref[layer, 0], ref[layer, 1])

    def prepare(layer, chunk):
        ones = ones_ref[...]
        perm = perm_ref[...]
        queries = jax.nn.silu(cols(0))
        keys = jax.nn.silu(cols(1))
        sums = head_sums(jnp.concatenate([queries * queries, keys * keys], axis=1), ones)
        queries = tokens(queries * lax.rsqrt(sums[:, :LANES] + EPS) * HEAD_DIM ** (-0.5))
        keys = tokens(keys * lax.rsqrt(sums[:, LANES:] + EPS))
        spread = bf16_dot(proj_ref[:, 4 * LANES : 4 * LANES + 2 * heads], spread_ref[...])
        biased = spread[:, :LANES] + lane_pair(offset_ref, layer)
        softplus = jnp.maximum(biased, 0.0) + jnp.log1p(jnp.exp(-jnp.abs(biased)))
        pace = -jnp.exp(lane_pair(magnitude_ref, layer))
        cumulative = tokens(pace * softplus) + sur_ref[layer, pl.ds(chunk * seqs, seqs)]
        beta = tokens(jax.nn.sigmoid(spread[:, LANES:]))
        token = lax.broadcasted_iota(jnp.int32, (seqs, steps, LANES), 1)
        shift = 1
        while shift < steps:
            moved = pltpu.roll(cumulative, shift, axis=1)
            cumulative = cumulative + jnp.where(token >= shift, moved, 0.0)
            shift *= 2
        grown = jnp.exp(cumulative)
        grown_ref[...] = grown
        solved_u = beta * tokens(jax.nn.silu(cols(2)))
        solved_p = beta * grown * keys
        for at in range(steps):
            causal = token >= at
            gap = jnp.where(causal, cumulative - cumulative[:, at : at + 1, :], 0.0)
            decay = jnp.where(causal, jnp.exp(gap), 0.0)
            key_row = keys[:, at : at + 1, :]
            pair = jnp.concatenate([queries * key_row, keys * key_row], axis=2)
            dots = bf16_dot(pair.reshape(rows, 2 * LANES).astype(bf16), ones)
            qk_ref[at] = tokens(dots[:, :LANES]) * decay
            if at < steps - 1:
                a_col = jnp.where(token > at, beta * decay * tokens(dots[:, LANES:]), 0.0)
                solved_u = solved_u - a_col * solved_u[:, at : at + 1, :]
                solved_p = solved_p - a_col * solved_p[:, at : at + 1, :]
        last = cumulative[:, steps - 1 : steps, :]
        faded = keys * jnp.exp(last - cumulative)

        def permuted(first, second):
            both = jnp.concatenate([first, second], axis=1).reshape(2 * rows, LANES)
            return bf16_dot(both.astype(bf16), perm).astype(bf16).reshape(seqs, 2 * steps, LANES)

        xq_ref[...] = permuted(queries, solved_p)
        kd_ref[...] = permuted(faded, faded)
        u_ref[...] = solved_u
        dec_ref[...] = jnp.broadcast_to(jnp.exp(last), (seqs, steps, LANES))

    state_rows = state_ref.shape[2]

    def advance(slot):
        even = iota((state_rows, LANES), 0) % 2 == 0
        left = iota((state_rows, LANES), 1) < HEAD_DIM
        kept = even == left

        def one_sequence(at, carry):
            state = state_ref[slot, at]
            turned = pltpu.roll(state, HEAD_DIM, axis=1)
            upper = jnp.where(kept, jnp.where(even, state, turned), 0.0)
            lower = jnp.where(kept, jnp.where(even, turned, state), 0.0)
            wide = jnp.concatenate([upper, lower], axis=0).astype(bf16)
            read = bf16_dot(xq_ref[at], wide)
            qs_ref[at] = read[:steps]
            update = u_ref[at] - read[steps:]
            u_ref[at] = update
            high = update.astype(bf16).astype(f32)
            split = jnp.concatenate([high, update - high], axis=0).astype(bf16)
            grow = lax.dot_general(
                kd_ref[at], split, (((0,), (0,)), ((), ())), preferred_element_type=f32
            )
            grow_0, grow_1 = grow[:state_rows], grow[state_rows:]
            crossed = pltpu.roll(jnp.where(even, grow_1, grow_0), HEAD_DIM, axis=1)
            added = jnp.where(kept, jnp.where(even, grow_0, grow_1), crossed)
            fade = dec_ref[at]
            fade_turned = pltpu.roll(fade, HEAD_DIM, axis=1)
            copies = state_rows // steps
            factor = jnp.where(
                kept,
                jnp.concatenate([fade] * copies, axis=0),
                jnp.concatenate([fade_turned] * copies, axis=0),
            )
            new_ref[slot, at] = factor * state + added
            return carry

        lax.fori_loop(0, seqs, one_sequence, 0, unroll=8)

    def read_out(item, layer):
        update = u_ref[...]
        output = grown_ref[...] * qs_ref[...]
        for at in range(steps):
            output = output + qk_ref[at] * update[:, at : at + 1, :]
        output = output.reshape(rows, LANES)
        sums = head_sums(output * output, ones_ref[:LANES, :LANES])
        output = output * lax.rsqrt(sums * (1.0 / HEAD_DIM) + EPS)
        gain = read_gain_ref[pl.ds(layer, 1), :]
        y_ref[item, me] = (output * gain * jax.nn.silu(cols(3))).astype(bf16)

    def emit(item):
        whole = jnp.concatenate([y_ref[item, origin] for origin in range(count)], axis=1)
        return bf16_dot(whole, wo_ref[item // chunks]).astype(bf16)

    def emit_middle(item):
        in_ref[item + chunks, me] = emit(item)

    def emit_last(item):
        mixed = emit(item)
        chunk = item - chunks
        mown_ref[chunk] = mixed
        wide = mixed.astype(f32)
        total = jnp.sum(squares(wide), axis=1, keepdims=True)
        sq_ref[chunk, me] = jnp.broadcast_to(total, (rows, LANES)).T[:1]

    def sums_begin(chunk):
        block = sq_ref.at[chunk, me]
        for step in range(1, count):
            remote(
                block, block, sq_sem.at[0, chunk], sq_sem.at[1, chunk], lax.rem(me + step, count)
            ).start()

    def sums_all(chunk):
        part = sq_ref.at[chunk, pl.ds(0, count - 1)]
        return remote(part, part, sq_sem.at[0, chunk], sq_sem.at[1, chunk], twin)

    def finish(chunk):
        sums_all(chunk).wait_recv()
        total = sq_ref[chunk, 0]
        for origin in range(1, count):
            total = total + sq_ref[chunk, origin]
        total = jnp.broadcast_to(total, (LANES, rows)).T
        scale = lax.rsqrt(total * (1.0 / D) + EPS)
        for half in range(width // LANES):
            at = pl.ds(half * LANES, LANES)
            gain = post_gain_ref[1:2, pl.ds(pl.multiple_of(me * width + half * LANES, LANES), LANES)]
            before = xown_ref[chunk, :, at].astype(f32)
            mixed = mown_ref[chunk, :, at].astype(f32)
            out_ref[pl.ds(chunk * rows, rows), at] = (before + mixed * scale * gain).astype(bf16)

    def when(condition, action, *operands):
        @pl.when(condition)
        def _():
            action(*operands)

    def slot_of(item, carry):
        layer, chunk, slot = item // chunks, lax.rem(item, chunks), lax.rem(item, 2)
        when(item + 1 < items, lambda: state_load(item + 1).start())
        when(item + 3 < chunks, lambda: begin_x(item + 3))
        complete(in_ref, in_sem, item)

        @pl.when(layer == 0)
        def _():
            own_copy(item).wait()
            first_hidden(item)

        when(layer == 1, second_hidden, item)
        proj_ref[...] = bf16_dot(h_ref[...], w_ref[layer]).astype(bf16)

        when(item >= 2, relay_twin, y_ref, y_sem, item - 2)
        when((item >= 4) & (item < 4 + chunks), relay_over, in_ref, in_sem, item - 4 + chunks)
        when((item >= 5) & (item < 5 + chunks), relay_twin, in_ref, in_sem, item - 5 + chunks)
        when(item + 1 < chunks, relay_twin, in_ref, in_sem, item + 1)
        prepare(layer, chunk)
        state_load(item).wait()
        when(item >= 2, lambda: state_store(item - 2).wait())
        advance(slot)
        when(item >= 1, relay_over, y_ref, y_sem, item - 1)
        when(item + 2 < chunks, relay_over, in_ref, in_sem, item + 2)
        read_out(item, layer)
        state_store(item).start()
        when(item >= 2, complete, y_ref, y_sem, item - 2)
        begin(y_ref, y_sem, item, y_ref.at[item, me])
        early = (item >= 2) & (item < chunks + 2)
        when(early, emit_middle, item - 2)
        when(item >= chunks + 2, emit_last, item - 2)

        @pl.when(early)
        def _():
            made = item - 2 + chunks
            begin(in_ref, in_sem, made, in_ref.at[made, me])

        when(item >= chunks + 2, sums_begin, item - 2 - chunks)
        return carry

    lax.fori_loop(0, items, slot_of, 0)
    final = items - 1
    relay_twin(y_ref, y_sem, final - 1)
    for chunk in range(chunks - 3):
        finish(chunk)
    relay_over(y_ref, y_sem, final)
    complete(y_ref, y_sem, final - 1)
    emit_last(final - 1)
    finish(chunks - 3)
    relay_twin(y_ref, y_sem, final)
    sums_begin(chunks - 2)
    state_store(final - 1).wait()
    state_store(final).wait()
    for item in range(items):
        drained(in_ref, in_sem, item)
        if item < final:
            drained(y_ref, y_sem, item)
    complete(y_ref, y_sem, final)
    emit_last(final)
    drained(y_ref, y_sem, final)
    sums_begin(chunks - 1)
    finish(chunks - 2)
    finish(chunks - 1)
    for chunk in range(chunks):
        sums_all(chunk).wait_send()


def local_two_heads(
    residual_channel,
    prior_block_multiplier,
    probe_map_matrix,
    lookup_map_matrix,
    content_map_matrix,
    emission_valve_matrix,
    forgetting_map_matrix,
    insertion_rate_matrix,
    forgetting_magnitude_exponent,
    channel_forgetting_offset,
    surplus_forgetting_amounts,
    readout_rescale_multiplier,
    emission_map_matrix,
    post_mixing_multiplier,
    recurrent_matrices,
):
    batch_total, steps, own_width = residual_channel.shape
    layers, _, head_count, state_size = recurrent_matrices.shape
    row_count = batch_total * steps
    count = lax.axis_size("tp")
    groups = state_size // LANES
    chunks = CHUNKS
    seqs, rows = batch_total // chunks, row_count // chunks
    heads = forgetting_map_matrix.shape[2]
    features = forgetting_map_matrix.shape[1]
    mix_width = emission_map_matrix.shape[1]
    states = (
        recurrent_matrices.reshape(layers, batch_total, head_count, groups, LANES)
        .transpose(0, 1, 3, 2, 4)
        .reshape(layers, batch_total, groups * head_count, LANES)
    )
    f32, bf16 = jnp.float32, jnp.bfloat16
    dma = pltpu.SemaphoreType.DMA
    hbm = pl.BlockSpec(memory_space=pl.ANY)
    vmem = pl.BlockSpec(memory_space=pltpu.VMEM)
    tile = (seqs, steps, LANES)
    state_tile = (2, seqs, groups * head_count, LANES)
    current, new_memory = pl.pallas_call(
        lambda *refs: step_kernel(count, chunks, *refs),
        out_shape=[
            jax.ShapeDtypeStruct((row_count, own_width), bf16),
            jax.ShapeDtypeStruct(states.shape, f32),
        ],
        in_specs=[hbm] * 15,
        out_specs=[vmem, hbm],
        scratch_shapes=[
            pltpu.VMEM((2 * chunks, count, rows, own_width), bf16),
            pltpu.VMEM((2 * chunks, count, rows, LANES), bf16),
            pltpu.VMEM((layers, features, 5 * LANES), bf16),
            pltpu.VMEM((layers, mix_width, own_width), bf16),
            pltpu.VMEM((layers, 2 * heads, features), bf16),
            pltpu.VMEM((rows, features), bf16),
            pltpu.VMEM((count, rows, own_width), bf16),
            pltpu.VMEM((chunks, rows, own_width), bf16),
            pltpu.VMEM((chunks, rows, own_width), bf16),
            pltpu.VMEM((chunks, count, 1, rows), f32),
            pltpu.VMEM((layers, batch_total, steps, LANES), f32),
            pltpu.VMEM(state_tile, f32),
            pltpu.VMEM(state_tile, f32),
            pltpu.VMEM((rows, 5 * LANES), bf16),
            pltpu.VMEM(tile, f32),
            pltpu.VMEM((steps,) + tile, f32),
            pltpu.VMEM((seqs, 2 * steps, LANES), bf16),
            pltpu.VMEM((seqs, 2 * steps, LANES), bf16),
            pltpu.VMEM(tile, f32),
            pltpu.VMEM(tile, f32),
            pltpu.VMEM(tile, f32),
            pltpu.VMEM((2 * heads, 2 * LANES), bf16),
            pltpu.VMEM((2 * LANES, 2 * LANES), bf16),
            pltpu.VMEM((LANES, LANES), bf16),
            pltpu.VMEM((layers, steps, head_count, batch_total), f32),
            pltpu.VMEM((layers, features), f32),
            pltpu.VMEM((layers, features), f32),
            pltpu.VMEM((layers, LANES), f32),
            pltpu.SMEM((layers, head_count), f32),
            pltpu.SMEM((layers, head_count), f32),
            dma((20,)),
            dma((2, 2)),
            dma((chunks,)),
            dma((4, 2 * chunks)),
            dma((4, 2 * chunks)),
            dma((2, chunks)),
        ],
        compiler_params=pltpu.CompilerParams(
            collective_id=1, has_side_effects=True, vmem_limit_bytes=62 * 1024 * 1024
        ),
        name="step",
    )(
        residual_channel.reshape(row_count, own_width),
        probe_map_matrix,
        lookup_map_matrix,
        content_map_matrix,
        emission_valve_matrix,
        forgetting_map_matrix.transpose(0, 2, 1),
        insertion_rate_matrix.transpose(0, 2, 1),
        emission_map_matrix,
        states,
        surplus_forgetting_amounts.transpose(0, 2, 3, 1),
        prior_block_multiplier,
        post_mixing_multiplier,
        readout_rescale_multiplier,
        forgetting_magnitude_exponent,
        channel_forgetting_offset,
    )
    new_memory = (
        new_memory.reshape(layers, batch_total, groups, head_count, LANES)
        .transpose(0, 1, 3, 2, 4)
        .reshape(recurrent_matrices.shape)
    )
    return current.reshape(batch_total, steps, own_width), new_memory


def local_any(*arrays):
    residual_channel, recurrent_matrices = arrays[0], arrays[-1]
    two_heads = (
        recurrent_matrices.shape[2] * HEAD_DIM == LANES
        and residual_channel.shape[1] == 8
        and residual_channel.shape[0] % (8 * CHUNKS) == 0
        and residual_channel.shape[2] % LANES == 0
        and lax.axis_size("tp") % 4 == 0
        and lax.axis_size("tp") > 4
    )
    return (local_two_heads if two_heads else local)(*arrays)


def solution(mesh):
    return jax.shard_map(
        local_any,
        mesh=mesh,
        in_specs=(
            P("grp", None, "tp"),
            P(),
            P(None, None, "tp"),
            P(None, None, "tp"),
            P(None, None, "tp"),
            P(None, None, "tp"),
            P(),
            P(),
            P(None, "tp"),
            P(None, "tp"),
            P(None, "grp", None, "tp"),
            P(None, "tp"),
            P(None, None, "tp"),
            P(),
            P(None, "grp", "tp", None),
        ),
        out_specs=(P("grp", None, "tp"), P(None, "grp", "tp", None)),
        check_vma=False,
    )
```

```python
import jax
import jax.numpy as jnp
from jax import lax
from jax.experimental import pallas as pl
from jax.experimental.pallas import tpu as pltpu
from jax.sharding import PartitionSpec as P

D = 4096
HEAD_DIM = 64
LAYERS = 2


EPS = 1e-06
HIGH = lax.Precision.HIGHEST


def solve_lower(a_mat, right_side):
    length = right_side.shape[-2]
    solved_rows = []
    for row_at in range(length):
        current_row = right_side[..., row_at, :]
        for col_at in range(row_at):
            current_row = current_row - a_mat[..., row_at, col_at][..., None] * solved_rows[col_at]
        solved_rows.append(current_row)
    return jnp.stack(solved_rows, axis=-2)


def delta_block(queries, key_rows, values, forgetting_exponent_amount, strength, matrix_state):
    length = queries.shape[2]
    causal = jnp.tril(jnp.ones((length, length), bool))
    strict = jnp.tril(jnp.ones((length, length), bool), -1)
    cumulative = jnp.cumsum(forgetting_exponent_amount, axis=-1)
    decay_mat = jnp.where(
        causal,
        jnp.exp(jnp.where(causal, cumulative[..., :, None] - cumulative[..., None, :], 0.0)),
        0.0,
    )
    key_gram = jnp.einsum("bhtd,bhsd->bhts", key_rows, key_rows, precision=HIGH)
    a_mat = jnp.where(strict, strength[..., :, None] * decay_mat * key_gram, 0.0)
    right_side = jnp.concatenate(
        [strength[..., None] * values, (strength * jnp.exp(cumulative))[..., None] * key_rows],
        axis=-1,
    )
    solved = solve_lower(a_mat, right_side)
    width_v = values.shape[-1]
    update = solved[..., :width_v] - jnp.einsum(
        "bhtk,bhkv->bhtv", solved[..., width_v:], matrix_state, precision=HIGH
    )
    scores = jnp.einsum("bhtd,bhsd->bhts", queries, key_rows, precision=HIGH) * decay_mat
    output = jnp.exp(cumulative)[..., None] * jnp.einsum(
        "bhtk,bhkv->bhtv", queries, matrix_state, precision=HIGH
    )
    output = output + jnp.einsum("bhts,bhsv->bhtv", scores, update, precision=HIGH)
    final_log = cumulative[..., -1:]
    revised_memory_matrix = jnp.exp(final_log)[..., None] * matrix_state + jnp.einsum(
        "bhsk,bhsv->bhkv",
        key_rows * jnp.exp(final_log - cumulative)[..., None],
        update,
        precision=HIGH,
    )
    return (output, revised_memory_matrix)


def unit_rows(matrix):
    return matrix * lax.rsqrt(jnp.sum(matrix * matrix, axis=-1, keepdims=True) + EPS)


def token_blender(
    mapped_token_vectors,
    magnitude_exponent,
    offset_terms_array,
    surplus_forgetting_exponent,
    multiplier_terms_array,
    incoming_memory_matrix,
    batch_total,
    generation_round_total,
):
    rounded = [
        lax.optimization_barrier(part_sum.astype(jnp.bfloat16)).astype(jnp.float32)
        for part_sum in mapped_token_vectors
    ]
    queries, keys_raw, values_raw, gate_raw, decay_pre, strength_pre = rounded
    head_count = incoming_memory_matrix.shape[1]

    def to_heads(matrix):
        return matrix.reshape(batch_total, generation_round_total, head_count, HEAD_DIM).transpose(
            0, 2, 1, 3
        )

    def per_head(matrix):
        return matrix.reshape(batch_total, generation_round_total, head_count).transpose(0, 2, 1)

    queries = unit_rows(jax.nn.silu(to_heads(queries))) * HEAD_DIM ** (-0.5)
    key_rows = unit_rows(jax.nn.silu(to_heads(keys_raw)))
    values = jax.nn.silu(to_heads(values_raw))
    forgetting_exponent_amount = -jnp.exp(magnitude_exponent)[None, :, None] * jax.nn.softplus(
        per_head(decay_pre) + offset_terms_array[None, :, None]
    )
    forgetting_exponent_amount = forgetting_exponent_amount + surplus_forgetting_exponent.transpose(
        0, 2, 1
    )
    strength = jax.nn.sigmoid(per_head(strength_pre))
    matrix_state = incoming_memory_matrix.reshape(batch_total, head_count, HEAD_DIM, HEAD_DIM)
    output, revised_memory_matrix = delta_block(
        queries, key_rows, values, forgetting_exponent_amount, strength, matrix_state
    )
    normed = output * lax.rsqrt(jnp.mean(output * output, axis=-1, keepdims=True) + EPS)
    normed = (
        normed
        * multiplier_terms_array.reshape(head_count, HEAD_DIM)[None, :, None, :]
        * jax.nn.silu(to_heads(gate_raw))
    )
    blended_token_vectors = (
        normed.transpose(0, 2, 1, 3)
        .reshape(batch_total * generation_round_total, head_count * HEAD_DIM)
        .astype(jnp.bfloat16)
    )
    return (
        blended_token_vectors,
        revised_memory_matrix.reshape(batch_total, head_count, HEAD_DIM * HEAD_DIM),
    )


LANES = 128


def bf16_dot(left, right):
    return jnp.dot(left, right, preferred_element_type=jnp.float32)


def head_sums(squares, ones):
    high = squares.astype(jnp.bfloat16)
    low = (squares - high.astype(jnp.float32)).astype(jnp.bfloat16)
    return bf16_dot(high, ones) + bf16_dot(low, ones)


def project(portion, weights):
    return tuple(
        (jnp.dot(portion, weight, preferred_element_type=jnp.float32) for weight in weights)
    )


def out_project(blended_token_vectors, weight_rows):
    return jnp.dot(
        lax.all_gather(blended_token_vectors, "tp", axis=1, tiled=True),
        weight_rows,
        preferred_element_type=jnp.float32,
    ).astype(jnp.bfloat16)


def post_residual(widened, mixed_out, multiplier_terms_array, complete):
    mixed_wide = lax.optimization_barrier(mixed_out).astype(jnp.float32)
    squares = jnp.sum(mixed_wide * mixed_wide, axis=-1)
    if not complete:
        squares = lax.psum(squares, "tp")
    post_rms = lax.rsqrt(squares / D + EPS)[:, None]
    return lax.optimization_barrier(
        (widened + mixed_wide * post_rms * multiplier_terms_array).astype(jnp.bfloat16)
    )


def local(
    residual_channel,
    prior_block_multiplier,
    probe_map_matrix,
    lookup_map_matrix,
    content_map_matrix,
    emission_valve_matrix,
    forgetting_map_matrix,
    insertion_rate_matrix,
    forgetting_magnitude_exponent,
    channel_forgetting_offset,
    surplus_forgetting_amounts,
    readout_rescale_multiplier,
    emission_map_matrix,
    post_mixing_multiplier,
    recurrent_matrices,
):
    batch_total, generation_round_total, own_width = residual_channel.shape
    head_count = recurrent_matrices.shape[2]
    row_count = batch_total * generation_round_total
    col_offset = lax.axis_index("tp") * own_width
    head_offset = lax.axis_index("tp") * head_count
    new_states = []

    def mix_layer(mapped_token_vectors, block_index_number):
        blended_token_vectors, revised_memory_matrix = token_blender(
            mapped_token_vectors,
            forgetting_magnitude_exponent[block_index_number],
            channel_forgetting_offset[block_index_number],
            surplus_forgetting_amounts[block_index_number],
            readout_rescale_multiplier[block_index_number],
            recurrent_matrices[block_index_number],
            batch_total,
            generation_round_total,
        )
        new_states.append(revised_memory_matrix)
        return out_project(blended_token_vectors, emission_map_matrix[block_index_number])

    def own_cols(matrix):
        return lax.dynamic_slice_in_dim(matrix, col_offset, own_width, matrix.ndim - 1)

    whole_rows = lax.all_gather(
        residual_channel.reshape(row_count, own_width), "tp", axis=1, tiled=True
    )
    current = whole_rows
    for block_index_number in range(LAYERS):
        widened = whole_rows.astype(jnp.float32)
        inv_rms = lax.rsqrt(jnp.mean(widened * widened, axis=-1, keepdims=True) + EPS)
        hidden = (widened * inv_rms * prior_block_multiplier[block_index_number]).astype(
            jnp.bfloat16
        )
        weights = (
            probe_map_matrix[block_index_number],
            lookup_map_matrix[block_index_number],
            content_map_matrix[block_index_number],
            emission_valve_matrix[block_index_number],
            lax.dynamic_slice_in_dim(
                forgetting_map_matrix[block_index_number], head_offset, head_count, 1
            ),
            lax.dynamic_slice_in_dim(
                insertion_rate_matrix[block_index_number], head_offset, head_count, 1
            ),
        )
        mapped_token_vectors = project(hidden, weights)
        mixed_out = mix_layer(mapped_token_vectors, block_index_number)
        if block_index_number < LAYERS - 1:
            gathered = lax.all_gather(mixed_out, "tp", axis=1, tiled=True)
            whole_rows = post_residual(
                widened, gathered, post_mixing_multiplier[block_index_number], True
            )
        else:
            current = post_residual(
                own_cols(widened),
                mixed_out,
                own_cols(post_mixing_multiplier[block_index_number]),
                False,
            )
    return (
        current.reshape(batch_total, generation_round_total, own_width),
        jnp.stack(new_states, axis=0),
    )


CHUNKS = 8
AHEAD = 8
GROUP_ROWS = 64


def step_kernel(
    count,
    chunks,
    x_hbm,
    probe_hbm,
    lookup_hbm,
    content_hbm,
    valve_hbm,
    forget_hbm,
    insert_hbm,
    emission_hbm,
    states_hbm,
    surplus_hbm,
    pre_gain_hbm,
    post_gain_hbm,
    read_gain_hbm,
    magnitude_hbm,
    offset_hbm,
    out_ref,
    new_hbm,
    in_ref,
    y_ref,
    w_ref,
    wo_ref,
    rates_ref,
    h_ref,
    x1_ref,
    xown_ref,
    mown_ref,
    sq_ref,
    sur_ref,
    state_ref,
    new_ref,
    proj_ref,
    grown_ref,
    qk_ref,
    xq_ref,
    kd_ref,
    u_ref,
    qs_ref,
    dec_ref,
    spread_ref,
    ones_ref,
    perm_ref,
    surplus_ref,
    pre_gain_ref,
    post_gain_ref,
    read_gain_ref,
    magnitude_ref,
    offset_ref,
    load_sem,
    state_sem,
    own_sem,
    in_sem,
    y_sem,
    sq_sem,
):
    f32, bf16 = jnp.float32, jnp.bfloat16
    me = lax.axis_index("tp")
    depth = count // 4
    core, row, line = lax.rem(me, 2), lax.rem(me // 2, 2), me // 4
    over, twin = me + 2 - 4 * row, me + 1 - 2 * core
    items = 2 * chunks
    rows = h_ref.shape[0]
    seqs, steps = qk_ref.shape[1], qk_ref.shape[2]
    width = in_ref.shape[3]
    heads = forget_hbm.shape[1]
    own_heads = heads // count

    barrier = pltpu.get_barrier_semaphore()
    for step in range(1, count):
        pl.semaphore_signal(
            barrier,
            inc=1,
            device_id={"tp": lax.rem(me + step, count)},
            device_id_type=pl.DeviceIdType.MESH,
        )

    loads = []
    for layer in range(2):
        for at, matrix in enumerate((probe_hbm, lookup_hbm, content_hbm, valve_hbm)):
            loads.append(
                (matrix.at[layer], w_ref.at[layer, :, pl.ds(at * LANES, LANES)])
            )
        loads.append((forget_hbm.at[layer], rates_ref.at[layer, pl.ds(0, heads), :]))
        loads.append((insert_hbm.at[layer], rates_ref.at[layer, pl.ds(heads, heads), :]))
        loads.append((emission_hbm.at[layer], wo_ref.at[layer]))
    loads += [
        (surplus_hbm, surplus_ref),
        (pre_gain_hbm, pre_gain_ref),
        (post_gain_hbm, post_gain_ref),
        (read_gain_hbm, read_gain_ref),
        (magnitude_hbm, magnitude_ref),
        (offset_hbm, offset_ref),
    ]
    loads = [
        pltpu.make_async_copy(source, target, load_sem.at[at])
        for at, (source, target) in enumerate(loads)
    ]
    for copy in loads:
        copy.start()

    def place(slot):
        past = slot - AHEAD
        odd = lax.rem(past + 2 * AHEAD, 2)
        layer = jnp.where(slot < AHEAD, 0, jnp.where(slot < items - AHEAD, 1 - odd, 1))
        middle = jnp.where(slot < items - AHEAD, past // 2 + AHEAD * odd, slot - chunks)
        return layer, jnp.where(slot < AHEAD, slot, middle)

    def item_at(slot):
        layer, chunk = place(slot)
        return layer * chunks + chunk

    def state_load(slot):
        layer, chunk = place(slot)
        return pltpu.make_async_copy(
            states_hbm.at[layer, pl.ds(chunk * seqs, seqs)],
            state_ref.at[lax.rem(slot, 2)],
            state_sem.at[0, lax.rem(slot, 2)],
        )

    def state_store(slot):
        layer, chunk = place(slot)
        return pltpu.make_async_copy(
            new_ref.at[lax.rem(slot, 2)],
            new_hbm.at[layer, pl.ds(chunk * seqs, seqs)],
            state_sem.at[1, lax.rem(slot, 2)],
        )

    state_load(0).start()

    pl.semaphore_wait(barrier, count - 1)

    def remote(source, target, send_sem, land_sem, device):
        return pltpu.make_async_remote_copy(
            src_ref=source,
            dst_ref=target,
            send_sem=send_sem,
            recv_sem=land_sem,
            device_id={"tp": device},
            device_id_type=pl.DeviceIdType.MESH,
        )

    def when(condition, action, *operands):
        @pl.when(condition)
        def _():
            action(*operands)

    inner = (line == 1) | (line == 2)
    shifts = (0, 1 - 2 * lax.rem(line, 2), 2 - 4 * (line // 2), 3 - 2 * line)

    def along(step):
        return 4 * shifts[step]

    def begin(buf, sems, item, source):
        target = buf.at[item, me]

        def out(kind, device):
            remote(source, target, sems.at[0, item], sems.at[kind, item], device).start()

        out(5, me + along(2))
        out(4, me + along(1))
        when(inner, out, 6, me + along(3))
        out(1, over)
        out(3, twin)

    def pass_on(buf, sems, item, origin, kind, device, half=None):
        block = buf.at[item, origin]
        if half is not None:
            block = buf.at[item, origin, pl.ds(half * (rows // 2), rows // 2)]
        remote(block, block, sems.at[0, item], sems.at[kind, item], device).start()

    def landed(buf, sems, item, kind, blocks):
        part = buf.at[item, pl.ds(0, blocks)]
        remote(part, part, sems.at[0, item], sems.at[kind, item], twin).wait_recv()

    def relay_near(buf, sems, item):
        landed(buf, sems, item, 5, 1)
        when(inner, pass_on, buf, sems, item, me + along(2), 6, me + along(1))
        pass_on(buf, sems, item, me + along(2), 2, over)
        pass_on(buf, sems, item, me + along(2), 3, twin)
        landed(buf, sems, item, 1, 1)
        pass_on(buf, sems, item, over, 2, me + along(1), 0)
        pass_on(buf, sems, item, over, 3, twin)
        landed(buf, sems, item, 4, 1)
        pass_on(buf, sems, item, me + along(1), 2, over, 1)
        pass_on(buf, sems, item, me + along(1), 3, twin)

    def relay_far(buf, sems, item):
        landed(buf, sems, item, 6, 1)
        pass_on(buf, sems, item, me + along(3), 2, over)
        pass_on(buf, sems, item, me + along(3), 3, twin)

    def relay_twin(buf, sems, item):
        landed(buf, sems, item, 2, depth - 1)
        for step in range(1, depth):
            pass_on(buf, sems, item, over + along(step), 3, twin)

    def complete(buf, sems, item):
        landed(buf, sems, item, 3, 2 * depth)

    def drained(buf, sems, item):
        def sent(blocks):
            part = buf.at[item, pl.ds(0, blocks)]
            remote(part, part, sems.at[0, item], sems.at[1, item], twin).wait_send()

        when(inner, sent, count)
        when(jnp.logical_not(inner), sent, count - 2)

    def own_copy(item):
        return pltpu.make_async_copy(
            x_hbm.at[pl.ds(item * rows, rows), :], in_ref.at[item, me], own_sem.at[item]
        )

    def begin_x(item):
        begin(in_ref, in_sem, item, x_hbm.at[pl.ds(item * rows, rows), :])
        own_copy(item).start()

    for item in range(3):
        begin_x(item)

    def iota(shape, axis):
        return lax.broadcasted_iota(jnp.int32, shape, axis)

    shape = (2 * heads, 2 * LANES)
    wanted = iota(shape, 1) // HEAD_DIM
    wanted = jnp.where(wanted >= 2, wanted - 2 + heads, wanted) + me * own_heads
    spread_ref[...] = jnp.where(iota(shape, 0) == wanted, 1.0, 0.0).astype(bf16)
    shape = (2 * LANES, 2 * LANES)
    ones_ref[...] = jnp.where(
        iota(shape, 0) // HEAD_DIM == iota(shape, 1) // HEAD_DIM, 1.0, 0.0
    ).astype(bf16)
    shape = (LANES, LANES)
    head, channel = iota(shape, 0) // HEAD_DIM, iota(shape, 0) % HEAD_DIM
    target = (channel % 2) * HEAD_DIM + (channel // 2) * 2 + head
    perm_ref[...] = jnp.where(target == iota(shape, 1), 1.0, 0.0).astype(bf16)
    for copy in loads:
        copy.wait()
    all_seqs = sur_ref.shape[1]
    first_head = iota((LANES, all_seqs), 0) < HEAD_DIM
    for layer in range(2):
        for step in range(steps):
            pair = surplus_ref[layer, step]
            wide = jnp.where(first_head, pair[0:1, :], pair[1:2, :])
            sur_ref[layer, :, step, :] = wide.T
        for origin in range(count):
            at = pl.ds(origin * width, width)
            pair = rates_ref[layer, :, at].astype(f32)
            filled = jnp.concatenate([pair, jnp.zeros((LANES - 2 * heads, width), f32)], axis=0)
            w_ref[layer, at, pl.ds(4 * LANES, LANES)] = filled.T.astype(bf16)

    relay_near(in_ref, in_sem, 0)
    relay_far(in_ref, in_sem, 0)
    relay_twin(in_ref, in_sem, 0)

    def squares(matrix):
        return matrix[:, :LANES] * matrix[:, :LANES] + matrix[:, LANES:] * matrix[:, LANES:]

    def inverse(total):
        return lax.rsqrt(jnp.sum(total, axis=1, keepdims=True) * (1.0 / D) + EPS)

    def cols_of(origin):
        return pl.ds(origin * width, width)

    def first_hidden(item):
        def part(group, carry):
            at = pl.ds(group * GROUP_ROWS, GROUP_ROWS)
            total = jnp.zeros((GROUP_ROWS, LANES), f32)
            for origin in range(count):
                total = total + squares(in_ref[item, origin, at, :].astype(f32))
            scale = inverse(total)
            for origin in range(count):
                block = in_ref[item, origin, at, :].astype(f32)
                gain = pre_gain_ref[0:1, cols_of(origin)]
                h_ref[at, cols_of(origin)] = (block * scale * gain).astype(bf16)
            return carry

        lax.fori_loop(0, rows // GROUP_ROWS, part, 0)

    def second_hidden(item):
        earlier = item - chunks

        def part(group, carry):
            at = pl.ds(group * GROUP_ROWS, GROUP_ROWS)
            total = jnp.zeros((GROUP_ROWS, LANES), f32)
            for origin in range(count):
                total = total + squares(in_ref[item, origin, at, :].astype(f32))
            scale = inverse(total)
            total = jnp.zeros((GROUP_ROWS, LANES), f32)
            for origin in range(count):
                mixed = in_ref[item, origin, at, :].astype(f32)
                before = in_ref[earlier, origin, at, :].astype(f32)
                gain = post_gain_ref[0:1, cols_of(origin)]
                after = (before + mixed * scale * gain).astype(bf16)
                x1_ref[origin, at, :] = after
                total = total + squares(after.astype(f32))
            scale = inverse(total)
            for origin in range(count):
                block = x1_ref[origin, at, :].astype(f32)
                gain = pre_gain_ref[1:2, cols_of(origin)]
                h_ref[at, cols_of(origin)] = (block * scale * gain).astype(bf16)
            xown_ref[earlier, at, :] = x1_ref[me, at, :]
            return carry

        lax.fori_loop(0, rows // GROUP_ROWS, part, 0)

    def cols(at):
        return proj_ref[:, at * LANES : (at + 1) * LANES].astype(f32)

    def tokens(matrix):
        return matrix.reshape(seqs, steps, LANES)

    def lane_pair(ref, layer):
        left = iota((1, LANES), 1) < HEAD_DIM
        return jnp.where(left, ref[layer, 0], ref[layer, 1])

    def prepare(layer, chunk):
        ones = ones_ref[...]
        perm = perm_ref[...]
        queries = jax.nn.silu(cols(0))
        keys = jax.nn.silu(cols(1))
        sums = head_sums(jnp.concatenate([queries * queries, keys * keys], axis=1), ones)
        queries = tokens(queries * lax.rsqrt(sums[:, :LANES] + EPS) * HEAD_DIM ** (-0.5))
        keys = tokens(keys * lax.rsqrt(sums[:, LANES:] + EPS))
        spread = bf16_dot(proj_ref[:, 4 * LANES : 4 * LANES + 2 * heads], spread_ref[...])
        biased = spread[:, :LANES] + lane_pair(offset_ref, layer)
        softplus = jnp.maximum(biased, 0.0) + jnp.log1p(jnp.exp(-jnp.abs(biased)))
        pace = -jnp.exp(lane_pair(magnitude_ref, layer))
        cumulative = tokens(pace * softplus) + sur_ref[layer, pl.ds(chunk * seqs, seqs)]
        beta = tokens(jax.nn.sigmoid(spread[:, LANES:]))
        token = lax.broadcasted_iota(jnp.int32, (seqs, steps, LANES), 1)
        shift = 1
        while shift < steps:
            moved = pltpu.roll(cumulative, shift, axis=1)
            cumulative = cumulative + jnp.where(token >= shift, moved, 0.0)
            shift *= 2
        grown = jnp.exp(cumulative)
        grown_ref[...] = grown
        solved_u = beta * tokens(jax.nn.silu(cols(2)))
        solved_p = beta * grown * keys
        for at in range(steps):
            causal = token >= at
            gap = jnp.where(causal, cumulative - cumulative[:, at : at + 1, :], 0.0)
            decay = jnp.where(causal, jnp.exp(gap), 0.0)
            key_row = keys[:, at : at + 1, :]
            pair = jnp.concatenate([queries * key_row, keys * key_row], axis=2)
            dots = bf16_dot(pair.reshape(rows, 2 * LANES).astype(bf16), ones)
            qk_ref[at] = tokens(dots[:, :LANES]) * decay
            if at < steps - 1:
                a_col = jnp.where(token > at, beta * decay * tokens(dots[:, LANES:]), 0.0)
                solved_u = solved_u - a_col * solved_u[:, at : at + 1, :]
                solved_p = solved_p - a_col * solved_p[:, at : at + 1, :]
        last = cumulative[:, steps - 1 : steps, :]
        faded = keys * jnp.exp(last - cumulative)

        def permuted(first, second):
            both = jnp.concatenate([first, second], axis=1).reshape(2 * rows, LANES)
            return bf16_dot(both.astype(bf16), perm).astype(bf16).reshape(seqs, 2 * steps, LANES)

        xq_ref[...] = permuted(queries, solved_p)
        kd_ref[...] = permuted(faded, faded)
        u_ref[...] = solved_u
        dec_ref[...] = jnp.broadcast_to(jnp.exp(last), (seqs, steps, LANES))

    state_rows = state_ref.shape[2]

    def advance(slot):
        even = iota((state_rows, LANES), 0) % 2 == 0
        left = iota((state_rows, LANES), 1) < HEAD_DIM
        kept = even == left

        def one_sequence(at, carry):
            state = state_ref[slot, at]
            turned = pltpu.roll(state, HEAD_DIM, axis=1)
            upper = jnp.where(kept, jnp.where(even, state, turned), 0.0)
            lower = jnp.where(kept, jnp.where(even, turned, state), 0.0)
            wide = jnp.concatenate([upper, lower], axis=0).astype(bf16)
            read = bf16_dot(xq_ref[at], wide)
            qs_ref[at] = read[:steps]
            update = u_ref[at] - read[steps:]
            u_ref[at] = update
            high = update.astype(bf16).astype(f32)
            split = jnp.concatenate([high, update - high], axis=0).astype(bf16)
            grow = lax.dot_general(
                kd_ref[at], split, (((0,), (0,)), ((), ())), preferred_element_type=f32
            )
            grow_0, grow_1 = grow[:state_rows], grow[state_rows:]
            crossed = pltpu.roll(jnp.where(even, grow_1, grow_0), HEAD_DIM, axis=1)
            added = jnp.where(kept, jnp.where(even, grow_0, grow_1), crossed)
            fade = dec_ref[at]
            fade_turned = pltpu.roll(fade, HEAD_DIM, axis=1)
            copies = state_rows // steps
            factor = jnp.where(
                kept,
                jnp.concatenate([fade] * copies, axis=0),
                jnp.concatenate([fade_turned] * copies, axis=0),
            )
            new_ref[slot, at] = factor * state + added
            return carry

        lax.fori_loop(0, seqs, one_sequence, 0, unroll=8)

    def read_out(item, layer):
        update = u_ref[...]
        output = grown_ref[...] * qs_ref[...]
        for at in range(steps):
            output = output + qk_ref[at] * update[:, at : at + 1, :]
        output = output.reshape(rows, LANES)
        sums = head_sums(output * output, ones_ref[:LANES, :LANES])
        output = output * lax.rsqrt(sums * (1.0 / HEAD_DIM) + EPS)
        gain = read_gain_ref[pl.ds(layer, 1), :]
        y_ref[item, me] = (output * gain * jax.nn.silu(cols(3))).astype(bf16)

    def emit(item):
        whole = jnp.concatenate([y_ref[item, origin] for origin in range(count)], axis=1)
        return bf16_dot(whole, wo_ref[item // chunks]).astype(bf16)

    def emit_middle(item):
        in_ref[item + chunks, me] = emit(item)

    def emit_last(item):
        mixed = emit(item)
        chunk = item - chunks
        mown_ref[chunk] = mixed
        wide = mixed.astype(f32)
        total = jnp.sum(squares(wide), axis=1, keepdims=True)
        sq_ref[chunk, me] = jnp.broadcast_to(total, (rows, LANES)).T[:1]

    def sums_begin(chunk):
        block = sq_ref.at[chunk, me]
        for step in range(1, count):
            remote(
                block, block, sq_sem.at[0, chunk], sq_sem.at[1, chunk], lax.rem(me + step, count)
            ).start()

    def sums_all(chunk):
        part = sq_ref.at[chunk, pl.ds(0, count - 1)]
        return remote(part, part, sq_sem.at[0, chunk], sq_sem.at[1, chunk], twin)

    def finish(chunk):
        sums_all(chunk).wait_recv()
        total = sq_ref[chunk, 0]
        for origin in range(1, count):
            total = total + sq_ref[chunk, origin]
        total = jnp.broadcast_to(total, (LANES, rows)).T
        scale = lax.rsqrt(total * (1.0 / D) + EPS)
        for half in range(width // LANES):
            at = pl.ds(half * LANES, LANES)
            gain = post_gain_ref[1:2, pl.ds(pl.multiple_of(me * width + half * LANES, LANES), LANES)]
            before = xown_ref[chunk, :, at].astype(f32)
            mixed = mown_ref[chunk, :, at].astype(f32)
            out_ref[pl.ds(chunk * rows, rows), at] = (before + mixed * scale * gain).astype(bf16)

    def slot_of(slot, carry):
        (layer, chunk), buffer = place(slot), lax.rem(slot, 2)
        item = layer * chunks + chunk
        first = layer == 0
        when(slot + 1 < items, lambda: state_load(slot + 1).start())
        when(first & (chunk + 3 < chunks), lambda: begin_x(chunk + 3))
        complete(in_ref, in_sem, item)

        @pl.when(first)
        def _():
            own_copy(chunk).wait()
            first_hidden(chunk)

        when(layer == 1, second_hidden, item)
        proj_ref[...] = bf16_dot(h_ref[...], w_ref[layer]).astype(bf16)

        def older(by):
            return item_at(slot - by)

        def mixed(by):
            return (slot >= by) & (place(slot - by)[0] == 0)

        when(mixed(5), relay_near, in_ref, in_sem, older(5) + chunks)
        when(slot == 0, relay_near, in_ref, in_sem, 1)
        when(slot >= 2, relay_far, y_ref, y_sem, older(2))
        when(mixed(6), relay_twin, in_ref, in_sem, older(6) + chunks)
        prepare(layer, chunk)
        when(first & (chunk + 2 < chunks), relay_near, in_ref, in_sem, chunk + 2)
        when(slot == 0, relay_far, in_ref, in_sem, 1)
        state_load(slot).wait()
        when(slot >= 2, lambda: state_store(slot - 2).wait())
        advance(buffer)
        when(mixed(5), relay_far, in_ref, in_sem, older(5) + chunks)
        when(slot >= 1, relay_near, y_ref, y_sem, older(1))
        when(first & (chunk + 2 < chunks), relay_far, in_ref, in_sem, chunk + 2)
        when(slot >= 2, relay_twin, y_ref, y_sem, older(2))
        read_out(item, layer)
        state_store(slot).start()
        past, (past_layer, past_chunk) = older(3), place(slot - 3)
        when(slot >= 3, complete, y_ref, y_sem, past)
        begin(y_ref, y_sem, item, y_ref.at[item, me])
        early = (slot >= 3) & (past_layer == 0)
        late = (slot >= 3) & (past_layer == 1)
        when(early, emit_middle, past)
        when(late, emit_last, past)
        when(first & (chunk + 1 < chunks), relay_twin, in_ref, in_sem, chunk + 1)

        @pl.when(early)
        def _():
            begin(in_ref, in_sem, past + chunks, in_ref.at[past + chunks, me])

        when(late, sums_begin, past_chunk)
        return carry

    lax.fori_loop(0, items, slot_of, 0)
    final = items - 1
    relay_far(y_ref, y_sem, final - 1)
    complete(y_ref, y_sem, final - 2)
    emit_last(final - 2)
    relay_near(y_ref, y_sem, final)
    relay_twin(y_ref, y_sem, final - 1)
    sums_begin(chunks - 3)
    for chunk in range(chunks - 4):
        finish(chunk)
    relay_far(y_ref, y_sem, final)
    complete(y_ref, y_sem, final - 1)
    emit_last(final - 1)
    finish(chunks - 4)
    sums_begin(chunks - 2)
    relay_twin(y_ref, y_sem, final)
    state_store(items - 2).wait()
    state_store(items - 1).wait()
    for item in range(items):
        drained(in_ref, in_sem, item)
        if item < final:
            drained(y_ref, y_sem, item)
    complete(y_ref, y_sem, final)
    emit_last(final)
    drained(y_ref, y_sem, final)
    sums_begin(chunks - 1)
    for chunk in range(chunks - 3, chunks):
        finish(chunk)
    for chunk in range(chunks):
        sums_all(chunk).wait_send()


def local_two_heads(
    residual_channel,
    prior_block_multiplier,
    probe_map_matrix,
    lookup_map_matrix,
    content_map_matrix,
    emission_valve_matrix,
    forgetting_map_matrix,
    insertion_rate_matrix,
    forgetting_magnitude_exponent,
    channel_forgetting_offset,
    surplus_forgetting_amounts,
    readout_rescale_multiplier,
    emission_map_matrix,
    post_mixing_multiplier,
    recurrent_matrices,
):
    batch_total, steps, own_width = residual_channel.shape
    layers, _, head_count, state_size = recurrent_matrices.shape
    row_count = batch_total * steps
    count = lax.axis_size("tp")
    groups = state_size // LANES
    chunks = CHUNKS
    seqs, rows = batch_total // chunks, row_count // chunks
    heads = forgetting_map_matrix.shape[2]
    features = forgetting_map_matrix.shape[1]
    mix_width = emission_map_matrix.shape[1]
    states = (
        recurrent_matrices.reshape(layers, batch_total, head_count, groups, LANES)
        .transpose(0, 1, 3, 2, 4)
        .reshape(layers, batch_total, groups * head_count, LANES)
    )
    f32, bf16 = jnp.float32, jnp.bfloat16
    dma = pltpu.SemaphoreType.DMA
    hbm = pl.BlockSpec(memory_space=pl.ANY)
    vmem = pl.BlockSpec(memory_space=pltpu.VMEM)
    tile = (seqs, steps, LANES)
    state_tile = (2, seqs, groups * head_count, LANES)
    current, new_memory = pl.pallas_call(
        lambda *refs: step_kernel(count, chunks, *refs),
        out_shape=[
            jax.ShapeDtypeStruct((row_count, own_width), bf16),
            jax.ShapeDtypeStruct(states.shape, f32),
        ],
        in_specs=[hbm] * 15,
        out_specs=[vmem, hbm],
        scratch_shapes=[
            pltpu.VMEM((2 * chunks, count, rows, own_width), bf16),
            pltpu.VMEM((2 * chunks, count, rows, LANES), bf16),
            pltpu.VMEM((layers, features, 5 * LANES), bf16),
            pltpu.VMEM((layers, mix_width, own_width), bf16),
            pltpu.VMEM((layers, 2 * heads, features), bf16),
            pltpu.VMEM((rows, features), bf16),
            pltpu.VMEM((count, rows, own_width), bf16),
            pltpu.VMEM((chunks, rows, own_width), bf16),
            pltpu.VMEM((chunks, rows, own_width), bf16),
            pltpu.VMEM((chunks, count, 1, rows), f32),
            pltpu.VMEM((layers, batch_total, steps, LANES), f32),
            pltpu.VMEM(state_tile, f32),
            pltpu.VMEM(state_tile, f32),
            pltpu.VMEM((rows, 5 * LANES), bf16),
            pltpu.VMEM(tile, f32),
            pltpu.VMEM((steps,) + tile, f32),
            pltpu.VMEM((seqs, 2 * steps, LANES), bf16),
            pltpu.VMEM((seqs, 2 * steps, LANES), bf16),
            pltpu.VMEM(tile, f32),
            pltpu.VMEM(tile, f32),
            pltpu.VMEM(tile, f32),
            pltpu.VMEM((2 * heads, 2 * LANES), bf16),
            pltpu.VMEM((2 * LANES, 2 * LANES), bf16),
            pltpu.VMEM((LANES, LANES), bf16),
            pltpu.VMEM((layers, steps, head_count, batch_total), f32),
            pltpu.VMEM((layers, features), f32),
            pltpu.VMEM((layers, features), f32),
            pltpu.VMEM((layers, LANES), f32),
            pltpu.SMEM((layers, head_count), f32),
            pltpu.SMEM((layers, head_count), f32),
            dma((20,)),
            dma((2, 2)),
            dma((chunks,)),
            dma((3 + count // 4, 2 * chunks)),
            dma((3 + count // 4, 2 * chunks)),
            dma((2, chunks)),
        ],
        compiler_params=pltpu.CompilerParams(
            collective_id=1, has_side_effects=True, vmem_limit_bytes=62 * 1024 * 1024
        ),
        name="step",
    )(
        residual_channel.reshape(row_count, own_width),
        probe_map_matrix,
        lookup_map_matrix,
        content_map_matrix,
        emission_valve_matrix,
        forgetting_map_matrix.transpose(0, 2, 1),
        insertion_rate_matrix.transpose(0, 2, 1),
        emission_map_matrix,
        states,
        surplus_forgetting_amounts.transpose(0, 2, 3, 1),
        prior_block_multiplier,
        post_mixing_multiplier,
        readout_rescale_multiplier,
        forgetting_magnitude_exponent,
        channel_forgetting_offset,
    )
    new_memory = (
        new_memory.reshape(layers, batch_total, groups, head_count, LANES)
        .transpose(0, 1, 3, 2, 4)
        .reshape(recurrent_matrices.shape)
    )
    return current.reshape(batch_total, steps, own_width), new_memory


def local_any(*arrays):
    residual_channel, recurrent_matrices = arrays[0], arrays[-1]
    two_heads = (
        recurrent_matrices.shape[2] * HEAD_DIM == LANES
        and residual_channel.shape[1] == 8
        and residual_channel.shape[0] % (8 * CHUNKS) == 0
        and residual_channel.shape[2] % LANES == 0
        and lax.axis_size("tp") == 16
    )
    return (local_two_heads if two_heads else local)(*arrays)


def solution(mesh):
    return jax.shard_map(
        local_any,
        mesh=mesh,
        in_specs=(
            P("grp", None, "tp"),
            P(),
            P(None, None, "tp"),
            P(None, None, "tp"),
            P(None, None, "tp"),
            P(None, None, "tp"),
            P(),
            P(),
            P(None, "tp"),
            P(None, "tp"),
            P(None, "grp", None, "tp"),
            P(None, "tp"),
            P(None, None, "tp"),
            P(),
            P(None, "grp", "tp", None),
        ),
        out_specs=(P("grp", None, "tp"), P(None, "grp", "tp", None)),
        check_vma=False,
    )
```

```python
import jax
import jax.numpy as jnp
from jax import lax
from jax.experimental import pallas as pl
from jax.experimental.pallas import tpu as pltpu
from jax.sharding import PartitionSpec as P

D = 4096
HEAD_DIM = 64
LAYERS = 2


EPS = 1e-06
HIGH = lax.Precision.HIGHEST


def solve_lower(a_mat, right_side):
    length = right_side.shape[-2]
    solved_rows = []
    for row_at in range(length):
        current_row = right_side[..., row_at, :]
        for col_at in range(row_at):
            current_row = current_row - a_mat[..., row_at, col_at][..., None] * solved_rows[col_at]
        solved_rows.append(current_row)
    return jnp.stack(solved_rows, axis=-2)


def delta_block(queries, key_rows, values, forgetting_exponent_amount, strength, matrix_state):
    length = queries.shape[2]
    causal = jnp.tril(jnp.ones((length, length), bool))
    strict = jnp.tril(jnp.ones((length, length), bool), -1)
    cumulative = jnp.cumsum(forgetting_exponent_amount, axis=-1)
    decay_mat = jnp.where(
        causal,
        jnp.exp(jnp.where(causal, cumulative[..., :, None] - cumulative[..., None, :], 0.0)),
        0.0,
    )
    key_gram = jnp.einsum("bhtd,bhsd->bhts", key_rows, key_rows, precision=HIGH)
    a_mat = jnp.where(strict, strength[..., :, None] * decay_mat * key_gram, 0.0)
    right_side = jnp.concatenate(
        [strength[..., None] * values, (strength * jnp.exp(cumulative))[..., None] * key_rows],
        axis=-1,
    )
    solved = solve_lower(a_mat, right_side)
    width_v = values.shape[-1]
    update = solved[..., :width_v] - jnp.einsum(
        "bhtk,bhkv->bhtv", solved[..., width_v:], matrix_state, precision=HIGH
    )
    scores = jnp.einsum("bhtd,bhsd->bhts", queries, key_rows, precision=HIGH) * decay_mat
    output = jnp.exp(cumulative)[..., None] * jnp.einsum(
        "bhtk,bhkv->bhtv", queries, matrix_state, precision=HIGH
    )
    output = output + jnp.einsum("bhts,bhsv->bhtv", scores, update, precision=HIGH)
    final_log = cumulative[..., -1:]
    revised_memory_matrix = jnp.exp(final_log)[..., None] * matrix_state + jnp.einsum(
        "bhsk,bhsv->bhkv",
        key_rows * jnp.exp(final_log - cumulative)[..., None],
        update,
        precision=HIGH,
    )
    return (output, revised_memory_matrix)


def unit_rows(matrix):
    return matrix * lax.rsqrt(jnp.sum(matrix * matrix, axis=-1, keepdims=True) + EPS)


def token_blender(
    mapped_token_vectors,
    magnitude_exponent,
    offset_terms_array,
    surplus_forgetting_exponent,
    multiplier_terms_array,
    incoming_memory_matrix,
    batch_total,
    generation_round_total,
):
    rounded = [
        lax.optimization_barrier(part_sum.astype(jnp.bfloat16)).astype(jnp.float32)
        for part_sum in mapped_token_vectors
    ]
    queries, keys_raw, values_raw, gate_raw, decay_pre, strength_pre = rounded
    head_count = incoming_memory_matrix.shape[1]

    def to_heads(matrix):
        return matrix.reshape(batch_total, generation_round_total, head_count, HEAD_DIM).transpose(
            0, 2, 1, 3
        )

    def per_head(matrix):
        return matrix.reshape(batch_total, generation_round_total, head_count).transpose(0, 2, 1)

    queries = unit_rows(jax.nn.silu(to_heads(queries))) * HEAD_DIM ** (-0.5)
    key_rows = unit_rows(jax.nn.silu(to_heads(keys_raw)))
    values = jax.nn.silu(to_heads(values_raw))
    forgetting_exponent_amount = -jnp.exp(magnitude_exponent)[None, :, None] * jax.nn.softplus(
        per_head(decay_pre) + offset_terms_array[None, :, None]
    )
    forgetting_exponent_amount = forgetting_exponent_amount + surplus_forgetting_exponent.transpose(
        0, 2, 1
    )
    strength = jax.nn.sigmoid(per_head(strength_pre))
    matrix_state = incoming_memory_matrix.reshape(batch_total, head_count, HEAD_DIM, HEAD_DIM)
    output, revised_memory_matrix = delta_block(
        queries, key_rows, values, forgetting_exponent_amount, strength, matrix_state
    )
    normed = output * lax.rsqrt(jnp.mean(output * output, axis=-1, keepdims=True) + EPS)
    normed = (
        normed
        * multiplier_terms_array.reshape(head_count, HEAD_DIM)[None, :, None, :]
        * jax.nn.silu(to_heads(gate_raw))
    )
    blended_token_vectors = (
        normed.transpose(0, 2, 1, 3)
        .reshape(batch_total * generation_round_total, head_count * HEAD_DIM)
        .astype(jnp.bfloat16)
    )
    return (
        blended_token_vectors,
        revised_memory_matrix.reshape(batch_total, head_count, HEAD_DIM * HEAD_DIM),
    )


LANES = 128


def bf16_dot(left, right):
    return jnp.dot(left, right, preferred_element_type=jnp.float32)


def head_sums(squares, ones):
    high = squares.astype(jnp.bfloat16)
    low = (squares - high.astype(jnp.float32)).astype(jnp.bfloat16)
    return bf16_dot(high, ones) + bf16_dot(low, ones)


def project(portion, weights):
    return tuple(
        (jnp.dot(portion, weight, preferred_element_type=jnp.float32) for weight in weights)
    )


def out_project(blended_token_vectors, weight_rows):
    return jnp.dot(
        lax.all_gather(blended_token_vectors, "tp", axis=1, tiled=True),
        weight_rows,
        preferred_element_type=jnp.float32,
    ).astype(jnp.bfloat16)


def post_residual(widened, mixed_out, multiplier_terms_array, complete):
    mixed_wide = lax.optimization_barrier(mixed_out).astype(jnp.float32)
    squares = jnp.sum(mixed_wide * mixed_wide, axis=-1)
    if not complete:
        squares = lax.psum(squares, "tp")
    post_rms = lax.rsqrt(squares / D + EPS)[:, None]
    return lax.optimization_barrier(
        (widened + mixed_wide * post_rms * multiplier_terms_array).astype(jnp.bfloat16)
    )


def local(
    residual_channel,
    prior_block_multiplier,
    probe_map_matrix,
    lookup_map_matrix,
    content_map_matrix,
    emission_valve_matrix,
    forgetting_map_matrix,
    insertion_rate_matrix,
    forgetting_magnitude_exponent,
    channel_forgetting_offset,
    surplus_forgetting_amounts,
    readout_rescale_multiplier,
    emission_map_matrix,
    post_mixing_multiplier,
    recurrent_matrices,
):
    batch_total, generation_round_total, own_width = residual_channel.shape
    head_count = recurrent_matrices.shape[2]
    row_count = batch_total * generation_round_total
    col_offset = lax.axis_index("tp") * own_width
    head_offset = lax.axis_index("tp") * head_count
    new_states = []

    def mix_layer(mapped_token_vectors, block_index_number):
        blended_token_vectors, revised_memory_matrix = token_blender(
            mapped_token_vectors,
            forgetting_magnitude_exponent[block_index_number],
            channel_forgetting_offset[block_index_number],
            surplus_forgetting_amounts[block_index_number],
            readout_rescale_multiplier[block_index_number],
            recurrent_matrices[block_index_number],
            batch_total,
            generation_round_total,
        )
        new_states.append(revised_memory_matrix)
        return out_project(blended_token_vectors, emission_map_matrix[block_index_number])

    def own_cols(matrix):
        return lax.dynamic_slice_in_dim(matrix, col_offset, own_width, matrix.ndim - 1)

    whole_rows = lax.all_gather(
        residual_channel.reshape(row_count, own_width), "tp", axis=1, tiled=True
    )
    current = whole_rows
    for block_index_number in range(LAYERS):
        widened = whole_rows.astype(jnp.float32)
        inv_rms = lax.rsqrt(jnp.mean(widened * widened, axis=-1, keepdims=True) + EPS)
        hidden = (widened * inv_rms * prior_block_multiplier[block_index_number]).astype(
            jnp.bfloat16
        )
        weights = (
            probe_map_matrix[block_index_number],
            lookup_map_matrix[block_index_number],
            content_map_matrix[block_index_number],
            emission_valve_matrix[block_index_number],
            lax.dynamic_slice_in_dim(
                forgetting_map_matrix[block_index_number], head_offset, head_count, 1
            ),
            lax.dynamic_slice_in_dim(
                insertion_rate_matrix[block_index_number], head_offset, head_count, 1
            ),
        )
        mapped_token_vectors = project(hidden, weights)
        mixed_out = mix_layer(mapped_token_vectors, block_index_number)
        if block_index_number < LAYERS - 1:
            gathered = lax.all_gather(mixed_out, "tp", axis=1, tiled=True)
            whole_rows = post_residual(
                widened, gathered, post_mixing_multiplier[block_index_number], True
            )
        else:
            current = post_residual(
                own_cols(widened),
                mixed_out,
                own_cols(post_mixing_multiplier[block_index_number]),
                False,
            )
    return (
        current.reshape(batch_total, generation_round_total, own_width),
        jnp.stack(new_states, axis=0),
    )


CHUNKS = 8
AHEAD = 8
GROUP_ROWS = 64


def step_kernel(
    count,
    chunks,
    x_hbm,
    probe_hbm,
    lookup_hbm,
    content_hbm,
    valve_hbm,
    forget_hbm,
    insert_hbm,
    emission_hbm,
    states_hbm,
    surplus_hbm,
    pre_gain_hbm,
    post_gain_hbm,
    read_gain_hbm,
    magnitude_hbm,
    offset_hbm,
    out_ref,
    new_ref,
    in_ref,
    y_ref,
    w_ref,
    wo_ref,
    rates_ref,
    h_ref,
    x1_ref,
    xown_ref,
    mown_ref,
    sq_ref,
    sur_ref,
    state_ref,
    proj_ref,
    grown_ref,
    qk_ref,
    xq_ref,
    kd_ref,
    u_ref,
    qs_ref,
    dec_ref,
    spread_ref,
    ones_ref,
    perm_ref,
    surplus_ref,
    pre_gain_ref,
    post_gain_ref,
    read_gain_ref,
    magnitude_ref,
    offset_ref,
    load_sem,
    state_sem,
    own_sem,
    in_sem,
    y_sem,
    sq_sem,
):
    f32, bf16 = jnp.float32, jnp.bfloat16
    me = lax.axis_index("tp")
    depth = count // 4
    core, row, line = lax.rem(me, 2), lax.rem(me // 2, 2), me // 4
    over, twin = me + 2 - 4 * row, me + 1 - 2 * core
    items = 2 * chunks
    rows = h_ref.shape[0]
    seqs, steps = qk_ref.shape[1], qk_ref.shape[2]
    width = in_ref.shape[3]
    heads = forget_hbm.shape[1]
    own_heads = heads // count

    barrier = pltpu.get_barrier_semaphore()
    for step in range(1, count):
        pl.semaphore_signal(
            barrier,
            inc=1,
            device_id={"tp": lax.rem(me + step, count)},
            device_id_type=pl.DeviceIdType.MESH,
        )

    loads = []
    for layer in range(2):
        for at, matrix in enumerate((probe_hbm, lookup_hbm, content_hbm, valve_hbm)):
            loads.append(
                (matrix.at[layer], w_ref.at[layer, :, pl.ds(at * LANES, LANES)])
            )
        loads.append((forget_hbm.at[layer], rates_ref.at[layer, pl.ds(0, heads), :]))
        loads.append((insert_hbm.at[layer], rates_ref.at[layer, pl.ds(heads, heads), :]))
        loads.append((emission_hbm.at[layer], wo_ref.at[layer]))
    loads += [
        (surplus_hbm, surplus_ref),
        (pre_gain_hbm, pre_gain_ref),
        (post_gain_hbm, post_gain_ref),
        (read_gain_hbm, read_gain_ref),
        (magnitude_hbm, magnitude_ref),
        (offset_hbm, offset_ref),
    ]
    loads = [
        pltpu.make_async_copy(source, target, load_sem.at[at])
        for at, (source, target) in enumerate(loads)
    ]
    for copy in loads:
        copy.start()

    def place(slot):
        past = slot - AHEAD
        odd = lax.rem(past + 2 * AHEAD, 2)
        layer = jnp.where(slot < AHEAD, 0, jnp.where(slot < items - AHEAD, 1 - odd, 1))
        middle = jnp.where(slot < items - AHEAD, past // 2 + AHEAD * odd, slot - chunks)
        return layer, jnp.where(slot < AHEAD, slot, middle)

    def item_at(slot):
        layer, chunk = place(slot)
        return layer * chunks + chunk

    def state_load(slot):
        layer, chunk = place(slot)
        return pltpu.make_async_copy(
            states_hbm.at[layer, pl.ds(chunk * seqs, seqs)],
            state_ref.at[lax.rem(slot, 2)],
            state_sem.at[lax.rem(slot, 2)],
        )

    state_load(0).start()

    pl.semaphore_wait(barrier, count - 1)

    def remote(source, target, send_sem, land_sem, device):
        return pltpu.make_async_remote_copy(
            src_ref=source,
            dst_ref=target,
            send_sem=send_sem,
            recv_sem=land_sem,
            device_id={"tp": device},
            device_id_type=pl.DeviceIdType.MESH,
        )

    def when(condition, action, *operands):
        @pl.when(condition)
        def _():
            action(*operands)

    inner = (line == 1) | (line == 2)
    shifts = (0, 1 - 2 * lax.rem(line, 2), 2 - 4 * (line // 2), 3 - 2 * line)

    def along(step):
        return 4 * shifts[step]

    def begin(buf, sems, item, source):
        target = buf.at[item, me]

        def out(kind, device):
            remote(source, target, sems.at[0, item], sems.at[kind, item], device).start()

        out(5, me + along(2))
        out(4, me + along(1))
        when(inner, out, 6, me + along(3))
        out(1, over)
        out(3, twin)

    def pass_on(buf, sems, item, origin, kind, device, half=None):
        block = buf.at[item, origin]
        if half is not None:
            block = buf.at[item, origin, pl.ds(half * (rows // 2), rows // 2)]
        remote(block, block, sems.at[0, item], sems.at[kind, item], device).start()

    def landed(buf, sems, item, kind, blocks):
        part = buf.at[item, pl.ds(0, blocks)]
        remote(part, part, sems.at[0, item], sems.at[kind, item], twin).wait_recv()

    def relay_near(buf, sems, item):
        landed(buf, sems, item, 5, 1)
        when(inner, pass_on, buf, sems, item, me + along(2), 6, me + along(1))
        pass_on(buf, sems, item, me + along(2), 2, over)
        pass_on(buf, sems, item, me + along(2), 3, twin)
        landed(buf, sems, item, 1, 1)
        pass_on(buf, sems, item, over, 2, me + along(1), 0)
        pass_on(buf, sems, item, over, 3, twin)
        landed(buf, sems, item, 4, 1)
        pass_on(buf, sems, item, me + along(1), 2, over, 1)
        pass_on(buf, sems, item, me + along(1), 3, twin)

    def relay_far(buf, sems, item):
        landed(buf, sems, item, 6, 1)
        pass_on(buf, sems, item, me + along(3), 2, over)
        pass_on(buf, sems, item, me + along(3), 3, twin)

    def relay_twin(buf, sems, item):
        landed(buf, sems, item, 2, depth - 1)
        for step in range(1, depth):
            pass_on(buf, sems, item, over + along(step), 3, twin)

    def complete(buf, sems, item):
        landed(buf, sems, item, 3, 2 * depth)

    def drained(buf, sems, item):
        def sent(blocks):
            part = buf.at[item, pl.ds(0, blocks)]
            remote(part, part, sems.at[0, item], sems.at[1, item], twin).wait_send()

        when(inner, sent, count)
        when(jnp.logical_not(inner), sent, count - 2)

    def own_copy(item):
        return pltpu.make_async_copy(
            x_hbm.at[pl.ds(item * rows, rows), :], in_ref.at[item, me], own_sem.at[item]
        )

    def begin_x(item):
        begin(in_ref, in_sem, item, x_hbm.at[pl.ds(item * rows, rows), :])
        own_copy(item).start()

    for item in range(3):
        begin_x(item)

    def iota(shape, axis):
        return lax.broadcasted_iota(jnp.int32, shape, axis)

    shape = (2 * heads, 2 * LANES)
    wanted = iota(shape, 1) // HEAD_DIM
    wanted = jnp.where(wanted >= 2, wanted - 2 + heads, wanted) + me * own_heads
    spread_ref[...] = jnp.where(iota(shape, 0) == wanted, 1.0, 0.0).astype(bf16)
    shape = (2 * LANES, 2 * LANES)
    ones_ref[...] = jnp.where(
        iota(shape, 0) // HEAD_DIM == iota(shape, 1) // HEAD_DIM, 1.0, 0.0
    ).astype(bf16)
    shape = (LANES, 4 * LANES)
    block, spot = iota(shape, 1) // LANES, iota(shape, 1) % LANES
    target = (block // 2) * HEAD_DIM + 2 * (spot // 2) + block % 2
    fits = (iota(shape, 0) == target) & (spot % 2 == block // 2) & (spot < HEAD_DIM)
    perm_ref[...] = jnp.where(fits, 1.0, 0.0).astype(bf16)
    for copy in loads:
        copy.wait()
    all_seqs = sur_ref.shape[1]
    first_head = iota((LANES, all_seqs), 0) < HEAD_DIM
    for layer in range(2):
        for step in range(steps):
            pair = surplus_ref[layer, step]
            wide = jnp.where(first_head, pair[0:1, :], pair[1:2, :])
            sur_ref[layer, :, step, :] = wide.T
        for origin in range(count):
            at = pl.ds(origin * width, width)
            pair = rates_ref[layer, :, at].astype(f32)
            filled = jnp.concatenate([pair, jnp.zeros((LANES - 2 * heads, width), f32)], axis=0)
            w_ref[layer, at, pl.ds(4 * LANES, LANES)] = filled.T.astype(bf16)

    relay_near(in_ref, in_sem, 0)
    relay_far(in_ref, in_sem, 0)
    relay_twin(in_ref, in_sem, 0)

    def squares(matrix):
        return matrix[:, :LANES] * matrix[:, :LANES] + matrix[:, LANES:] * matrix[:, LANES:]

    def inverse(total):
        return lax.rsqrt(jnp.sum(total, axis=1, keepdims=True) * (1.0 / D) + EPS)

    def cols_of(origin):
        return pl.ds(origin * width, width)

    def first_hidden(item):
        def part(group, carry):
            at = pl.ds(group * GROUP_ROWS, GROUP_ROWS)
            total = jnp.zeros((GROUP_ROWS, LANES), f32)
            for origin in range(count):
                total = total + squares(in_ref[item, origin, at, :].astype(f32))
            scale = inverse(total)
            for origin in range(count):
                block = in_ref[item, origin, at, :].astype(f32)
                gain = pre_gain_ref[0:1, cols_of(origin)]
                h_ref[at, cols_of(origin)] = (block * scale * gain).astype(bf16)
            return carry

        lax.fori_loop(0, rows // GROUP_ROWS, part, 0)

    def second_hidden(item):
        earlier = item - chunks

        def part(group, carry):
            at = pl.ds(group * GROUP_ROWS, GROUP_ROWS)
            total = jnp.zeros((GROUP_ROWS, LANES), f32)
            for origin in range(count):
                total = total + squares(in_ref[item, origin, at, :].astype(f32))
            scale = inverse(total)
            total = jnp.zeros((GROUP_ROWS, LANES), f32)
            for origin in range(count):
                mixed = in_ref[item, origin, at, :].astype(f32)
                before = in_ref[earlier, origin, at, :].astype(f32)
                gain = post_gain_ref[0:1, cols_of(origin)]
                after = (before + mixed * scale * gain).astype(bf16)
                x1_ref[origin, at, :] = after
                total = total + squares(after.astype(f32))
            scale = inverse(total)
            for origin in range(count):
                block = x1_ref[origin, at, :].astype(f32)
                gain = pre_gain_ref[1:2, cols_of(origin)]
                h_ref[at, cols_of(origin)] = (block * scale * gain).astype(bf16)
            xown_ref[earlier, at, :] = x1_ref[me, at, :]
            return carry

        lax.fori_loop(0, rows // GROUP_ROWS, part, 0)

    def cols(at):
        return proj_ref[:, at * LANES : (at + 1) * LANES].astype(f32)

    def tokens(matrix):
        return matrix.reshape(seqs, steps, LANES)

    def lane_pair(ref, layer):
        left = iota((1, LANES), 1) < HEAD_DIM
        return jnp.where(left, ref[layer, 0], ref[layer, 1])

    def prepare(layer, chunk):
        ones = ones_ref[...]
        perm = perm_ref[...]
        queries = jax.nn.silu(cols(0))
        keys = jax.nn.silu(cols(1))
        sums = head_sums(jnp.concatenate([queries * queries, keys * keys], axis=1), ones)
        queries = tokens(queries * lax.rsqrt(sums[:, :LANES] + EPS) * HEAD_DIM ** (-0.5))
        keys = tokens(keys * lax.rsqrt(sums[:, LANES:] + EPS))
        spread = bf16_dot(proj_ref[:, 4 * LANES : 4 * LANES + 2 * heads], spread_ref[...])
        biased = spread[:, :LANES] + lane_pair(offset_ref, layer)
        softplus = jnp.maximum(biased, 0.0) + jnp.log1p(jnp.exp(-jnp.abs(biased)))
        pace = -jnp.exp(lane_pair(magnitude_ref, layer))
        cumulative = tokens(pace * softplus) + sur_ref[layer, pl.ds(chunk * seqs, seqs)]
        beta = tokens(jax.nn.sigmoid(spread[:, LANES:]))
        token = lax.broadcasted_iota(jnp.int32, (seqs, steps, LANES), 1)
        shift = 1
        while shift < steps:
            moved = pltpu.roll(cumulative, shift, axis=1)
            cumulative = cumulative + jnp.where(token >= shift, moved, 0.0)
            shift *= 2
        grown = jnp.exp(cumulative)
        grown_ref[...] = grown
        solved_u = beta * tokens(jax.nn.silu(cols(2)))
        solved_p = beta * grown * keys
        for at in range(steps):
            causal = token >= at
            gap = jnp.where(causal, cumulative - cumulative[:, at : at + 1, :], 0.0)
            decay = jnp.where(causal, jnp.exp(gap), 0.0)
            key_row = keys[:, at : at + 1, :]
            pair = jnp.concatenate([queries * key_row, keys * key_row], axis=2)
            dots = bf16_dot(pair.reshape(rows, 2 * LANES).astype(bf16), ones)
            qk_ref[at] = tokens(dots[:, :LANES]) * decay
            if at < steps - 1:
                a_col = jnp.where(token > at, beta * decay * tokens(dots[:, LANES:]), 0.0)
                solved_u = solved_u - a_col * solved_u[:, at : at + 1, :]
                solved_p = solved_p - a_col * solved_p[:, at : at + 1, :]
        last = cumulative[:, steps - 1 : steps, :]
        faded = keys * jnp.exp(last - cumulative)

        def scattered(matrix):
            placed = bf16_dot(matrix.reshape(-1, LANES).astype(bf16), perm)
            blocks = [placed[:, at * LANES : (at + 1) * LANES] for at in range(4)]
            return [block.reshape(seqs, -1, LANES) for block in blocks]

        for at, block in enumerate(scattered(jnp.concatenate([queries, solved_p], axis=1))):
            xq_ref[:, at * 2 * steps : (at + 1) * 2 * steps, :] = block.astype(bf16)
        blocks = scattered(faded)
        for at in (0, 2):
            both = jnp.concatenate([blocks[at], blocks[at + 1]], axis=1).astype(bf16)
            kd_ref[:, at * steps : (at + 2) * steps, :] = both
            kd_ref[:, (at + 4) * steps : (at + 6) * steps, :] = both
        u_ref[...] = solved_u
        fade = jnp.broadcast_to(jnp.exp(last), (seqs, steps, LANES))
        lane = lax.broadcasted_iota(jnp.int32, (seqs, steps, LANES), 2)
        kept = (token % 2 == 0) == (lane < HEAD_DIM)
        dec_ref[...] = jnp.where(kept, fade, pltpu.roll(fade, HEAD_DIM, axis=2))

    state_rows = state_ref.shape[2]

    def advance(slot, layer, chunk):
        pair_left = iota((2 * steps, LANES), 1) < HEAD_DIM
        left = iota((steps, LANES), 1) < HEAD_DIM

        def one_sequence(at, carry):
            state = state_ref[slot, at]
            read = bf16_dot(xq_ref[at, :, pl.ds(0, state_rows)], state.astype(bf16))
            parts = [read[2 * steps * b : 2 * steps * (b + 1)] for b in range(4)]
            straight = jnp.where(pair_left, parts[0], parts[3])
            crossed = jnp.where(pair_left, parts[2], parts[1])
            read = straight + pltpu.roll(crossed, HEAD_DIM, axis=1)
            qs_ref[at] = read[:steps]
            update = u_ref[at] - read[steps:]
            u_ref[at] = update
            high = update.astype(bf16).astype(f32)
            spread = []
            for part in (high, update - high):
                turned = pltpu.roll(part, HEAD_DIM, axis=1)
                spread += [
                    jnp.where(left, part, 0.0),
                    jnp.where(left, 0.0, turned),
                    jnp.where(left, turned, 0.0),
                    jnp.where(left, 0.0, part),
                ]
            grow = lax.dot_general(
                kd_ref[at, :, pl.ds(0, state_rows)],
                jnp.concatenate(spread, axis=0).astype(bf16),
                (((0,), (0,)), ((), ())),
                preferred_element_type=f32,
            )
            factor = jnp.concatenate([dec_ref[at]] * (state_rows // steps), axis=0)
            new_ref[layer, chunk * seqs + at] = factor * state + grow
            return carry

        lax.fori_loop(0, seqs, one_sequence, 0, unroll=8)

    def read_out(item, layer):
        update = u_ref[...]
        output = grown_ref[...] * qs_ref[...]
        for at in range(steps):
            output = output + qk_ref[at] * update[:, at : at + 1, :]
        output = output.reshape(rows, LANES)
        sums = head_sums(output * output, ones_ref[:LANES, :LANES])
        output = output * lax.rsqrt(sums * (1.0 / HEAD_DIM) + EPS)
        gain = read_gain_ref[pl.ds(layer, 1), :]
        y_ref[item, me] = (output * gain * jax.nn.silu(cols(3))).astype(bf16)

    def emit(item):
        whole = jnp.concatenate([y_ref[item, origin] for origin in range(count)], axis=1)
        return bf16_dot(whole, wo_ref[item // chunks]).astype(bf16)

    def emit_middle(item):
        in_ref[item + chunks, me] = emit(item)

    def emit_last(item):
        mixed = emit(item)
        chunk = item - chunks
        mown_ref[chunk] = mixed
        wide = mixed.astype(f32)
        total = jnp.sum(squares(wide), axis=1, keepdims=True)
        sq_ref[chunk, me] = jnp.broadcast_to(total, (rows, LANES)).T[:1]

    def sums_begin(chunk):
        block = sq_ref.at[chunk, me]
        for step in range(1, count):
            remote(
                block, block, sq_sem.at[0, chunk], sq_sem.at[1, chunk], lax.rem(me + step, count)
            ).start()

    def sums_all(chunk):
        part = sq_ref.at[chunk, pl.ds(0, count - 1)]
        return remote(part, part, sq_sem.at[0, chunk], sq_sem.at[1, chunk], twin)

    def finish(chunk):
        sums_all(chunk).wait_recv()
        total = sq_ref[chunk, 0]
        for origin in range(1, count):
            total = total + sq_ref[chunk, origin]
        total = jnp.broadcast_to(total, (LANES, rows)).T
        scale = lax.rsqrt(total * (1.0 / D) + EPS)
        for half in range(width // LANES):
            at = pl.ds(half * LANES, LANES)
            gain = post_gain_ref[1:2, pl.ds(pl.multiple_of(me * width + half * LANES, LANES), LANES)]
            before = xown_ref[chunk, :, at].astype(f32)
            mixed = mown_ref[chunk, :, at].astype(f32)
            out_ref[pl.ds(chunk * rows, rows), at] = (before + mixed * scale * gain).astype(bf16)

    def slot_of(slot, carry):
        (layer, chunk), buffer = place(slot), lax.rem(slot, 2)
        item = layer * chunks + chunk
        first = layer == 0
        when(slot + 1 < items, lambda: state_load(slot + 1).start())
        when(first & (chunk + 3 < chunks), lambda: begin_x(chunk + 3))
        complete(in_ref, in_sem, item)

        @pl.when(first)
        def _():
            own_copy(chunk).wait()
            first_hidden(chunk)

        when(layer == 1, second_hidden, item)
        proj_ref[...] = bf16_dot(h_ref[...], w_ref[layer]).astype(bf16)

        def older(by):
            return item_at(slot - by)

        def mixed(by):
            return (slot >= by) & (place(slot - by)[0] == 0)

        when(mixed(5), relay_near, in_ref, in_sem, older(5) + chunks)
        when(slot == 0, relay_near, in_ref, in_sem, 1)
        when(slot >= 2, relay_far, y_ref, y_sem, older(2))
        when(mixed(6), relay_twin, in_ref, in_sem, older(6) + chunks)
        prepare(layer, chunk)
        when(first & (chunk + 2 < chunks), relay_near, in_ref, in_sem, chunk + 2)
        when(slot == 0, relay_far, in_ref, in_sem, 1)
        state_load(slot).wait()
        advance(buffer, layer, chunk)
        when(mixed(5), relay_far, in_ref, in_sem, older(5) + chunks)
        when(slot >= 1, relay_near, y_ref, y_sem, older(1))
        when(first & (chunk + 2 < chunks), relay_far, in_ref, in_sem, chunk + 2)
        when(slot >= 2, relay_twin, y_ref, y_sem, older(2))
        read_out(item, layer)
        past, (past_layer, past_chunk) = older(3), place(slot - 3)
        when(slot >= 3, complete, y_ref, y_sem, past)
        begin(y_ref, y_sem, item, y_ref.at[item, me])
        early = (slot >= 3) & (past_layer == 0)
        late = (slot >= 3) & (past_layer == 1)
        when(early, emit_middle, past)
        when(late, emit_last, past)
        when(first & (chunk + 1 < chunks), relay_twin, in_ref, in_sem, chunk + 1)

        @pl.when(early)
        def _():
            begin(in_ref, in_sem, past + chunks, in_ref.at[past + chunks, me])

        when(late, sums_begin, past_chunk)
        return carry

    lax.fori_loop(0, items, slot_of, 0)
    final = items - 1
    relay_far(y_ref, y_sem, final - 1)
    complete(y_ref, y_sem, final - 2)
    emit_last(final - 2)
    relay_near(y_ref, y_sem, final)
    relay_twin(y_ref, y_sem, final - 1)
    sums_begin(chunks - 3)
    for chunk in range(chunks - 4):
        finish(chunk)
    relay_far(y_ref, y_sem, final)
    complete(y_ref, y_sem, final - 1)
    emit_last(final - 1)
    finish(chunks - 4)
    sums_begin(chunks - 2)
    relay_twin(y_ref, y_sem, final)
    for item in range(items):
        drained(in_ref, in_sem, item)
        if item < final:
            drained(y_ref, y_sem, item)
    complete(y_ref, y_sem, final)
    emit_last(final)
    drained(y_ref, y_sem, final)
    sums_begin(chunks - 1)
    for chunk in range(chunks - 3, chunks):
        finish(chunk)
    for chunk in range(chunks):
        sums_all(chunk).wait_send()


def deliver_kernel(first_ref, second_ref, first_hbm, second_hbm, sem):
    layers, parts = second_ref.shape[0], 4
    size = second_ref.shape[1] // parts
    copies = [pltpu.make_async_copy(first_ref, first_hbm, sem.at[layers * parts])]
    for layer in range(layers):
        for part in range(parts):
            at = pl.ds(part * size, size)
            copies.append(
                pltpu.make_async_copy(
                    second_ref.at[layer, at],
                    second_hbm.at[layer, at],
                    sem.at[layer * parts + part],
                )
            )
    for copy in copies:
        copy.start()
    for copy in copies:
        copy.wait()


def deliver(first, second):
    hbm = pl.BlockSpec(memory_space=pl.ANY)
    return pl.pallas_call(
        deliver_kernel,
        out_shape=[
            jax.ShapeDtypeStruct(first.shape, first.dtype),
            jax.ShapeDtypeStruct(second.shape, second.dtype),
        ],
        in_specs=[hbm, hbm],
        out_specs=[hbm, hbm],
        scratch_shapes=[pltpu.SemaphoreType.DMA((4 * second.shape[0] + 1,))],
        compiler_params=pltpu.CompilerParams(vmem_limit_bytes=1024 * 1024),
        name="deliver",
    )(first, second)


def local_two_heads(
    residual_channel,
    prior_block_multiplier,
    probe_map_matrix,
    lookup_map_matrix,
    content_map_matrix,
    emission_valve_matrix,
    forgetting_map_matrix,
    insertion_rate_matrix,
    forgetting_magnitude_exponent,
    channel_forgetting_offset,
    surplus_forgetting_amounts,
    readout_rescale_multiplier,
    emission_map_matrix,
    post_mixing_multiplier,
    recurrent_matrices,
):
    batch_total, steps, own_width = residual_channel.shape
    layers, _, head_count, state_size = recurrent_matrices.shape
    row_count = batch_total * steps
    count = lax.axis_size("tp")
    groups = state_size // LANES
    chunks = CHUNKS
    seqs, rows = batch_total // chunks, row_count // chunks
    heads = forgetting_map_matrix.shape[2]
    features = forgetting_map_matrix.shape[1]
    mix_width = emission_map_matrix.shape[1]
    states = (
        recurrent_matrices.reshape(layers, batch_total, head_count, groups, LANES)
        .transpose(0, 1, 3, 2, 4)
        .reshape(layers, batch_total, groups * head_count, LANES)
    )
    f32, bf16 = jnp.float32, jnp.bfloat16
    dma = pltpu.SemaphoreType.DMA
    hbm = pl.BlockSpec(memory_space=pl.ANY)
    vmem = pl.BlockSpec(memory_space=pltpu.VMEM)
    tile = (seqs, steps, LANES)
    state_tile = (2, seqs, groups * head_count, LANES)
    current, new_memory = pl.pallas_call(
        lambda *refs: step_kernel(count, chunks, *refs),
        out_shape=[
            pltpu.VMEM((row_count, own_width), bf16),
            pltpu.VMEM(states.shape, f32),
        ],
        in_specs=[hbm] * 15,
        out_specs=[vmem, vmem],
        scratch_shapes=[
            pltpu.VMEM((2 * chunks, count, rows, own_width), bf16),
            pltpu.VMEM((2 * chunks, count, rows, LANES), bf16),
            pltpu.VMEM((layers, features, 5 * LANES), bf16),
            pltpu.VMEM((layers, mix_width, own_width), bf16),
            pltpu.VMEM((layers, 2 * heads, features), bf16),
            pltpu.VMEM((rows, features), bf16),
            pltpu.VMEM((count, rows, own_width), bf16),
            pltpu.VMEM((chunks, rows, own_width), bf16),
            pltpu.VMEM((chunks, rows, own_width), bf16),
            pltpu.VMEM((chunks, count, 1, rows), f32),
            pltpu.VMEM((layers, batch_total, steps, LANES), f32),
            pltpu.VMEM(state_tile, f32),
            pltpu.VMEM((rows, 5 * LANES), bf16),
            pltpu.VMEM(tile, f32),
            pltpu.VMEM((steps,) + tile, f32),
            pltpu.VMEM((seqs, 8 * steps, LANES), bf16),
            pltpu.VMEM((seqs, 8 * steps, LANES), bf16),
            pltpu.VMEM(tile, f32),
            pltpu.VMEM(tile, f32),
            pltpu.VMEM(tile, f32),
            pltpu.VMEM((2 * heads, 2 * LANES), bf16),
            pltpu.VMEM((2 * LANES, 2 * LANES), bf16),
            pltpu.VMEM((LANES, 4 * LANES), bf16),
            pltpu.VMEM((layers, steps, head_count, batch_total), f32),
            pltpu.VMEM((layers, features), f32),
            pltpu.VMEM((layers, features), f32),
            pltpu.VMEM((layers, LANES), f32),
            pltpu.SMEM((layers, head_count), f32),
            pltpu.SMEM((layers, head_count), f32),
            dma((20,)),
            dma((2,)),
            dma((chunks,)),
            dma((3 + count // 4, 2 * chunks)),
            dma((3 + count // 4, 2 * chunks)),
            dma((2, chunks)),
        ],
        compiler_params=pltpu.CompilerParams(
            collective_id=1, has_side_effects=True, vmem_limit_bytes=46 * 1024 * 1024
        ),
        name="step",
    )(
        residual_channel.reshape(row_count, own_width),
        probe_map_matrix,
        lookup_map_matrix,
        content_map_matrix,
        emission_valve_matrix,
        forgetting_map_matrix.transpose(0, 2, 1),
        insertion_rate_matrix.transpose(0, 2, 1),
        emission_map_matrix,
        states,
        surplus_forgetting_amounts.transpose(0, 2, 3, 1),
        prior_block_multiplier,
        post_mixing_multiplier,
        readout_rescale_multiplier,
        forgetting_magnitude_exponent,
        channel_forgetting_offset,
    )
    current, new_memory = deliver(current, new_memory)
    new_memory = (
        new_memory.reshape(layers, batch_total, groups, head_count, LANES)
        .transpose(0, 1, 3, 2, 4)
        .reshape(recurrent_matrices.shape)
    )
    return current.reshape(batch_total, steps, own_width), new_memory


def local_any(*arrays):
    residual_channel, recurrent_matrices = arrays[0], arrays[-1]
    two_heads = (
        recurrent_matrices.shape[2] * HEAD_DIM == LANES
        and residual_channel.shape[1] == 8
        and residual_channel.shape[0] % (8 * CHUNKS) == 0
        and residual_channel.shape[2] % LANES == 0
        and lax.axis_size("tp") == 16
    )
    return (local_two_heads if two_heads else local)(*arrays)


def solution(mesh):
    return jax.shard_map(
        local_any,
        mesh=mesh,
        in_specs=(
            P("grp", None, "tp"),
            P(),
            P(None, None, "tp"),
            P(None, None, "tp"),
            P(None, None, "tp"),
            P(None, None, "tp"),
            P(),
            P(),
            P(None, "tp"),
            P(None, "tp"),
            P(None, "grp", None, "tp"),
            P(None, "tp"),
            P(None, None, "tp"),
            P(),
            P(None, "grp", "tp", None),
        ),
        out_specs=(P("grp", None, "tp"), P(None, "grp", "tp", None)),
        check_vma=False,
    )
```

```python
import jax
import jax.numpy as jnp
from jax import lax
from jax.experimental import pallas as pl
from jax.experimental.pallas import tpu as pltpu
from jax.sharding import PartitionSpec as P

D = 4096
HEAD_DIM = 64
LAYERS = 2


EPS = 1e-06
HIGH = lax.Precision.HIGHEST


def solve_lower(a_mat, right_side):
    length = right_side.shape[-2]
    solved_rows = []
    for row_at in range(length):
        current_row = right_side[..., row_at, :]
        for col_at in range(row_at):
            current_row = current_row - a_mat[..., row_at, col_at][..., None] * solved_rows[col_at]
        solved_rows.append(current_row)
    return jnp.stack(solved_rows, axis=-2)


def delta_block(queries, key_rows, values, forgetting_exponent_amount, strength, matrix_state):
    length = queries.shape[2]
    causal = jnp.tril(jnp.ones((length, length), bool))
    strict = jnp.tril(jnp.ones((length, length), bool), -1)
    cumulative = jnp.cumsum(forgetting_exponent_amount, axis=-1)
    decay_mat = jnp.where(
        causal,
        jnp.exp(jnp.where(causal, cumulative[..., :, None] - cumulative[..., None, :], 0.0)),
        0.0,
    )
    key_gram = jnp.einsum("bhtd,bhsd->bhts", key_rows, key_rows, precision=HIGH)
    a_mat = jnp.where(strict, strength[..., :, None] * decay_mat * key_gram, 0.0)
    right_side = jnp.concatenate(
        [strength[..., None] * values, (strength * jnp.exp(cumulative))[..., None] * key_rows],
        axis=-1,
    )
    solved = solve_lower(a_mat, right_side)
    width_v = values.shape[-1]
    update = solved[..., :width_v] - jnp.einsum(
        "bhtk,bhkv->bhtv", solved[..., width_v:], matrix_state, precision=HIGH
    )
    scores = jnp.einsum("bhtd,bhsd->bhts", queries, key_rows, precision=HIGH) * decay_mat
    output = jnp.exp(cumulative)[..., None] * jnp.einsum(
        "bhtk,bhkv->bhtv", queries, matrix_state, precision=HIGH
    )
    output = output + jnp.einsum("bhts,bhsv->bhtv", scores, update, precision=HIGH)
    final_log = cumulative[..., -1:]
    revised_memory_matrix = jnp.exp(final_log)[..., None] * matrix_state + jnp.einsum(
        "bhsk,bhsv->bhkv",
        key_rows * jnp.exp(final_log - cumulative)[..., None],
        update,
        precision=HIGH,
    )
    return (output, revised_memory_matrix)


def unit_rows(matrix):
    return matrix * lax.rsqrt(jnp.sum(matrix * matrix, axis=-1, keepdims=True) + EPS)


def token_blender(
    mapped_token_vectors,
    magnitude_exponent,
    offset_terms_array,
    surplus_forgetting_exponent,
    multiplier_terms_array,
    incoming_memory_matrix,
    batch_total,
    generation_round_total,
):
    rounded = [
        lax.optimization_barrier(part_sum.astype(jnp.bfloat16)).astype(jnp.float32)
        for part_sum in mapped_token_vectors
    ]
    queries, keys_raw, values_raw, gate_raw, decay_pre, strength_pre = rounded
    head_count = incoming_memory_matrix.shape[1]

    def to_heads(matrix):
        return matrix.reshape(batch_total, generation_round_total, head_count, HEAD_DIM).transpose(
            0, 2, 1, 3
        )

    def per_head(matrix):
        return matrix.reshape(batch_total, generation_round_total, head_count).transpose(0, 2, 1)

    queries = unit_rows(jax.nn.silu(to_heads(queries))) * HEAD_DIM ** (-0.5)
    key_rows = unit_rows(jax.nn.silu(to_heads(keys_raw)))
    values = jax.nn.silu(to_heads(values_raw))
    forgetting_exponent_amount = -jnp.exp(magnitude_exponent)[None, :, None] * jax.nn.softplus(
        per_head(decay_pre) + offset_terms_array[None, :, None]
    )
    forgetting_exponent_amount = forgetting_exponent_amount + surplus_forgetting_exponent.transpose(
        0, 2, 1
    )
    strength = jax.nn.sigmoid(per_head(strength_pre))
    matrix_state = incoming_memory_matrix.reshape(batch_total, head_count, HEAD_DIM, HEAD_DIM)
    output, revised_memory_matrix = delta_block(
        queries, key_rows, values, forgetting_exponent_amount, strength, matrix_state
    )
    normed = output * lax.rsqrt(jnp.mean(output * output, axis=-1, keepdims=True) + EPS)
    normed = (
        normed
        * multiplier_terms_array.reshape(head_count, HEAD_DIM)[None, :, None, :]
        * jax.nn.silu(to_heads(gate_raw))
    )
    blended_token_vectors = (
        normed.transpose(0, 2, 1, 3)
        .reshape(batch_total * generation_round_total, head_count * HEAD_DIM)
        .astype(jnp.bfloat16)
    )
    return (
        blended_token_vectors,
        revised_memory_matrix.reshape(batch_total, head_count, HEAD_DIM * HEAD_DIM),
    )


LANES = 128


def bf16_dot(left, right):
    return jnp.dot(left, right, preferred_element_type=jnp.float32)


def head_sums(squares, ones):
    high = squares.astype(jnp.bfloat16)
    low = (squares - high.astype(jnp.float32)).astype(jnp.bfloat16)
    return bf16_dot(high, ones) + bf16_dot(low, ones)


def project(portion, weights):
    return tuple(
        (jnp.dot(portion, weight, preferred_element_type=jnp.float32) for weight in weights)
    )


def out_project(blended_token_vectors, weight_rows):
    return jnp.dot(
        lax.all_gather(blended_token_vectors, "tp", axis=1, tiled=True),
        weight_rows,
        preferred_element_type=jnp.float32,
    ).astype(jnp.bfloat16)


def post_residual(widened, mixed_out, multiplier_terms_array, complete):
    mixed_wide = lax.optimization_barrier(mixed_out).astype(jnp.float32)
    squares = jnp.sum(mixed_wide * mixed_wide, axis=-1)
    if not complete:
        squares = lax.psum(squares, "tp")
    post_rms = lax.rsqrt(squares / D + EPS)[:, None]
    return lax.optimization_barrier(
        (widened + mixed_wide * post_rms * multiplier_terms_array).astype(jnp.bfloat16)
    )


def local(
    residual_channel,
    prior_block_multiplier,
    probe_map_matrix,
    lookup_map_matrix,
    content_map_matrix,
    emission_valve_matrix,
    forgetting_map_matrix,
    insertion_rate_matrix,
    forgetting_magnitude_exponent,
    channel_forgetting_offset,
    surplus_forgetting_amounts,
    readout_rescale_multiplier,
    emission_map_matrix,
    post_mixing_multiplier,
    recurrent_matrices,
):
    batch_total, generation_round_total, own_width = residual_channel.shape
    head_count = recurrent_matrices.shape[2]
    row_count = batch_total * generation_round_total
    col_offset = lax.axis_index("tp") * own_width
    head_offset = lax.axis_index("tp") * head_count
    new_states = []

    def mix_layer(mapped_token_vectors, block_index_number):
        blended_token_vectors, revised_memory_matrix = token_blender(
            mapped_token_vectors,
            forgetting_magnitude_exponent[block_index_number],
            channel_forgetting_offset[block_index_number],
            surplus_forgetting_amounts[block_index_number],
            readout_rescale_multiplier[block_index_number],
            recurrent_matrices[block_index_number],
            batch_total,
            generation_round_total,
        )
        new_states.append(revised_memory_matrix)
        return out_project(blended_token_vectors, emission_map_matrix[block_index_number])

    def own_cols(matrix):
        return lax.dynamic_slice_in_dim(matrix, col_offset, own_width, matrix.ndim - 1)

    whole_rows = lax.all_gather(
        residual_channel.reshape(row_count, own_width), "tp", axis=1, tiled=True
    )
    current = whole_rows
    for block_index_number in range(LAYERS):
        widened = whole_rows.astype(jnp.float32)
        inv_rms = lax.rsqrt(jnp.mean(widened * widened, axis=-1, keepdims=True) + EPS)
        hidden = (widened * inv_rms * prior_block_multiplier[block_index_number]).astype(
            jnp.bfloat16
        )
        weights = (
            probe_map_matrix[block_index_number],
            lookup_map_matrix[block_index_number],
            content_map_matrix[block_index_number],
            emission_valve_matrix[block_index_number],
            lax.dynamic_slice_in_dim(
                forgetting_map_matrix[block_index_number], head_offset, head_count, 1
            ),
            lax.dynamic_slice_in_dim(
                insertion_rate_matrix[block_index_number], head_offset, head_count, 1
            ),
        )
        mapped_token_vectors = project(hidden, weights)
        mixed_out = mix_layer(mapped_token_vectors, block_index_number)
        if block_index_number < LAYERS - 1:
            gathered = lax.all_gather(mixed_out, "tp", axis=1, tiled=True)
            whole_rows = post_residual(
                widened, gathered, post_mixing_multiplier[block_index_number], True
            )
        else:
            current = post_residual(
                own_cols(widened),
                mixed_out,
                own_cols(post_mixing_multiplier[block_index_number]),
                False,
            )
    return (
        current.reshape(batch_total, generation_round_total, own_width),
        jnp.stack(new_states, axis=0),
    )


CHUNKS = 8
GROUP_ROWS = 64


def step_kernel(
    count,
    chunks,
    x_hbm,
    probe_hbm,
    lookup_hbm,
    content_hbm,
    valve_hbm,
    forget_hbm,
    insert_hbm,
    emission_hbm,
    states_hbm,
    surplus_hbm,
    pre_gain_hbm,
    post_gain_hbm,
    read_gain_hbm,
    magnitude_hbm,
    offset_hbm,
    out_ref,
    new_ref,
    in_ref,
    y_ref,
    w_ref,
    wo_ref,
    rates_ref,
    h_ref,
    x1_ref,
    xown_ref,
    mown_ref,
    sq_ref,
    sur_ref,
    state_ref,
    proj_ref,
    grown_ref,
    qk_ref,
    xq_ref,
    kd_ref,
    u_ref,
    qs_ref,
    dec_ref,
    spread_ref,
    ones_ref,
    perm_ref,
    surplus_ref,
    pre_gain_ref,
    post_gain_ref,
    read_gain_ref,
    magnitude_ref,
    offset_ref,
    load_sem,
    state_sem,
    own_sem,
    in_sem,
    y_sem,
    sq_sem,
):
    f32, bf16 = jnp.float32, jnp.bfloat16
    me = lax.axis_index("tp")
    depth = count // 4
    core, row, line = lax.rem(me, 2), lax.rem(me // 2, 2), me // 4
    over, twin = me + 2 - 4 * row, me + 1 - 2 * core
    items = 2 * chunks
    rows = h_ref.shape[0]
    seqs, steps = qk_ref.shape[1], qk_ref.shape[2]
    width = in_ref.shape[3]
    heads = forget_hbm.shape[1]
    own_heads = heads // count

    barrier = pltpu.get_barrier_semaphore()
    inner = (line == 1) | (line == 2)
    shifts = (0, 1 - 2 * lax.rem(line, 2), 2 - 4 * (line // 2), 3 - 2 * line)

    def along(step):
        return 4 * shifts[step]

    def when(condition, action, *operands):
        @pl.when(condition)
        def _():
            action(*operands)

    def greet(device):
        pl.semaphore_signal(
            barrier, inc=1, device_id={"tp": device}, device_id_type=pl.DeviceIdType.MESH
        )

    for device in (over, twin, me + along(1), me + along(2)):
        greet(device)
    when(inner, greet, me + along(3))

    loads = []
    for layer in range(2):
        for at, matrix in enumerate((probe_hbm, lookup_hbm, content_hbm, valve_hbm)):
            loads.append(
                (matrix.at[layer], w_ref.at[layer, :, pl.ds(at * LANES, LANES)])
            )
        loads.append((forget_hbm.at[layer], rates_ref.at[layer, pl.ds(0, heads), :]))
        loads.append((insert_hbm.at[layer], rates_ref.at[layer, pl.ds(heads, heads), :]))
        loads.append((emission_hbm.at[layer], wo_ref.at[layer]))
    loads += [
        (surplus_hbm, surplus_ref),
        (pre_gain_hbm, pre_gain_ref),
        (post_gain_hbm, post_gain_ref),
        (read_gain_hbm, read_gain_ref),
        (magnitude_hbm, magnitude_ref),
        (offset_hbm, offset_ref),
    ]
    loads = [
        pltpu.make_async_copy(source, target, load_sem.at[at])
        for at, (source, target) in enumerate(loads)
    ]
    for copy in loads:
        copy.start()

    def state_load(slot):
        layer, chunk = slot // chunks, lax.rem(slot, chunks)
        return pltpu.make_async_copy(
            states_hbm.at[layer, pl.ds(chunk * seqs, seqs)],
            state_ref.at[lax.rem(slot, 2)],
            state_sem.at[lax.rem(slot, 2)],
        )

    state_load(0).start()

    pl.semaphore_wait(barrier, 4 + lax.rem((line + 1) // 2, 2))

    def remote(source, target, send_sem, land_sem, device):
        return pltpu.make_async_remote_copy(
            src_ref=source,
            dst_ref=target,
            send_sem=send_sem,
            recv_sem=land_sem,
            device_id={"tp": device},
            device_id_type=pl.DeviceIdType.MESH,
        )

    def begin(buf, sems, item, source):
        target = buf.at[item, me]

        def out(kind, device):
            remote(source, target, sems.at[0, item], sems.at[kind, item], device).start()

        out(5, me + along(2))
        out(4, me + along(1))
        when(inner, out, 6, me + along(3))
        out(1, over)
        out(3, twin)

    def pass_on(buf, sems, item, origin, kind, device, half=None):
        block = buf.at[item, origin]
        if half is not None:
            block = buf.at[item, origin, pl.ds(half * (rows // 2), rows // 2)]
        remote(block, block, sems.at[0, item], sems.at[kind, item], device).start()

    def landed(buf, sems, item, kind, blocks):
        part = buf.at[item, pl.ds(0, blocks)]
        remote(part, part, sems.at[0, item], sems.at[kind, item], twin).wait_recv()

    def relay_near(buf, sems, item):
        landed(buf, sems, item, 5, 1)
        when(inner, pass_on, buf, sems, item, me + along(2), 6, me + along(1))
        pass_on(buf, sems, item, me + along(2), 2, over)
        pass_on(buf, sems, item, me + along(2), 3, twin)
        landed(buf, sems, item, 1, 1)
        pass_on(buf, sems, item, over, 2, me + along(1), 0)
        pass_on(buf, sems, item, over, 3, twin)
        landed(buf, sems, item, 4, 1)
        pass_on(buf, sems, item, me + along(1), 2, over, 1)
        pass_on(buf, sems, item, me + along(1), 3, twin)

    def relay_far(buf, sems, item):
        landed(buf, sems, item, 6, 1)
        pass_on(buf, sems, item, me + along(3), 2, over)
        pass_on(buf, sems, item, me + along(3), 3, twin)

    def relay_twin(buf, sems, item):
        landed(buf, sems, item, 2, depth - 1)
        for step in range(1, depth):
            pass_on(buf, sems, item, over + along(step), 3, twin)

    def complete(buf, sems, item):
        landed(buf, sems, item, 3, 2 * depth)

    def drained(buf, sems, item):
        def sent(blocks):
            part = buf.at[item, pl.ds(0, blocks)]
            remote(part, part, sems.at[0, item], sems.at[1, item], twin).wait_send()

        when(inner, sent, count)
        when(jnp.logical_not(inner), sent, count - 2)

    def own_copy(item):
        return pltpu.make_async_copy(
            x_hbm.at[pl.ds(item * rows, rows), :], in_ref.at[item, me], own_sem.at[item]
        )

    def begin_x(item):
        begin(in_ref, in_sem, item, x_hbm.at[pl.ds(item * rows, rows), :])
        own_copy(item).start()

    begin_x(0)

    def iota(shape, axis):
        return lax.broadcasted_iota(jnp.int32, shape, axis)

    shape = (2 * heads, 2 * LANES)
    wanted = iota(shape, 1) // HEAD_DIM
    wanted = jnp.where(wanted >= 2, wanted - 2 + heads, wanted) + me * own_heads
    spread_ref[...] = jnp.where(iota(shape, 0) == wanted, 1.0, 0.0).astype(bf16)
    shape = (2 * LANES, 2 * LANES)
    ones_ref[...] = jnp.where(
        iota(shape, 0) // HEAD_DIM == iota(shape, 1) // HEAD_DIM, 1.0, 0.0
    ).astype(bf16)
    shape = (LANES, 4 * LANES)
    block, spot = iota(shape, 1) // LANES, iota(shape, 1) % LANES
    target = (block // 2) * HEAD_DIM + 2 * (spot // 2) + block % 2
    fits = (iota(shape, 0) == target) & (spot % 2 == block // 2) & (spot < HEAD_DIM)
    perm_ref[...] = jnp.where(fits, 1.0, 0.0).astype(bf16)
    for copy in loads:
        copy.wait()
    all_seqs = sur_ref.shape[1]
    first_head = iota((LANES, all_seqs), 0) < HEAD_DIM
    for layer in range(2):
        for step in range(steps):
            pair = surplus_ref[layer, step]
            wide = jnp.where(first_head, pair[0:1, :], pair[1:2, :])
            sur_ref[layer, :, step, :] = wide.T
        for origin in range(count):
            at = pl.ds(origin * width, width)
            pair = rates_ref[layer, :, at].astype(f32)
            padded = jnp.concatenate([pair, jnp.zeros((LANES - 2 * heads, width), f32)], axis=0)
            w_ref[layer, at, pl.ds(4 * LANES, LANES)] = padded.T.astype(bf16)

    relay_near(in_ref, in_sem, 0)
    relay_far(in_ref, in_sem, 0)
    begin_x(1)
    relay_twin(in_ref, in_sem, 0)
    begin_x(2)

    def squares(matrix):
        return matrix[:, :LANES] * matrix[:, :LANES] + matrix[:, LANES:] * matrix[:, LANES:]

    def inverse(total):
        return lax.rsqrt(jnp.sum(total, axis=1, keepdims=True) * (1.0 / D) + EPS)

    def cols_of(origin):
        return pl.ds(origin * width, width)

    def first_hidden(item):
        def part(group, carry):
            at = pl.ds(group * GROUP_ROWS, GROUP_ROWS)
            total = jnp.zeros((GROUP_ROWS, LANES), f32)
            for origin in range(count):
                total = total + squares(in_ref[item, origin, at, :].astype(f32))
            scale = inverse(total)
            for origin in range(count):
                block = in_ref[item, origin, at, :].astype(f32)
                gain = pre_gain_ref[0:1, cols_of(origin)]
                h_ref[at, cols_of(origin)] = (block * scale * gain).astype(bf16)
            return carry

        lax.fori_loop(0, rows // GROUP_ROWS, part, 0)

    def second_hidden(item):
        earlier = item - chunks

        def part(group, carry):
            at = pl.ds(group * GROUP_ROWS, GROUP_ROWS)
            total = jnp.zeros((GROUP_ROWS, LANES), f32)
            for origin in range(count):
                total = total + squares(in_ref[item, origin, at, :].astype(f32))
            scale = inverse(total)
            total = jnp.zeros((GROUP_ROWS, LANES), f32)
            for origin in range(count):
                mixed = in_ref[item, origin, at, :].astype(f32)
                before = in_ref[earlier, origin, at, :].astype(f32)
                gain = post_gain_ref[0:1, cols_of(origin)]
                after = (before + mixed * scale * gain).astype(bf16)
                x1_ref[origin, at, :] = after
                total = total + squares(after.astype(f32))
            scale = inverse(total)
            for origin in range(count):
                block = x1_ref[origin, at, :].astype(f32)
                gain = pre_gain_ref[1:2, cols_of(origin)]
                h_ref[at, cols_of(origin)] = (block * scale * gain).astype(bf16)
            xown_ref[earlier, at, :] = x1_ref[me, at, :]
            return carry

        lax.fori_loop(0, rows // GROUP_ROWS, part, 0)

    def cols(at):
        return proj_ref[:, at * LANES : (at + 1) * LANES].astype(f32)

    def tokens(matrix):
        return matrix.reshape(seqs, steps, LANES)

    def lane_pair(ref, layer):
        left = iota((1, LANES), 1) < HEAD_DIM
        return jnp.where(left, ref[layer, 0], ref[layer, 1])

    def prepare(layer, chunk):
        ones = ones_ref[...]
        perm = perm_ref[...]
        queries = jax.nn.silu(cols(0))
        keys = jax.nn.silu(cols(1))
        sums = head_sums(jnp.concatenate([queries * queries, keys * keys], axis=1), ones)
        queries = tokens(queries * lax.rsqrt(sums[:, :LANES] + EPS) * HEAD_DIM ** (-0.5))
        keys = tokens(keys * lax.rsqrt(sums[:, LANES:] + EPS))
        spread = bf16_dot(proj_ref[:, 4 * LANES : 4 * LANES + 2 * heads], spread_ref[...])
        biased = spread[:, :LANES] + lane_pair(offset_ref, layer)
        softplus = jnp.maximum(biased, 0.0) + jnp.log1p(jnp.exp(-jnp.abs(biased)))
        pace = -jnp.exp(lane_pair(magnitude_ref, layer))
        cumulative = tokens(pace * softplus) + sur_ref[layer, pl.ds(chunk * seqs, seqs)]
        beta = tokens(jax.nn.sigmoid(spread[:, LANES:]))
        token = lax.broadcasted_iota(jnp.int32, (seqs, steps, LANES), 1)
        shift = 1
        while shift < steps:
            moved = pltpu.roll(cumulative, shift, axis=1)
            cumulative = cumulative + jnp.where(token >= shift, moved, 0.0)
            shift *= 2
        grown = jnp.exp(cumulative)
        grown_ref[...] = grown
        solved_u = beta * tokens(jax.nn.silu(cols(2)))
        solved_p = beta * grown * keys
        for at in range(steps):
            causal = token >= at
            gap = jnp.where(causal, cumulative - cumulative[:, at : at + 1, :], 0.0)
            decay = jnp.where(causal, jnp.exp(gap), 0.0)
            key_row = keys[:, at : at + 1, :]
            pair = jnp.concatenate([queries * key_row, keys * key_row], axis=2)
            dots = bf16_dot(pair.reshape(rows, 2 * LANES).astype(bf16), ones)
            qk_ref[at] = tokens(dots[:, :LANES]) * decay
            if at < steps - 1:
                a_col = jnp.where(token > at, beta * decay * tokens(dots[:, LANES:]), 0.0)
                solved_u = solved_u - a_col * solved_u[:, at : at + 1, :]
                solved_p = solved_p - a_col * solved_p[:, at : at + 1, :]
        last = cumulative[:, steps - 1 : steps, :]
        faded = keys * jnp.exp(last - cumulative)

        def scattered(matrix):
            placed = bf16_dot(matrix.reshape(-1, LANES).astype(bf16), perm)
            blocks = [placed[:, at * LANES : (at + 1) * LANES] for at in range(4)]
            return [block.reshape(seqs, -1, LANES) for block in blocks]

        for at, block in enumerate(scattered(jnp.concatenate([queries, solved_p], axis=1))):
            xq_ref[:, at * 2 * steps : (at + 1) * 2 * steps, :] = block.astype(bf16)
        blocks = scattered(faded)
        for at in (0, 2):
            both = jnp.concatenate([blocks[at], blocks[at + 1]], axis=1).astype(bf16)
            kd_ref[:, at * steps : (at + 2) * steps, :] = both
            kd_ref[:, (at + 4) * steps : (at + 6) * steps, :] = both
        u_ref[...] = solved_u
        fade = jnp.broadcast_to(jnp.exp(last), (seqs, steps, LANES))
        lane = lax.broadcasted_iota(jnp.int32, (seqs, steps, LANES), 2)
        kept = (token % 2 == 0) == (lane < HEAD_DIM)
        dec_ref[...] = jnp.where(kept, fade, pltpu.roll(fade, HEAD_DIM, axis=2))

    state_rows = state_ref.shape[2]

    def advance(slot, layer, chunk):
        pair_left = iota((2 * steps, LANES), 1) < HEAD_DIM
        left = iota((steps, LANES), 1) < HEAD_DIM

        def one_sequence(at, carry):
            state = state_ref[slot, at]
            read = bf16_dot(xq_ref[at, :, pl.ds(0, state_rows)], state.astype(bf16))
            parts = [read[2 * steps * b : 2 * steps * (b + 1)] for b in range(4)]
            straight = jnp.where(pair_left, parts[0], parts[3])
            crossed = jnp.where(pair_left, parts[2], parts[1])
            read = straight + pltpu.roll(crossed, HEAD_DIM, axis=1)
            qs_ref[at] = read[:steps]
            update = u_ref[at] - read[steps:]
            u_ref[at] = update
            high = update.astype(bf16).astype(f32)
            spread = []
            for part in (high, update - high):
                turned = pltpu.roll(part, HEAD_DIM, axis=1)
                spread += [
                    jnp.where(left, part, 0.0),
                    jnp.where(left, 0.0, turned),
                    jnp.where(left, turned, 0.0),
                    jnp.where(left, 0.0, part),
                ]
            grow = lax.dot_general(
                kd_ref[at, :, pl.ds(0, state_rows)],
                jnp.concatenate(spread, axis=0).astype(bf16),
                (((0,), (0,)), ((), ())),
                preferred_element_type=f32,
            )
            factor = jnp.concatenate([dec_ref[at]] * (state_rows // steps), axis=0)
            new_ref[layer, chunk * seqs + at] = factor * state + grow
            return carry

        lax.fori_loop(0, seqs, one_sequence, 0, unroll=8)

    def read_out(item, layer):
        update = u_ref[...]
        output = grown_ref[...] * qs_ref[...]
        for at in range(steps):
            output = output + qk_ref[at] * update[:, at : at + 1, :]
        output = output.reshape(rows, LANES)
        sums = head_sums(output * output, ones_ref[:LANES, :LANES])
        output = output * lax.rsqrt(sums * (1.0 / HEAD_DIM) + EPS)
        gain = read_gain_ref[pl.ds(layer, 1), :]
        y_ref[item, me] = (output * gain * jax.nn.silu(cols(3))).astype(bf16)

    def emit(item):
        whole = jnp.concatenate([y_ref[item, origin] for origin in range(count)], axis=1)
        return bf16_dot(whole, wo_ref[item // chunks]).astype(bf16)

    def emit_middle(item):
        in_ref[item + chunks, me] = emit(item)

    def emit_last(item):
        mixed = emit(item)
        chunk = item - chunks
        mown_ref[chunk] = mixed
        wide = mixed.astype(f32)
        total = jnp.sum(squares(wide), axis=1, keepdims=True)
        sq_ref[chunk, me] = jnp.broadcast_to(total, (rows, LANES)).T[:1]

    def sums_begin(chunk):
        block = sq_ref.at[chunk, me]
        for step in range(1, count):
            remote(
                block, block, sq_sem.at[0, chunk], sq_sem.at[1, chunk], lax.rem(me + step, count)
            ).start()

    def sums_all(chunk):
        part = sq_ref.at[chunk, pl.ds(0, count - 1)]
        return remote(part, part, sq_sem.at[0, chunk], sq_sem.at[1, chunk], twin)

    def finish(chunk):
        sums_all(chunk).wait_recv()
        total = sq_ref[chunk, 0]
        for origin in range(1, count):
            total = total + sq_ref[chunk, origin]
        total = jnp.broadcast_to(total, (LANES, rows)).T
        scale = lax.rsqrt(total * (1.0 / D) + EPS)
        for half in range(width // LANES):
            at = pl.ds(half * LANES, LANES)
            gain = post_gain_ref[1:2, pl.ds(pl.multiple_of(me * width + half * LANES, LANES), LANES)]
            before = xown_ref[chunk, :, at].astype(f32)
            mixed = mown_ref[chunk, :, at].astype(f32)
            out_ref[pl.ds(pl.multiple_of(chunk * rows, rows), rows), at] = (before + mixed * scale * gain).astype(bf16)

    hold = chunks + 3

    def slot_of(slot, carry):
        layer, chunk, buffer = slot // chunks, lax.rem(slot, chunks), lax.rem(slot, 2)
        busy, first = slot < items, slot < chunks

        def early(by):
            return (slot >= by) & (slot < by + chunks)

        def late(by, action, *operands):
            for side in (1, 0):
                at = 2 * (slot - by - hold) - side
                when((at >= 0) & (at < chunks), action, *operands, at + chunks)

        when(slot + 1 < items, lambda: state_load(slot + 1).start())
        when(slot + 3 < chunks, lambda: begin_x(slot + 3))
        when(busy, complete, in_ref, in_sem, slot)

        @pl.when(first)
        def _():
            own_copy(slot).wait()
            first_hidden(slot)

        when(busy & (slot >= chunks), second_hidden, slot)

        @pl.when(busy)
        def _():
            proj_ref[...] = bf16_dot(h_ref[...], w_ref[layer]).astype(bf16)

        when(early(6), relay_far, in_ref, in_sem, slot - 6 + chunks)
        when(slot == 0, relay_near, in_ref, in_sem, 1)
        when(early(2), relay_far, y_ref, y_sem, slot - 2)
        late(2, relay_far, y_ref, y_sem)
        when(early(7), relay_twin, in_ref, in_sem, slot - 7 + chunks)
        when(early(3), relay_twin, y_ref, y_sem, slot - 3)
        late(3, relay_twin, y_ref, y_sem)
        when(busy, prepare, layer, chunk)
        when(slot + 2 < chunks, relay_near, in_ref, in_sem, slot + 2)
        when(slot == 0, relay_far, in_ref, in_sem, 1)

        @pl.when(busy)
        def _():
            state_load(slot).wait()
            advance(buffer, layer, chunk)

        when(early(1), relay_near, y_ref, y_sem, slot - 1)
        when(early(5), relay_near, in_ref, in_sem, slot - 5 + chunks)
        late(1, relay_near, y_ref, y_sem)
        when(slot + 2 < chunks, relay_far, in_ref, in_sem, slot + 2)
        when(busy, read_out, slot, layer)
        when(early(3), complete, y_ref, y_sem, slot - 3)
        when(first, lambda: begin(y_ref, y_sem, slot, y_ref.at[slot, me]))
        when(early(3), emit_middle, slot - 3)
        late(3, complete, y_ref, y_sem)
        late(3, emit_last)
        when(slot + 1 < chunks, relay_twin, in_ref, in_sem, slot + 1)
        late(0, lambda item: begin(y_ref, y_sem, item, y_ref.at[item, me]))

        @pl.when(early(3))
        def _():
            made = slot - 3 + chunks
            begin(in_ref, in_sem, made, in_ref.at[made, me])

        late(3, lambda item: sums_begin(item - chunks))
        late(5, lambda item: finish(item - chunks))
        return carry

    lax.fori_loop(0, items + 3, slot_of, 0)

    def drain(item, carry):
        drained(in_ref, in_sem, item)
        drained(y_ref, y_sem, item)
        return carry

    lax.fori_loop(0, items, drain, 0)
    for chunk in range(chunks - 3, chunks):
        finish(chunk)
    for chunk in range(chunks):
        sums_all(chunk).wait_send()


def deliver_kernel(first_ref, second_ref, first_hbm, second_hbm, sem):
    layers, parts = second_ref.shape[0], 4
    size = second_ref.shape[1] // parts
    copies = [pltpu.make_async_copy(first_ref, first_hbm, sem.at[layers * parts])]
    for layer in range(layers):
        for part in range(parts):
            at = pl.ds(part * size, size)
            copies.append(
                pltpu.make_async_copy(
                    second_ref.at[layer, at],
                    second_hbm.at[layer, at],
                    sem.at[layer * parts + part],
                )
            )
    for copy in copies:
        copy.start()
    for copy in copies:
        copy.wait()


def deliver(first, second):
    hbm = pl.BlockSpec(memory_space=pl.ANY)
    return pl.pallas_call(
        deliver_kernel,
        out_shape=[
            jax.ShapeDtypeStruct(first.shape, first.dtype),
            jax.ShapeDtypeStruct(second.shape, second.dtype),
        ],
        in_specs=[hbm, hbm],
        out_specs=[hbm, hbm],
        scratch_shapes=[pltpu.SemaphoreType.DMA((4 * second.shape[0] + 1,))],
        compiler_params=pltpu.CompilerParams(vmem_limit_bytes=1024 * 1024),
        name="deliver",
    )(first, second)


def local_two_heads(
    residual_channel,
    prior_block_multiplier,
    probe_map_matrix,
    lookup_map_matrix,
    content_map_matrix,
    emission_valve_matrix,
    forgetting_map_matrix,
    insertion_rate_matrix,
    forgetting_magnitude_exponent,
    channel_forgetting_offset,
    surplus_forgetting_amounts,
    readout_rescale_multiplier,
    emission_map_matrix,
    post_mixing_multiplier,
    recurrent_matrices,
):
    batch_total, steps, own_width = residual_channel.shape
    layers, _, head_count, state_size = recurrent_matrices.shape
    row_count = batch_total * steps
    count = lax.axis_size("tp")
    groups = state_size // LANES
    chunks = CHUNKS
    seqs, rows = batch_total // chunks, row_count // chunks
    heads = forgetting_map_matrix.shape[2]
    features = forgetting_map_matrix.shape[1]
    mix_width = emission_map_matrix.shape[1]
    states = (
        recurrent_matrices.reshape(layers, batch_total, head_count, groups, LANES)
        .transpose(0, 1, 3, 2, 4)
        .reshape(layers, batch_total, groups * head_count, LANES)
    )
    f32, bf16 = jnp.float32, jnp.bfloat16
    dma = pltpu.SemaphoreType.DMA
    hbm = pl.BlockSpec(memory_space=pl.ANY)
    vmem = pl.BlockSpec(memory_space=pltpu.VMEM)
    tile = (seqs, steps, LANES)
    state_tile = (2, seqs, groups * head_count, LANES)
    current, new_memory = pl.pallas_call(
        lambda *refs: step_kernel(count, chunks, *refs),
        out_shape=[
            pltpu.VMEM((row_count, own_width), bf16),
            pltpu.VMEM(states.shape, f32),
        ],
        in_specs=[hbm] * 15,
        out_specs=[vmem, vmem],
        scratch_shapes=[
            pltpu.VMEM((2 * chunks, count, rows, own_width), bf16),
            pltpu.VMEM((2 * chunks, count, rows, LANES), bf16),
            pltpu.VMEM((layers, features, 5 * LANES), bf16),
            pltpu.VMEM((layers, mix_width, own_width), bf16),
            pltpu.VMEM((layers, 2 * heads, features), bf16),
            pltpu.VMEM((rows, features), bf16),
            pltpu.VMEM((count, rows, own_width), bf16),
            pltpu.VMEM((chunks, rows, own_width), bf16),
            pltpu.VMEM((chunks, rows, own_width), bf16),
            pltpu.VMEM((chunks, count, 1, rows), f32),
            pltpu.VMEM((layers, batch_total, steps, LANES), f32),
            pltpu.VMEM(state_tile, f32),
            pltpu.VMEM((rows, 5 * LANES), bf16),
            pltpu.VMEM(tile, f32),
            pltpu.VMEM((steps,) + tile, f32),
            pltpu.VMEM((seqs, 8 * steps, LANES), bf16),
            pltpu.VMEM((seqs, 8 * steps, LANES), bf16),
            pltpu.VMEM(tile, f32),
            pltpu.VMEM(tile, f32),
            pltpu.VMEM(tile, f32),
            pltpu.VMEM((2 * heads, 2 * LANES), bf16),
            pltpu.VMEM((2 * LANES, 2 * LANES), bf16),
            pltpu.VMEM((LANES, 4 * LANES), bf16),
            pltpu.VMEM((layers, steps, head_count, batch_total), f32),
            pltpu.VMEM((layers, features), f32),
            pltpu.VMEM((layers, features), f32),
            pltpu.VMEM((layers, LANES), f32),
            pltpu.SMEM((layers, head_count), f32),
            pltpu.SMEM((layers, head_count), f32),
            dma((20,)),
            dma((2,)),
            dma((chunks,)),
            dma((3 + count // 4, 2 * chunks)),
            dma((3 + count // 4, 2 * chunks)),
            dma((2, chunks)),
        ],
        compiler_params=pltpu.CompilerParams(
            collective_id=1, has_side_effects=True, vmem_limit_bytes=46 * 1024 * 1024
        ),
        name="step",
    )(
        residual_channel.reshape(row_count, own_width),
        probe_map_matrix,
        lookup_map_matrix,
        content_map_matrix,
        emission_valve_matrix,
        forgetting_map_matrix.transpose(0, 2, 1),
        insertion_rate_matrix.transpose(0, 2, 1),
        emission_map_matrix,
        states,
        surplus_forgetting_amounts.transpose(0, 2, 3, 1),
        prior_block_multiplier,
        post_mixing_multiplier,
        readout_rescale_multiplier,
        forgetting_magnitude_exponent,
        channel_forgetting_offset,
    )
    current, new_memory = deliver(current, new_memory)
    new_memory = (
        new_memory.reshape(layers, batch_total, groups, head_count, LANES)
        .transpose(0, 1, 3, 2, 4)
        .reshape(recurrent_matrices.shape)
    )
    return current.reshape(batch_total, steps, own_width), new_memory


def local_any(*arrays):
    residual_channel, recurrent_matrices = arrays[0], arrays[-1]
    two_heads = (
        recurrent_matrices.shape[2] * HEAD_DIM == LANES
        and residual_channel.shape[1] == 8
        and residual_channel.shape[0] % (8 * CHUNKS) == 0
        and residual_channel.shape[2] % LANES == 0
        and lax.axis_size("tp") == 16
    )
    return (local_two_heads if two_heads else local)(*arrays)


def solution(mesh):
    return jax.shard_map(
        local_any,
        mesh=mesh,
        in_specs=(
            P("grp", None, "tp"),
            P(),
            P(None, None, "tp"),
            P(None, None, "tp"),
            P(None, None, "tp"),
            P(None, None, "tp"),
            P(),
            P(),
            P(None, "tp"),
            P(None, "tp"),
            P(None, "grp", None, "tp"),
            P(None, "tp"),
            P(None, None, "tp"),
            P(),
            P(None, "grp", "tp", None),
        ),
        out_specs=(P("grp", None, "tp"), P(None, "grp", "tp", None)),
        check_vma=False,
    )
```

```python
import jax
import jax.numpy as jnp
from jax import lax
from jax.experimental import pallas as pl
from jax.experimental.pallas import tpu as pltpu
from jax.sharding import PartitionSpec as P

D = 4096
HEAD_DIM = 64
LAYERS = 2


EPS = 1e-06
HIGH = lax.Precision.HIGHEST


def solve_lower(a_mat, right_side):
    length = right_side.shape[-2]
    solved_rows = []
    for row_at in range(length):
        current_row = right_side[..., row_at, :]
        for col_at in range(row_at):
            current_row = current_row - a_mat[..., row_at, col_at][..., None] * solved_rows[col_at]
        solved_rows.append(current_row)
    return jnp.stack(solved_rows, axis=-2)


def delta_block(queries, key_rows, values, forgetting_exponent_amount, strength, matrix_state):
    length = queries.shape[2]
    causal = jnp.tril(jnp.ones((length, length), bool))
    strict = jnp.tril(jnp.ones((length, length), bool), -1)
    cumulative = jnp.cumsum(forgetting_exponent_amount, axis=-1)
    decay_mat = jnp.where(
        causal,
        jnp.exp(jnp.where(causal, cumulative[..., :, None] - cumulative[..., None, :], 0.0)),
        0.0,
    )
    key_gram = jnp.einsum("bhtd,bhsd->bhts", key_rows, key_rows, precision=HIGH)
    a_mat = jnp.where(strict, strength[..., :, None] * decay_mat * key_gram, 0.0)
    right_side = jnp.concatenate(
        [strength[..., None] * values, (strength * jnp.exp(cumulative))[..., None] * key_rows],
        axis=-1,
    )
    solved = solve_lower(a_mat, right_side)
    width_v = values.shape[-1]
    update = solved[..., :width_v] - jnp.einsum(
        "bhtk,bhkv->bhtv", solved[..., width_v:], matrix_state, precision=HIGH
    )
    scores = jnp.einsum("bhtd,bhsd->bhts", queries, key_rows, precision=HIGH) * decay_mat
    output = jnp.exp(cumulative)[..., None] * jnp.einsum(
        "bhtk,bhkv->bhtv", queries, matrix_state, precision=HIGH
    )
    output = output + jnp.einsum("bhts,bhsv->bhtv", scores, update, precision=HIGH)
    final_log = cumulative[..., -1:]
    revised_memory_matrix = jnp.exp(final_log)[..., None] * matrix_state + jnp.einsum(
        "bhsk,bhsv->bhkv",
        key_rows * jnp.exp(final_log - cumulative)[..., None],
        update,
        precision=HIGH,
    )
    return (output, revised_memory_matrix)


def unit_rows(matrix):
    return matrix * lax.rsqrt(jnp.sum(matrix * matrix, axis=-1, keepdims=True) + EPS)


def token_blender(
    mapped_token_vectors,
    magnitude_exponent,
    offset_terms_array,
    surplus_forgetting_exponent,
    multiplier_terms_array,
    incoming_memory_matrix,
    batch_total,
    generation_round_total,
):
    rounded = [
        lax.optimization_barrier(part_sum.astype(jnp.bfloat16)).astype(jnp.float32)
        for part_sum in mapped_token_vectors
    ]
    queries, keys_raw, values_raw, gate_raw, decay_pre, strength_pre = rounded
    head_count = incoming_memory_matrix.shape[1]

    def to_heads(matrix):
        return matrix.reshape(batch_total, generation_round_total, head_count, HEAD_DIM).transpose(
            0, 2, 1, 3
        )

    def per_head(matrix):
        return matrix.reshape(batch_total, generation_round_total, head_count).transpose(0, 2, 1)

    queries = unit_rows(jax.nn.silu(to_heads(queries))) * HEAD_DIM ** (-0.5)
    key_rows = unit_rows(jax.nn.silu(to_heads(keys_raw)))
    values = jax.nn.silu(to_heads(values_raw))
    forgetting_exponent_amount = -jnp.exp(magnitude_exponent)[None, :, None] * jax.nn.softplus(
        per_head(decay_pre) + offset_terms_array[None, :, None]
    )
    forgetting_exponent_amount = forgetting_exponent_amount + surplus_forgetting_exponent.transpose(
        0, 2, 1
    )
    strength = jax.nn.sigmoid(per_head(strength_pre))
    matrix_state = incoming_memory_matrix.reshape(batch_total, head_count, HEAD_DIM, HEAD_DIM)
    output, revised_memory_matrix = delta_block(
        queries, key_rows, values, forgetting_exponent_amount, strength, matrix_state
    )
    normed = output * lax.rsqrt(jnp.mean(output * output, axis=-1, keepdims=True) + EPS)
    normed = (
        normed
        * multiplier_terms_array.reshape(head_count, HEAD_DIM)[None, :, None, :]
        * jax.nn.silu(to_heads(gate_raw))
    )
    blended_token_vectors = (
        normed.transpose(0, 2, 1, 3)
        .reshape(batch_total * generation_round_total, head_count * HEAD_DIM)
        .astype(jnp.bfloat16)
    )
    return (
        blended_token_vectors,
        revised_memory_matrix.reshape(batch_total, head_count, HEAD_DIM * HEAD_DIM),
    )


LANES = 128


def bf16_dot(left, right):
    return jnp.dot(left, right, preferred_element_type=jnp.float32)


def head_sums(squares, ones):
    high = squares.astype(jnp.bfloat16)
    low = (squares - high.astype(jnp.float32)).astype(jnp.bfloat16)
    return bf16_dot(high, ones) + bf16_dot(low, ones)


def project(portion, weights):
    return tuple(
        (jnp.dot(portion, weight, preferred_element_type=jnp.float32) for weight in weights)
    )


def out_project(blended_token_vectors, weight_rows):
    return jnp.dot(
        lax.all_gather(blended_token_vectors, "tp", axis=1, tiled=True),
        weight_rows,
        preferred_element_type=jnp.float32,
    ).astype(jnp.bfloat16)


def post_residual(widened, mixed_out, multiplier_terms_array, complete):
    mixed_wide = lax.optimization_barrier(mixed_out).astype(jnp.float32)
    squares = jnp.sum(mixed_wide * mixed_wide, axis=-1)
    if not complete:
        squares = lax.psum(squares, "tp")
    post_rms = lax.rsqrt(squares / D + EPS)[:, None]
    return lax.optimization_barrier(
        (widened + mixed_wide * post_rms * multiplier_terms_array).astype(jnp.bfloat16)
    )


def local(
    residual_channel,
    prior_block_multiplier,
    probe_map_matrix,
    lookup_map_matrix,
    content_map_matrix,
    emission_valve_matrix,
    forgetting_map_matrix,
    insertion_rate_matrix,
    forgetting_magnitude_exponent,
    channel_forgetting_offset,
    surplus_forgetting_amounts,
    readout_rescale_multiplier,
    emission_map_matrix,
    post_mixing_multiplier,
    recurrent_matrices,
):
    batch_total, generation_round_total, own_width = residual_channel.shape
    head_count = recurrent_matrices.shape[2]
    row_count = batch_total * generation_round_total
    col_offset = lax.axis_index("tp") * own_width
    head_offset = lax.axis_index("tp") * head_count
    new_states = []

    def mix_layer(mapped_token_vectors, block_index_number):
        blended_token_vectors, revised_memory_matrix = token_blender(
            mapped_token_vectors,
            forgetting_magnitude_exponent[block_index_number],
            channel_forgetting_offset[block_index_number],
            surplus_forgetting_amounts[block_index_number],
            readout_rescale_multiplier[block_index_number],
            recurrent_matrices[block_index_number],
            batch_total,
            generation_round_total,
        )
        new_states.append(revised_memory_matrix)
        return out_project(blended_token_vectors, emission_map_matrix[block_index_number])

    def own_cols(matrix):
        return lax.dynamic_slice_in_dim(matrix, col_offset, own_width, matrix.ndim - 1)

    whole_rows = lax.all_gather(
        residual_channel.reshape(row_count, own_width), "tp", axis=1, tiled=True
    )
    current = whole_rows
    for block_index_number in range(LAYERS):
        widened = whole_rows.astype(jnp.float32)
        inv_rms = lax.rsqrt(jnp.mean(widened * widened, axis=-1, keepdims=True) + EPS)
        hidden = (widened * inv_rms * prior_block_multiplier[block_index_number]).astype(
            jnp.bfloat16
        )
        weights = (
            probe_map_matrix[block_index_number],
            lookup_map_matrix[block_index_number],
            content_map_matrix[block_index_number],
            emission_valve_matrix[block_index_number],
            lax.dynamic_slice_in_dim(
                forgetting_map_matrix[block_index_number], head_offset, head_count, 1
            ),
            lax.dynamic_slice_in_dim(
                insertion_rate_matrix[block_index_number], head_offset, head_count, 1
            ),
        )
        mapped_token_vectors = project(hidden, weights)
        mixed_out = mix_layer(mapped_token_vectors, block_index_number)
        if block_index_number < LAYERS - 1:
            gathered = lax.all_gather(mixed_out, "tp", axis=1, tiled=True)
            whole_rows = post_residual(
                widened, gathered, post_mixing_multiplier[block_index_number], True
            )
        else:
            current = post_residual(
                own_cols(widened),
                mixed_out,
                own_cols(post_mixing_multiplier[block_index_number]),
                False,
            )
    return (
        current.reshape(batch_total, generation_round_total, own_width),
        jnp.stack(new_states, axis=0),
    )


CHUNKS = 8
GROUP_ROWS = 64


def step_kernel(
    count,
    chunks,
    x_hbm,
    probe_hbm,
    lookup_hbm,
    content_hbm,
    valve_hbm,
    forget_hbm,
    insert_hbm,
    emission_hbm,
    states_hbm,
    surplus_hbm,
    pre_gain_hbm,
    post_gain_hbm,
    read_gain_hbm,
    magnitude_hbm,
    offset_hbm,
    out_ref,
    new_ref,
    in_ref,
    y_ref,
    w_ref,
    wo_ref,
    rates_ref,
    h_ref,
    x1_ref,
    xown_ref,
    mown_ref,
    sq_ref,
    sur_ref,
    state_ref,
    proj_ref,
    grown_ref,
    qk_ref,
    xq_ref,
    kd_ref,
    u_ref,
    qs_ref,
    dec_ref,
    spread_ref,
    ones_ref,
    perm_ref,
    surplus_ref,
    pre_gain_ref,
    post_gain_ref,
    read_gain_ref,
    magnitude_ref,
    offset_ref,
    load_sem,
    state_sem,
    own_sem,
    in_sem,
    y_sem,
    sq_sem,
):
    f32, bf16 = jnp.float32, jnp.bfloat16
    me = lax.axis_index("tp")
    depth = count // 4
    core, row, line = lax.rem(me, 2), lax.rem(me // 2, 2), me // 4
    over, twin = me + 2 - 4 * row, me + 1 - 2 * core
    items = 2 * chunks
    rows = h_ref.shape[0]
    seqs, steps = qk_ref.shape[1], qk_ref.shape[2]
    width = in_ref.shape[3]
    heads = forget_hbm.shape[1]
    own_heads = heads // count

    barrier = pltpu.get_barrier_semaphore()
    inner = (line == 1) | (line == 2)
    shifts = (0, 1 - 2 * lax.rem(line, 2), 2 - 4 * (line // 2), 3 - 2 * line)

    def along(step):
        return 4 * shifts[step]

    def when(condition, action, *operands):
        @pl.when(condition)
        def _():
            action(*operands)

    def greet(device):
        pl.semaphore_signal(
            barrier, inc=1, device_id={"tp": device}, device_id_type=pl.DeviceIdType.MESH
        )

    for device in (over, twin, me + along(1), me + along(2)):
        greet(device)
    when(inner, greet, me + along(3))

    loads = []
    for layer in range(2):
        for at, matrix in enumerate((probe_hbm, lookup_hbm, content_hbm, valve_hbm)):
            loads.append(
                (matrix.at[layer], w_ref.at[layer, :, pl.ds(at * LANES, LANES)])
            )
        loads.append((forget_hbm.at[layer], rates_ref.at[layer, pl.ds(0, heads), :]))
        loads.append((insert_hbm.at[layer], rates_ref.at[layer, pl.ds(heads, heads), :]))
        loads.append((emission_hbm.at[layer], wo_ref.at[layer]))
    loads += [
        (surplus_hbm, surplus_ref),
        (pre_gain_hbm, pre_gain_ref),
        (post_gain_hbm, post_gain_ref),
        (read_gain_hbm, read_gain_ref),
        (magnitude_hbm, magnitude_ref),
        (offset_hbm, offset_ref),
    ]
    loads = [
        pltpu.make_async_copy(source, target, load_sem.at[at])
        for at, (source, target) in enumerate(loads)
    ]
    for copy in loads:
        copy.start()

    def state_load(slot):
        layer, chunk = slot // chunks, lax.rem(slot, chunks)
        return pltpu.make_async_copy(
            states_hbm.at[layer, pl.ds(chunk * seqs, seqs)],
            state_ref.at[lax.rem(slot, 2)],
            state_sem.at[lax.rem(slot, 2)],
        )

    state_load(0).start()

    pl.semaphore_wait(barrier, 4 + lax.rem((line + 1) // 2, 2))

    def remote(source, target, send_sem, land_sem, device):
        return pltpu.make_async_remote_copy(
            src_ref=source,
            dst_ref=target,
            send_sem=send_sem,
            recv_sem=land_sem,
            device_id={"tp": device},
            device_id_type=pl.DeviceIdType.MESH,
        )

    def plain(buf, item):
        return (item == items - 1) if buf is y_ref else (item < 0)

    def begin(buf, sems, item, source):
        target = buf.at[item, me]

        def out(kind, device):
            remote(source, target, sems.at[0, item], sems.at[kind, item], device).start()

        out(5, me + along(2))
        out(4, me + along(1))
        when(inner | (plain(buf, item)), out, 6, me + along(3))
        out(1, over)
        out(3, twin)

    def pass_on(buf, sems, item, origin, kind, device, half=None):
        block = buf.at[item, origin]
        if half is not None:
            block = buf.at[item, origin, pl.ds(half * (rows // 2), rows // 2)]
        remote(block, block, sems.at[0, item], sems.at[kind, item], device).start()

    def landed(buf, sems, item, kind, blocks):
        part = buf.at[item, pl.ds(0, blocks)]
        remote(part, part, sems.at[0, item], sems.at[kind, item], twin).wait_recv()

    def relay_near(buf, sems, item):
        landed(buf, sems, item, 5, 1)
        onward = inner & jnp.logical_not(plain(buf, item))
        when(onward, pass_on, buf, sems, item, me + along(2), 6, me + along(1))
        pass_on(buf, sems, item, me + along(2), 2, over)
        pass_on(buf, sems, item, me + along(2), 3, twin)
        landed(buf, sems, item, 1, 1)
        pass_on(buf, sems, item, over, 2, me + along(1), 0)
        pass_on(buf, sems, item, over, 3, twin)
        landed(buf, sems, item, 4, 1)
        pass_on(buf, sems, item, me + along(1), 2, over, 1)
        pass_on(buf, sems, item, me + along(1), 3, twin)

    def relay_far(buf, sems, item):
        landed(buf, sems, item, 6, 1)
        pass_on(buf, sems, item, me + along(3), 2, over)
        pass_on(buf, sems, item, me + along(3), 3, twin)

    def relay_twin(buf, sems, item):
        landed(buf, sems, item, 2, depth - 1)
        for step in range(1, depth):
            pass_on(buf, sems, item, over + along(step), 3, twin)

    def complete(buf, sems, item):
        landed(buf, sems, item, 3, 2 * depth)

    def drained(buf, sems, item):
        def sent(blocks):
            part = buf.at[item, pl.ds(0, blocks)]
            remote(part, part, sems.at[0, item], sems.at[1, item], twin).wait_send()

        last = plain(buf, item)
        when(last, sent, count - 1)
        when(inner & jnp.logical_not(last), sent, count)
        when(jnp.logical_not(inner | last), sent, count - 2)

    def own_copy(item):
        return pltpu.make_async_copy(
            x_hbm.at[pl.ds(item * rows, rows), :], in_ref.at[item, me], own_sem.at[item]
        )

    def begin_x(item):
        begin(in_ref, in_sem, item, x_hbm.at[pl.ds(item * rows, rows), :])
        own_copy(item).start()

    begin_x(0)

    def iota(shape, axis):
        return lax.broadcasted_iota(jnp.int32, shape, axis)

    shape = (2 * heads, 2 * LANES)
    wanted = iota(shape, 1) // HEAD_DIM
    wanted = jnp.where(wanted >= 2, wanted - 2 + heads, wanted) + me * own_heads
    spread_ref[...] = jnp.where(iota(shape, 0) == wanted, 1.0, 0.0).astype(bf16)
    shape = (2 * LANES, 2 * LANES)
    ones_ref[...] = jnp.where(
        iota(shape, 0) // HEAD_DIM == iota(shape, 1) // HEAD_DIM, 1.0, 0.0
    ).astype(bf16)
    shape = (LANES, 4 * LANES)
    block, spot = iota(shape, 1) // LANES, iota(shape, 1) % LANES
    target = (block // 2) * HEAD_DIM + 2 * (spot // 2) + block % 2
    fits = (iota(shape, 0) == target) & (spot % 2 == block // 2) & (spot < HEAD_DIM)
    perm_ref[...] = jnp.where(fits, 1.0, 0.0).astype(bf16)
    for copy in loads:
        copy.wait()
    all_seqs = sur_ref.shape[1]
    first_head = iota((LANES, all_seqs), 0) < HEAD_DIM
    for layer in range(2):
        for step in range(steps):
            pair = surplus_ref[layer, step]
            wide = jnp.where(first_head, pair[0:1, :], pair[1:2, :])
            sur_ref[layer, :, step, :] = wide.T
        for origin in range(count):
            at = pl.ds(origin * width, width)
            pair = rates_ref[layer, :, at].astype(f32)
            padded = jnp.concatenate([pair, jnp.zeros((LANES - 2 * heads, width), f32)], axis=0)
            w_ref[layer, at, pl.ds(4 * LANES, LANES)] = padded.T.astype(bf16)

    relay_near(in_ref, in_sem, 0)
    relay_far(in_ref, in_sem, 0)
    begin_x(1)
    relay_twin(in_ref, in_sem, 0)
    begin_x(2)
    begin_x(3)

    def squares(matrix):
        return matrix[:, :LANES] * matrix[:, :LANES] + matrix[:, LANES:] * matrix[:, LANES:]

    def inverse(total):
        return lax.rsqrt(jnp.sum(total, axis=1, keepdims=True) * (1.0 / D) + EPS)

    def cols_of(origin):
        return pl.ds(origin * width, width)

    def first_hidden(item):
        def part(group, carry):
            at = pl.ds(group * GROUP_ROWS, GROUP_ROWS)
            total = jnp.zeros((GROUP_ROWS, LANES), f32)
            for origin in range(count):
                total = total + squares(in_ref[item, origin, at, :].astype(f32))
            scale = inverse(total)
            for origin in range(count):
                block = in_ref[item, origin, at, :].astype(f32)
                gain = pre_gain_ref[0:1, cols_of(origin)]
                h_ref[at, cols_of(origin)] = (block * scale * gain).astype(bf16)
            return carry

        lax.fori_loop(0, rows // GROUP_ROWS, part, 0)

    def second_hidden(item):
        earlier = item - chunks

        def part(group, carry):
            at = pl.ds(group * GROUP_ROWS, GROUP_ROWS)
            total = jnp.zeros((GROUP_ROWS, LANES), f32)
            for origin in range(count):
                total = total + squares(in_ref[item, origin, at, :].astype(f32))
            scale = inverse(total)
            total = jnp.zeros((GROUP_ROWS, LANES), f32)
            for origin in range(count):
                mixed = in_ref[item, origin, at, :].astype(f32)
                before = in_ref[earlier, origin, at, :].astype(f32)
                gain = post_gain_ref[0:1, cols_of(origin)]
                after = (before + mixed * scale * gain).astype(bf16)
                x1_ref[origin, at, :] = after
                total = total + squares(after.astype(f32))
            scale = inverse(total)
            for origin in range(count):
                block = x1_ref[origin, at, :].astype(f32)
                gain = pre_gain_ref[1:2, cols_of(origin)]
                h_ref[at, cols_of(origin)] = (block * scale * gain).astype(bf16)
            xown_ref[earlier, at, :] = x1_ref[me, at, :]
            return carry

        lax.fori_loop(0, rows // GROUP_ROWS, part, 0)

    def cols(at):
        return proj_ref[:, at * LANES : (at + 1) * LANES].astype(f32)

    def tokens(matrix):
        return matrix.reshape(seqs, steps, LANES)

    def lane_pair(ref, layer):
        left = iota((1, LANES), 1) < HEAD_DIM
        return jnp.where(left, ref[layer, 0], ref[layer, 1])

    def prepare(layer, chunk):
        ones = ones_ref[...]
        perm = perm_ref[...]
        queries = jax.nn.silu(cols(0))
        keys = jax.nn.silu(cols(1))
        sums = head_sums(jnp.concatenate([queries * queries, keys * keys], axis=1), ones)
        queries = tokens(queries * lax.rsqrt(sums[:, :LANES] + EPS) * HEAD_DIM ** (-0.5))
        keys = tokens(keys * lax.rsqrt(sums[:, LANES:] + EPS))
        spread = bf16_dot(proj_ref[:, 4 * LANES : 4 * LANES + 2 * heads], spread_ref[...])
        biased = spread[:, :LANES] + lane_pair(offset_ref, layer)
        softplus = jnp.maximum(biased, 0.0) + jnp.log1p(jnp.exp(-jnp.abs(biased)))
        pace = -jnp.exp(lane_pair(magnitude_ref, layer))
        cumulative = tokens(pace * softplus) + sur_ref[layer, pl.ds(chunk * seqs, seqs)]
        beta = tokens(jax.nn.sigmoid(spread[:, LANES:]))
        token = lax.broadcasted_iota(jnp.int32, (seqs, steps, LANES), 1)
        shift = 1
        while shift < steps:
            moved = pltpu.roll(cumulative, shift, axis=1)
            cumulative = cumulative + jnp.where(token >= shift, moved, 0.0)
            shift *= 2
        grown = jnp.exp(cumulative)
        grown_ref[...] = grown
        solved_u = beta * tokens(jax.nn.silu(cols(2)))
        solved_p = beta * grown * keys
        for at in range(steps):
            causal = token >= at
            gap = jnp.where(causal, cumulative - cumulative[:, at : at + 1, :], 0.0)
            decay = jnp.where(causal, jnp.exp(gap), 0.0)
            key_row = keys[:, at : at + 1, :]
            pair = jnp.concatenate([queries * key_row, keys * key_row], axis=2)
            dots = bf16_dot(pair.reshape(rows, 2 * LANES).astype(bf16), ones)
            qk_ref[at] = tokens(dots[:, :LANES]) * decay
            if at < steps - 1:
                a_col = jnp.where(token > at, beta * decay * tokens(dots[:, LANES:]), 0.0)
                solved_u = solved_u - a_col * solved_u[:, at : at + 1, :]
                solved_p = solved_p - a_col * solved_p[:, at : at + 1, :]
        last = cumulative[:, steps - 1 : steps, :]
        faded = keys * jnp.exp(last - cumulative)

        def scattered(matrix):
            placed = bf16_dot(matrix.reshape(-1, LANES).astype(bf16), perm)
            blocks = [placed[:, at * LANES : (at + 1) * LANES] for at in range(4)]
            return [block.reshape(seqs, -1, LANES) for block in blocks]

        for at, block in enumerate(scattered(jnp.concatenate([queries, solved_p], axis=1))):
            xq_ref[:, at * 2 * steps : (at + 1) * 2 * steps, :] = block.astype(bf16)
        blocks = scattered(faded)
        for at in (0, 2):
            both = jnp.concatenate([blocks[at], blocks[at + 1]], axis=1).astype(bf16)
            kd_ref[:, at * steps : (at + 2) * steps, :] = both
            kd_ref[:, (at + 4) * steps : (at + 6) * steps, :] = both
        u_ref[...] = solved_u
        fade = jnp.broadcast_to(jnp.exp(last), (seqs, steps, LANES))
        lane = lax.broadcasted_iota(jnp.int32, (seqs, steps, LANES), 2)
        kept = (token % 2 == 0) == (lane < HEAD_DIM)
        dec_ref[...] = jnp.where(kept, fade, pltpu.roll(fade, HEAD_DIM, axis=2))

    state_rows = state_ref.shape[2]

    def advance(slot, layer, chunk):
        pair_left = iota((2 * steps, LANES), 1) < HEAD_DIM
        left = iota((steps, LANES), 1) < HEAD_DIM

        def one_sequence(at, carry):
            state = state_ref[slot, at]
            read = bf16_dot(xq_ref[at, :, pl.ds(0, state_rows)], state.astype(bf16))
            parts = [read[2 * steps * b : 2 * steps * (b + 1)] for b in range(4)]
            straight = jnp.where(pair_left, parts[0], parts[3])
            crossed = jnp.where(pair_left, parts[2], parts[1])
            read = straight + pltpu.roll(crossed, HEAD_DIM, axis=1)
            qs_ref[at] = read[:steps]
            update = u_ref[at] - read[steps:]
            u_ref[at] = update
            high = update.astype(bf16).astype(f32)
            spread = []
            for part in (high, update - high):
                turned = pltpu.roll(part, HEAD_DIM, axis=1)
                spread += [
                    jnp.where(left, part, 0.0),
                    jnp.where(left, 0.0, turned),
                    jnp.where(left, turned, 0.0),
                    jnp.where(left, 0.0, part),
                ]
            grow = lax.dot_general(
                kd_ref[at, :, pl.ds(0, state_rows)],
                jnp.concatenate(spread, axis=0).astype(bf16),
                (((0,), (0,)), ((), ())),
                preferred_element_type=f32,
            )
            factor = jnp.concatenate([dec_ref[at]] * (state_rows // steps), axis=0)
            new_ref[layer, chunk * seqs + at] = factor * state + grow
            return carry

        lax.fori_loop(0, seqs, one_sequence, 0, unroll=8)

    def read_out(item, layer):
        update = u_ref[...]
        output = grown_ref[...] * qs_ref[...]
        for at in range(steps):
            output = output + qk_ref[at] * update[:, at : at + 1, :]
        output = output.reshape(rows, LANES)
        sums = head_sums(output * output, ones_ref[:LANES, :LANES])
        output = output * lax.rsqrt(sums * (1.0 / HEAD_DIM) + EPS)
        gain = read_gain_ref[pl.ds(layer, 1), :]
        y_ref[item, me] = (output * gain * jax.nn.silu(cols(3))).astype(bf16)

    def emit(item):
        whole = jnp.concatenate([y_ref[item, origin] for origin in range(count)], axis=1)
        return bf16_dot(whole, wo_ref[item // chunks]).astype(bf16)

    def emit_middle(item):
        in_ref[item + chunks, me] = emit(item)

    def emit_last(item):
        mixed = emit(item)
        chunk = item - chunks
        mown_ref[chunk] = mixed
        wide = mixed.astype(f32)
        total = jnp.sum(squares(wide), axis=1, keepdims=True)
        sq_ref[chunk, me] = jnp.broadcast_to(total, (rows, LANES)).T[:1]

    def sums_begin(chunk):
        block = sq_ref.at[chunk, me]
        for step in range(1, count):
            remote(
                block, block, sq_sem.at[0, chunk], sq_sem.at[1, chunk], lax.rem(me + step, count)
            ).start()

    def sums_all(chunk):
        part = sq_ref.at[chunk, pl.ds(0, count - 1)]
        return remote(part, part, sq_sem.at[0, chunk], sq_sem.at[1, chunk], twin)

    def finish(chunk):
        sums_all(chunk).wait_recv()
        total = sq_ref[chunk, 0]
        for origin in range(1, count):
            total = total + sq_ref[chunk, origin]
        total = jnp.broadcast_to(total, (LANES, rows)).T
        scale = lax.rsqrt(total * (1.0 / D) + EPS)
        for half in range(width // LANES):
            at = pl.ds(half * LANES, LANES)
            gain = post_gain_ref[1:2, pl.ds(pl.multiple_of(me * width + half * LANES, LANES), LANES)]
            before = xown_ref[chunk, :, at].astype(f32)
            mixed = mown_ref[chunk, :, at].astype(f32)
            out_ref[pl.ds(pl.multiple_of(chunk * rows, rows), rows), at] = (before + mixed * scale * gain).astype(bf16)

    hold = chunks + 3

    def slot_of(slot, carry):
        layer, chunk, buffer = slot // chunks, lax.rem(slot, chunks), lax.rem(slot, 2)
        busy, first = slot < items, slot < chunks

        def early(by):
            return (slot >= by) & (slot < by + chunks)

        def late(by, action, *operands):
            for side in (1, 0):
                at = 2 * (slot - by - hold) - side
                when((at >= 0) & (at < chunks), action, *operands, at + chunks)

        when(slot + 1 < items, lambda: state_load(slot + 1).start())
        when(slot + 4 < chunks, lambda: begin_x(slot + 4))
        when(busy, complete, in_ref, in_sem, slot)

        @pl.when(first)
        def _():
            own_copy(slot).wait()
            first_hidden(slot)

        when(busy & (slot >= chunks), second_hidden, slot)

        @pl.when(busy)
        def _():
            proj_ref[...] = bf16_dot(h_ref[...], w_ref[layer]).astype(bf16)

        when(early(6), relay_far, in_ref, in_sem, slot - 6 + chunks)
        when(slot == 0, relay_near, in_ref, in_sem, 1)
        when(early(2), relay_far, y_ref, y_sem, slot - 2)
        late(2, relay_far, y_ref, y_sem)
        when(early(7), relay_twin, in_ref, in_sem, slot - 7 + chunks)
        when(early(3), relay_twin, y_ref, y_sem, slot - 3)
        late(3, relay_twin, y_ref, y_sem)
        when(busy, prepare, layer, chunk)
        when(slot + 2 < chunks, relay_near, in_ref, in_sem, slot + 2)
        when(slot == 0, relay_far, in_ref, in_sem, 1)

        @pl.when(busy)
        def _():
            state_load(slot).wait()
            advance(buffer, layer, chunk)

        when(early(1), relay_near, y_ref, y_sem, slot - 1)
        when(early(5), relay_near, in_ref, in_sem, slot - 5 + chunks)
        late(1, relay_near, y_ref, y_sem)
        when(slot + 2 < chunks, relay_far, in_ref, in_sem, slot + 2)
        when(busy, read_out, slot, layer)
        when(early(3), complete, y_ref, y_sem, slot - 3)
        when(first, lambda: begin(y_ref, y_sem, slot, y_ref.at[slot, me]))
        when(early(3), emit_middle, slot - 3)
        late(3, complete, y_ref, y_sem)
        late(3, emit_last)
        when(slot + 1 < chunks, relay_twin, in_ref, in_sem, slot + 1)
        late(0, lambda item: begin(y_ref, y_sem, item, y_ref.at[item, me]))

        @pl.when(early(3))
        def _():
            made = slot - 3 + chunks
            begin(in_ref, in_sem, made, in_ref.at[made, me])

        late(3, lambda item: sums_begin(item - chunks))
        return carry

    lax.fori_loop(0, items, slot_of, 0)
    final = items - 1

    def emit_pair(*targets):
        for target in targets:
            complete(y_ref, y_sem, target)
            emit_last(target)
        for target in targets:
            sums_begin(target - chunks)

    for target in (final - 2, final - 1):
        relay_far(y_ref, y_sem, target)
    for target in (final - 4, final - 3):
        relay_twin(y_ref, y_sem, target)
    relay_near(y_ref, y_sem, final)
    relay_far(y_ref, y_sem, final)
    emit_pair(final - 4, final - 3)
    for target in (final - 2, final - 1):
        relay_twin(y_ref, y_sem, target)
    for chunk in range(3):
        finish(chunk)
    emit_pair(final - 2, final - 1)
    relay_twin(y_ref, y_sem, final)
    for chunk in range(3, 5):
        finish(chunk)
    emit_pair(final)

    def drain(item, carry):
        drained(in_ref, in_sem, item)
        drained(y_ref, y_sem, item)
        return carry

    lax.fori_loop(0, items, drain, 0)
    for chunk in range(chunks - 3, chunks):
        finish(chunk)
    for chunk in range(chunks):
        sums_all(chunk).wait_send()


def deliver_kernel(first_ref, second_ref, first_hbm, second_hbm, sem):
    layers, parts = second_ref.shape[0], 16
    size = second_ref.shape[1] // parts
    copies = [pltpu.make_async_copy(first_ref, first_hbm, sem.at[layers * parts])]
    for layer in range(layers):
        for part in range(parts):
            at = pl.ds(part * size, size)
            copies.append(
                pltpu.make_async_copy(
                    second_ref.at[layer, at],
                    second_hbm.at[layer, at],
                    sem.at[layer * parts + part],
                )
            )
    for copy in copies:
        copy.start()
    for copy in copies:
        copy.wait()


def deliver(first, second):
    hbm = pl.BlockSpec(memory_space=pl.ANY)
    return pl.pallas_call(
        deliver_kernel,
        out_shape=[
            jax.ShapeDtypeStruct(first.shape, first.dtype),
            jax.ShapeDtypeStruct(second.shape, second.dtype),
        ],
        in_specs=[hbm, hbm],
        out_specs=[hbm, hbm],
        scratch_shapes=[pltpu.SemaphoreType.DMA((16 * second.shape[0] + 1,))],
        compiler_params=pltpu.CompilerParams(vmem_limit_bytes=1024 * 1024),
        name="deliver",
    )(first, second)


def local_two_heads(
    residual_channel,
    prior_block_multiplier,
    probe_map_matrix,
    lookup_map_matrix,
    content_map_matrix,
    emission_valve_matrix,
    forgetting_map_matrix,
    insertion_rate_matrix,
    forgetting_magnitude_exponent,
    channel_forgetting_offset,
    surplus_forgetting_amounts,
    readout_rescale_multiplier,
    emission_map_matrix,
    post_mixing_multiplier,
    recurrent_matrices,
):
    batch_total, steps, own_width = residual_channel.shape
    layers, _, head_count, state_size = recurrent_matrices.shape
    row_count = batch_total * steps
    count = lax.axis_size("tp")
    groups = state_size // LANES
    chunks = CHUNKS
    seqs, rows = batch_total // chunks, row_count // chunks
    heads = forgetting_map_matrix.shape[2]
    features = forgetting_map_matrix.shape[1]
    mix_width = emission_map_matrix.shape[1]
    states = (
        recurrent_matrices.reshape(layers, batch_total, head_count, groups, LANES)
        .transpose(0, 1, 3, 2, 4)
        .reshape(layers, batch_total, groups * head_count, LANES)
    )
    f32, bf16 = jnp.float32, jnp.bfloat16
    dma = pltpu.SemaphoreType.DMA
    hbm = pl.BlockSpec(memory_space=pl.ANY)
    vmem = pl.BlockSpec(memory_space=pltpu.VMEM)
    tile = (seqs, steps, LANES)
    state_tile = (2, seqs, groups * head_count, LANES)
    current, new_memory = pl.pallas_call(
        lambda *refs: step_kernel(count, chunks, *refs),
        out_shape=[
            pltpu.VMEM((row_count, own_width), bf16),
            pltpu.VMEM(states.shape, f32),
        ],
        in_specs=[hbm] * 15,
        out_specs=[vmem, vmem],
        scratch_shapes=[
            pltpu.VMEM((2 * chunks, count, rows, own_width), bf16),
            pltpu.VMEM((2 * chunks, count, rows, LANES), bf16),
            pltpu.VMEM((layers, features, 5 * LANES), bf16),
            pltpu.VMEM((layers, mix_width, own_width), bf16),
            pltpu.VMEM((layers, 2 * heads, features), bf16),
            pltpu.VMEM((rows, features), bf16),
            pltpu.VMEM((count, rows, own_width), bf16),
            pltpu.VMEM((chunks, rows, own_width), bf16),
            pltpu.VMEM((chunks, rows, own_width), bf16),
            pltpu.VMEM((chunks, count, 1, rows), f32),
            pltpu.VMEM((layers, batch_total, steps, LANES), f32),
            pltpu.VMEM(state_tile, f32),
            pltpu.VMEM((rows, 5 * LANES), bf16),
            pltpu.VMEM(tile, f32),
            pltpu.VMEM((steps,) + tile, f32),
            pltpu.VMEM((seqs, 8 * steps, LANES), bf16),
            pltpu.VMEM((seqs, 8 * steps, LANES), bf16),
            pltpu.VMEM(tile, f32),
            pltpu.VMEM(tile, f32),
            pltpu.VMEM(tile, f32),
            pltpu.VMEM((2 * heads, 2 * LANES), bf16),
            pltpu.VMEM((2 * LANES, 2 * LANES), bf16),
            pltpu.VMEM((LANES, 4 * LANES), bf16),
            pltpu.VMEM((layers, steps, head_count, batch_total), f32),
            pltpu.VMEM((layers, features), f32),
            pltpu.VMEM((layers, features), f32),
            pltpu.VMEM((layers, LANES), f32),
            pltpu.SMEM((layers, head_count), f32),
            pltpu.SMEM((layers, head_count), f32),
            dma((20,)),
            dma((2,)),
            dma((chunks,)),
            dma((3 + count // 4, 2 * chunks)),
            dma((3 + count // 4, 2 * chunks)),
            dma((2, chunks)),
        ],
        compiler_params=pltpu.CompilerParams(
            collective_id=1, has_side_effects=True, vmem_limit_bytes=46 * 1024 * 1024
        ),
        name="step",
    )(
        residual_channel.reshape(row_count, own_width),
        probe_map_matrix,
        lookup_map_matrix,
        content_map_matrix,
        emission_valve_matrix,
        forgetting_map_matrix.transpose(0, 2, 1),
        insertion_rate_matrix.transpose(0, 2, 1),
        emission_map_matrix,
        states,
        surplus_forgetting_amounts.transpose(0, 2, 3, 1),
        prior_block_multiplier,
        post_mixing_multiplier,
        readout_rescale_multiplier,
        forgetting_magnitude_exponent,
        channel_forgetting_offset,
    )
    current, new_memory = deliver(current, new_memory)
    new_memory = (
        new_memory.reshape(layers, batch_total, groups, head_count, LANES)
        .transpose(0, 1, 3, 2, 4)
        .reshape(recurrent_matrices.shape)
    )
    return current.reshape(batch_total, steps, own_width), new_memory


def local_any(*arrays):
    residual_channel, recurrent_matrices = arrays[0], arrays[-1]
    two_heads = (
        recurrent_matrices.shape[2] * HEAD_DIM == LANES
        and residual_channel.shape[1] == 8
        and residual_channel.shape[0] % (8 * CHUNKS) == 0
        and residual_channel.shape[2] % LANES == 0
        and lax.axis_size("tp") == 16
    )
    return (local_two_heads if two_heads else local)(*arrays)


def solution(mesh):
    return jax.shard_map(
        local_any,
        mesh=mesh,
        in_specs=(
            P("grp", None, "tp"),
            P(),
            P(None, None, "tp"),
            P(None, None, "tp"),
            P(None, None, "tp"),
            P(None, None, "tp"),
            P(),
            P(),
            P(None, "tp"),
            P(None, "tp"),
            P(None, "grp", None, "tp"),
            P(None, "tp"),
            P(None, None, "tp"),
            P(),
            P(None, "grp", "tp", None),
        ),
        out_specs=(P("grp", None, "tp"), P(None, "grp", "tp", None)),
        check_vma=False,
    )
```
